128 devices in a mesh: sp: 32 (over z, y, core), tp: 4 (over x).
Axes of the slice: x: 4, y: 4, z: 4, core: 2. Of those that a mesh axis runs over, the one named last changes fastest.
Arguments:
- queries: bfloat16 [12288, 2048], P('sp', 'tp'), may hold values from -6 to 6
- keys: bfloat16 [12288, 2048], P('sp', 'tp'), may hold values from -6 to 6
- values: bfloat16 [12288, 2048], P('sp', 'tp'), may hold values from -6 to 6
- gates: bfloat16 [12288, 2048], P('sp', 'tp'), may hold values from -8 to 8
- decay_pre: float32 [32, 12288], P('tp', 'sp'), may hold values from -18 to 3
- beta_pre: float32 [32, 12288], P('tp', 'sp'), may hold values from -10 to 3
- out_gain: float32 [64], replicated, may hold values from 0.1 to 1.9
- w_out: bfloat16 [2048, 2048], P('tp'), may hold values from -0.125 to 0.125
- stream: bfloat16 [12288, 2048], P(('sp', 'tp')), may hold values from -6 to 6
- norm_gain: float32 [2048], replicated, may hold values from 0.1 to 1.9
- w_gate: bfloat16 [2048, 5632], P('sp', 'tp'), may hold values from -0.125 to 0.125
- w_up: bfloat16 [2048, 5632], P('sp', 'tp'), may hold values from -0.125 to 0.125
- w_down: bfloat16 [5632, 2048], P('tp', 'sp'), may hold values from -0.078125 to 0.078125
Outputs:
- updated: bfloat16 [12288, 2048], P(('sp', 'tp'))
The draws below stay inside these ranges and needn't reach their ends.
All inputs are finite; a program needn't handle non-finite values.
Results may differ from the reference program's by a relative error of at most 0.019.
Values may be sent and summed in bfloat16 or wider, within the bound.
No kernel may reach another device: no remote copies, remote signals or barrier semaphores. Data moves between devices by JAX's collectives and lax.ppermute only.
A program may use at most 128 MiB of HBM per device.

```python
import math
import jax
import jax.numpy as jnp
from jax import lax

D = 2048
HEADS = 32
HEAD_DIM = 64
FF = 5632
BLOCK = 64
TOK_DEV = 384
TOKEN_POSITIONS = 12288
N_TP = 4


def slow_heads(key):
    order = jax.random.permutation(jax.random.fold_in(key, 17), HEADS)
    keep_count = HEADS // 2
    return order < keep_count


def draw_decay_pre(key, part):
    slow = slow_heads(key)[:, None]
    noise_random_key, shard_random_key, spike_random_key = jax.random.split(jax.random.fold_in(key, 29), 3)
    small_noise = jnp.clip(jax.random.normal(noise_random_key, (HEADS, TOKEN_POSITIONS), jnp.float32), -3.0, 3.0)
    span_levels = jax.random.uniform(shard_random_key, (HEADS, TOKEN_POSITIONS // TOK_DEV), jnp.float32, -0.7, 0.7)
    noise_deviation = jnp.repeat(span_levels, TOK_DEV, axis=1)
    slow_level = math.log(0.35 / TOKEN_POSITIONS) - 0.5
    fast_level = math.log(0.04) - 0.5
    noise_amplitude = jnp.where(slow, slow_level, fast_level)
    spike_locations = jax.random.randint(spike_random_key, (3,), 0, TOKEN_POSITIONS)
    token_places = jnp.arange(TOKEN_POSITIONS)
    spike_mask = jnp.any(token_places[None, :] == spike_locations[:, None], axis=0)
    return jnp.where(spike_mask[None, :], -1.0, noise_amplitude + small_noise + noise_deviation).astype(jnp.float32)


def draw_beta_pre(key, part):
    slow = slow_heads(key)[:, None]
    noise_random_key = jax.random.fold_in(key, 43)
    small_noise = jnp.clip(0.6 * jax.random.normal(noise_random_key, (HEADS, TOKEN_POSITIONS), jnp.float32), -3.0, 3.0)
    rate = min(82.0 / TOKEN_POSITIONS, 0.5)
    slow_level = math.log(rate / (1.0 - rate))
    return (jnp.where(slow, slow_level, 0.0) + small_noise).astype(jnp.float32)


def shard_levels(stream_key, dims, cuts, least, largest):
    def one(position, blocks):
        heights = jax.random.uniform(jax.random.fold_in(jax.random.fold_in(stream_key, 6), position), (blocks,), jnp.float32, least / len(cuts), largest / len(cuts))
        return jnp.repeat(jnp.exp(heights), dims[position] // blocks).reshape((-1,) + (1,) * (len(dims) - position - 1))

    level = one(*cuts[0])
    for cut in cuts[1:]:
        level = level * one(*cut)
    return level


def centred(own_key, shape, spread, bound, shards=(), kind=jnp.bfloat16):
    values = jax.random.normal(own_key, shape, jnp.float32) * spread
    if len(shards) > 0:
        values = shard_levels(own_key, shape, shards, -0.22, 0.18) * values
    return jnp.clip(values, min=-bound, max=bound).astype(kind)


def setup_inputs(seed: int = 0) -> dict:
    key_of = jax.random.split(jax.random.key(seed), 14)
    return {
        "queries": centred(key_of[0], (TOKEN_POSITIONS, HEADS * HEAD_DIM), 1.0, 6.0, ((0, 32), (1, 4))),
        "keys": centred(key_of[1], (TOKEN_POSITIONS, HEADS * HEAD_DIM), 1.0, 6.0, ((0, 32), (1, 4))),
        "values": centred(key_of[2], (TOKEN_POSITIONS, HEADS * HEAD_DIM), 1.0, 6.0, ((0, 32), (1, 4))),
        "gates": centred(key_of[3], (TOKEN_POSITIONS, HEADS * HEAD_DIM), 1.5, 8.0, ((0, 32), (1, 4))),
        "decay_pre": draw_decay_pre(jax.random.fold_in(key_of[13], 71), 0),
        "beta_pre": draw_beta_pre(jax.random.fold_in(key_of[13], 71), 0),
        "out_gain": jnp.clip(1.0 + 0.18 * jax.random.normal(key_of[6], (HEAD_DIM,), jnp.float32), 0.1, 1.9),
        "w_out": centred(key_of[7], (HEADS * HEAD_DIM, D), (HEADS * HEAD_DIM) ** -0.5, 0.125, ((0, 4),)),
        "stream": centred(key_of[8], (TOKEN_POSITIONS, D), 1.0, 6.0, ((0, 128),)),
        "norm_gain": jnp.clip(1.0 + 0.18 * jax.random.normal(key_of[9], (D,), jnp.float32), 0.1, 1.9),
        "w_gate": centred(key_of[10], (D, FF), D ** -0.5, 0.125, ((0, 32), (1, 4))),
        "w_up": centred(key_of[11], (D, FF), D ** -0.5, 0.125, ((0, 32), (1, 4))),
        "w_down": centred(key_of[12], (FF, D), FF ** -0.5, 0.078125, ((0, 4), (1, 32))),
    }


EPSILON = 1e-06
EXACT_PRECISION = lax.Precision.HIGHEST

def unit_lower_inverse(lower_mat):
    span_len = lower_mat.shape[-1]
    identity = jnp.eye(span_len, dtype=jnp.float32)
    power = -lower_mat
    inverse = identity + power
    steps = 1
    while 1 << steps < span_len:
        power = jnp.einsum('...ij,...jk->...ik', power, power, precision=EXACT_PRECISION)
        inverse = jnp.einsum('...ij,...jk->...ik', inverse, identity + power, precision=EXACT_PRECISION)
        steps = steps + 1
    return inverse

def prepare(queries, keys, values, beta_pre, decay_pre):
    length = queries.shape[0]
    heads = queries.shape[1] // HEAD_DIM

    def split_heads(arr):
        return arr.astype(jnp.float32).reshape(length, heads, HEAD_DIM)
    query_unit = jax.nn.silu(split_heads(queries))
    query_unit = query_unit * lax.rsqrt(lax.optimization_barrier(jnp.sum(query_unit * query_unit, axis=-1, keepdims=True)) + EPSILON)
    query_unit = (query_unit * HEAD_DIM ** (-0.5)).astype(jnp.bfloat16)
    key_unit = jax.nn.silu(split_heads(keys))
    key_unit = (key_unit * lax.rsqrt(lax.optimization_barrier(jnp.sum(key_unit * key_unit, axis=-1, keepdims=True)) + EPSILON)).astype(jnp.bfloat16)
    value_act = jax.nn.silu(split_heads(values))
    strength = jax.nn.sigmoid(beta_pre.astype(jnp.float32))
    log_decay = -jax.nn.softplus(decay_pre.astype(jnp.float32))
    nblocks = length // BLOCK

    def blocked(arr):
        return arr.reshape(nblocks, BLOCK, heads, HEAD_DIM).transpose(0, 2, 1, 3)

    def blocked_rates(arr):
        return arr.reshape(heads, nblocks, BLOCK).transpose(1, 0, 2)
    return (blocked(query_unit), blocked(key_unit), blocked(value_act), blocked_rates(strength), blocked_rates(log_decay))

def block_terms(query_blk, key_blk, value_blk, strength_blk, decay_blk):
    span_len = query_blk.shape[-2]
    query_f = query_blk.astype(jnp.float32)
    key_f = key_blk.astype(jnp.float32)
    cumulative = jnp.cumsum(decay_blk, axis=-1)
    row_ids = jnp.arange(span_len)[:, None]
    col_ids = jnp.arange(span_len)[None, :]
    inclusive = row_ids >= col_ids
    strict = row_ids > col_ids
    decay_mat = jnp.exp(jnp.where(inclusive, cumulative[..., :, None] - cumulative[..., None, :], -jnp.inf))
    key_inner = jnp.einsum('...id,...jd->...ij', key_f, key_f, precision=EXACT_PRECISION)
    lower_mat = jnp.where(strict, strength_blk[..., :, None] * key_inner * decay_mat, 0.0)
    key_strong = key_f * strength_blk[..., None]
    right_side = jnp.concatenate([value_blk * strength_blk[..., None], key_strong * jnp.exp(cumulative)[..., None]], axis=-1)
    solved = jnp.einsum('...ij,...jk->...ik', unit_lower_inverse(lower_mat), right_side, precision=EXACT_PRECISION)
    width = value_blk.shape[-1]
    update_values = solved[..., :width]
    update_keys = solved[..., width:]
    query_inner = jnp.einsum('...id,...jd->...ij', query_f, key_f, precision=EXACT_PRECISION)
    inside_span = jnp.where(inclusive, query_inner * decay_mat, 0.0)
    final_decay = cumulative[..., -1:]
    key_attenuated = key_f * jnp.exp(final_decay - cumulative)[..., None]
    query_attenuated = query_f * jnp.exp(cumulative)[..., None]
    return (update_values, update_keys, inside_span, query_attenuated, key_attenuated, final_decay)

def advance(matrix_state, terms):
    update_values, update_keys, inside_span, query_attenuated, key_attenuated, final_decay = terms
    value_corrected = update_values - jnp.einsum('jod,jdg->jog', update_keys, matrix_state, precision=EXACT_PRECISION)
    output_result = jnp.einsum('jod,jdg->jog', query_attenuated, matrix_state, precision=EXACT_PRECISION) + jnp.einsum('oyn,onk->oyk', inside_span, value_corrected, precision=EXACT_PRECISION)
    matrix_state = matrix_state * jnp.exp(final_decay)[..., None] + jnp.einsum('lyq,lyf->lqf', key_attenuated, value_corrected, precision=EXACT_PRECISION)
    return (matrix_state, output_result)

def finish(outputs, gates, out_gain):
    length = gates.shape[0]
    heads = gates.shape[1] // HEAD_DIM
    heads_out = outputs.transpose(0, 2, 1, 3).reshape(length, heads, HEAD_DIM)
    heads_out = heads_out * lax.rsqrt(lax.optimization_barrier(jnp.mean(heads_out * heads_out, axis=-1, keepdims=True)) + EPSILON)
    heads_out = heads_out * out_gain.astype(jnp.float32)
    gated = heads_out * jax.nn.silu(gates.astype(jnp.float32).reshape(length, heads, HEAD_DIM))
    return gated.reshape(length, heads * HEAD_DIM).astype(jnp.bfloat16)

def reference(queries, keys, values, gates, decay_pre, beta_pre, out_gain, w_out, stream, norm_gain, w_gate, w_up, w_down):
    blocks = prepare(queries, keys, values, beta_pre, decay_pre)
    terms = block_terms(*blocks)
    heads = queries.shape[1] // HEAD_DIM
    start_state = jnp.zeros((heads, HEAD_DIM, HEAD_DIM), jnp.float32)
    _, outputs = lax.scan(advance, start_state, terms)
    mixed_heads = finish(outputs, gates, out_gain)
    projected = jnp.dot(mixed_heads, w_out, preferred_element_type=jnp.float32)
    middle = (stream.astype(jnp.float32) + projected).astype(jnp.bfloat16)
    middle_f = middle.astype(jnp.float32)
    normed = middle_f * lax.rsqrt(lax.optimization_barrier(jnp.mean(middle_f * middle_f, axis=-1, keepdims=True)) + EPSILON)
    normed = (normed * norm_gain.astype(jnp.float32)).astype(jnp.bfloat16)
    length = normed.shape[0]
    group_width = FF // N_TP

    def ffn_block(rows):
        gate_hidden = jnp.dot(rows, w_gate, preferred_element_type=jnp.float32)
        up_hidden = jnp.dot(rows, w_up, preferred_element_type=jnp.float32)
        hidden = (jax.nn.silu(gate_hidden) * up_hidden).astype(jnp.bfloat16)
        total = jnp.zeros((rows.shape[0], w_down.shape[1]), jnp.float32)
        for member in range(N_TP):
            partial_sum = jnp.dot(hidden[:, member * group_width:(member + 1) * group_width], w_down[member * group_width:(member + 1) * group_width], preferred_element_type=jnp.float32).astype(jnp.bfloat16)
            partial_sum = lax.optimization_barrier(partial_sum)
            total = total + partial_sum.astype(jnp.float32)
        return total
    row_blocks = normed.reshape(length // TOK_DEV, TOK_DEV, normed.shape[1])
    channel_sum = lax.map(ffn_block, row_blocks).reshape(length, normed.shape[1])
    return (middle_f + 0.5 * channel_sum).astype(jnp.bfloat16)
```

```python
import jax
import jax.numpy as jnp
from jax import lax
from jax.experimental import pallas as pl
from jax.experimental.pallas import tpu as pltpu
from jax.sharding import Mesh
from jax.sharding import PartitionSpec as P

HEAD_DIM = 64
PAIR = 2 * HEAD_DIM
CHUNK = 128
SP = ("sp_0", "sp_1", "sp_2")
SP_TP = ("sp_0", "sp_1", "sp_2", "tp")
EPSILON = 1e-06
BF = jnp.bfloat16
F32 = jnp.float32
NT = (((1,), (1,)), ((), ()))
HIGH = lax.Precision.HIGHEST


def dot(a, b):
    return jnp.dot(a, b, preferred_element_type=F32)


def dot_nt(a, b, precision=None):
    return lax.dot_general(a, b, NT, precision=precision, preferred_element_type=F32)


def silu(x):
    return x / (1.0 + jnp.exp(-x))


def places():
    row = lax.broadcasted_iota(jnp.int32, (PAIR, PAIR), 0)
    col = lax.broadcasted_iota(jnp.int32, (PAIR, PAIR), 1)
    return row, col


def half_sums(squares, ones):
    high = squares.astype(BF)
    low = (squares - high.astype(F32)).astype(BF)
    return dot(high, ones) + dot(low, ones)


def softplus(x):
    small = jnp.exp(-jnp.abs(x))
    series = small * (1.0 - small * (0.5 - small * (1.0 / 3.0 - 0.25 * small)))
    return jnp.maximum(x, 0.0) + jnp.where(small < 0.015, series, jnp.log(1.0 + small))


def turned(z):
    return pltpu.roll(z, HEAD_DIM, 1)


def keys_kernel(
    k_ref, v_ref, beta_ref, decay_ref,
    before_ref, total_ref, y_ref, d_ref, kb_ref, ec_ref,
    run_ref, l_ref, x_ref, r_ref,
):
    chunk = pl.program_id(0)
    row, col = places()
    left = col < HEAD_DIM
    top = row < HEAD_DIM
    same = left == top
    ones = jnp.where(same, 1.0, 0.0).astype(BF)
    inclusive = row >= col
    strict = row > col
    differ = row ^ col
    eye = jnp.where(row == col, 1.0, 0.0)
    off_eye = differ == HEAD_DIM
    triangle = jnp.where(inclusive, 1.0, 0.0)
    pairs = k_ref.shape[1] // PAIR

    @pl.when(chunk == 0)
    def _():
        for p in range(pairs):
            run_ref[p] = jnp.where(off_eye, 1.0, 0.0).astype(BF)

    rates = -softplus(decay_ref[...])
    strength = 1.0 / (1.0 + jnp.exp(-beta_ref[...]))
    cum_row = dot_nt(rates, triangle, HIGH)
    cum_col = dot_nt(triangle, rates, HIGH)
    beta_col = dot_nt(eye, strength, HIGH)
    kept = []
    for p in range(pairs):
        lanes = slice(p * PAIR, (p + 1) * PAIR)
        key = silu(k_ref[:, lanes].astype(F32))
        key = (key * lax.rsqrt(half_sums(key * key, ones) + EPSILON)).astype(BF)
        kb_ref[:, lanes] = key
        key_f = key.astype(F32)
        cums = [cum_col[:, h : h + 1] for h in (2 * p, 2 * p + 1)]
        betas = [beta_col[:, h : h + 1] for h in (2 * p, 2 * p + 1)]
        cum = jnp.where(left, cums[0], cums[1])
        beta = jnp.where(left, betas[0], betas[1])
        grown = jnp.exp(cum)
        ec_ref[:, lanes] = grown
        strong = turned(key_f * (beta * grown))
        value = silu(v_ref[:, lanes].astype(F32)) * beta
        r_ref[2 * p] = jnp.where(left, value, strong).astype(BF)
        r_ref[2 * p + 1] = jnp.where(left, strong, value).astype(BF)
        fade = jnp.exp(cum[CHUNK - 1 : CHUNK, :] - cum)
        faded = (key_f * fade).T.astype(BF)
        ends = [jnp.exp(c[CHUNK - 1 : CHUNK, :]) for c in cums]
        kept.append((faded, jnp.where(off_eye, jnp.where(top, ends[0], ends[1]), 0.0)))
        for s in range(2):
            h = 2 * p + s
            mine = left if s == 0 else jnp.logical_not(left)
            own = jnp.where(mine, key_f, 0.0).astype(BF)
            inner = dot_nt(own, key)
            decay = jnp.where(inclusive, jnp.exp(cums[s] - cum_row[h : h + 1, :]), 0.0)
            d_ref[h] = decay.astype(BF)
            lower = jnp.where(strict, inner * decay * betas[s], 0.0)
            l_ref[h] = lower.astype(BF)
            x_ref[h] = (eye - jnp.where(differ == 1, lower, 0.0)).astype(BF)
    heads = 2 * pairs
    for level in range(1, 7):
        mask = jnp.where((differ >> level) == 1, 1.0, 0.0).astype(BF)
        parts = [dot(x_ref[h], l_ref[h] * mask).astype(BF) for h in range(heads)]
        for h in range(heads):
            x = x_ref[h]
            x_ref[h] = x - dot(parts[h], x).astype(BF)
    for p in range(pairs):
        faded, ends = kept[p]
        got = []
        for h in (2 * p, 2 * p + 1):
            y = dot(x_ref[h], r_ref[h]).astype(BF)
            y_ref[h] = y
            got.append(dot(faded, y))
        z = jnp.where(top, got[0], got[1])
        z = jnp.where(same, z, ends - z)
        step = jnp.where(same, turned(z), 0.0).astype(BF)
        run = run_ref[p]
        before_ref[p] = run
        run = (dot(step, run) + jnp.where(same, z, 0.0)).astype(BF)
        run_ref[p] = run
        total_ref[p] = run


def keys_side(keys, values, beta_pre, decay_pre):
    length, width = keys.shape
    heads = width // HEAD_DIM
    pairs = width // PAIR
    steps = length // CHUNK
    rows = pl.BlockSpec((CHUNK, width), lambda c: (c, 0))
    rates = pl.BlockSpec((heads, CHUNK), lambda c: (0, c))
    per_head = pl.BlockSpec((None, heads, CHUNK, PAIR), lambda c: (c, 0, 0, 0))
    return pl.pallas_call(
        keys_kernel,
        grid=(steps,),
        in_specs=[rows, rows, rates, rates],
        out_specs=[
            pl.BlockSpec((None, pairs, PAIR, PAIR), lambda c: (c, 0, 0, 0)),
            pl.BlockSpec((pairs, PAIR, PAIR), lambda c: (0, 0, 0)),
            per_head,
            per_head,
            rows,
            rows,
        ],
        out_shape=[
            jax.ShapeDtypeStruct((steps, pairs, PAIR, PAIR), BF),
            jax.ShapeDtypeStruct((pairs, PAIR, PAIR), BF),
            jax.ShapeDtypeStruct((steps, heads, CHUNK, PAIR), BF),
            jax.ShapeDtypeStruct((steps, heads, CHUNK, CHUNK), BF),
            jax.ShapeDtypeStruct((length, width), BF),
            jax.ShapeDtypeStruct((length, width), F32),
        ],
        scratch_shapes=[
            pltpu.VMEM((pairs, PAIR, PAIR), BF),
            pltpu.VMEM((heads, CHUNK, CHUNK), BF),
            pltpu.VMEM((heads, CHUNK, CHUNK), BF),
            pltpu.VMEM((heads, CHUNK, PAIR), BF),
        ],
        name="keys_side",
    )(keys, values, beta_pre, decay_pre)


def queries_kernel(q_ref, kb_ref, d_ref, y_ref, before_ref, ec_ref, o_ref, q1_ref):
    row, col = places()
    left = col < HEAD_DIM
    same = left == (row < HEAD_DIM)
    ones = jnp.where(same, 1.0, 0.0).astype(BF)
    for p in range(q_ref.shape[1] // PAIR):
        lanes = slice(p * PAIR, (p + 1) * PAIR)
        query = silu(q_ref[:, lanes].astype(F32))
        query = query * lax.rsqrt(half_sums(query * query, ones) + EPSILON)
        query = (query * HEAD_DIM ** (-0.5)).astype(BF)
        query_f = query.astype(F32)
        key = kb_ref[:, lanes]
        got = []
        for s in range(2):
            h = 2 * p + s
            mine = left if s == 0 else jnp.logical_not(left)
            own = jnp.where(mine, query_f, 0.0).astype(BF)
            inside = (dot_nt(own, key) * d_ref[h].astype(F32)).astype(BF)
            got.append(dot(inside, y_ref[h]))
        local = jnp.where(left, got[0], got[1])
        crossed = turned(jnp.where(left, got[1], got[0]))
        query = (query_f * ec_ref[:, lanes] - crossed).astype(BF)
        before = before_ref[p].astype(F32)
        offset = jnp.where(same, before, 0.0).astype(BF)
        trans = jnp.where(same, turned(before), 0.0).astype(BF)
        o_ref[:, lanes] = local + dot(query, offset)
        q1_ref[:, lanes] = dot(query, trans).astype(BF)


def queries_side(queries, key_unit, decay, solved, before, grown):
    length, width = queries.shape
    heads = width // HEAD_DIM
    pairs = width // PAIR
    rows = pl.BlockSpec((CHUNK, width), lambda c: (c, 0))
    per_head = pl.BlockSpec((None, heads, CHUNK, PAIR), lambda c: (c, 0, 0, 0))
    return pl.pallas_call(
        queries_kernel,
        grid=(length // CHUNK,),
        in_specs=[
            rows,
            rows,
            per_head,
            per_head,
            pl.BlockSpec((None, pairs, PAIR, PAIR), lambda c: (c, 0, 0, 0)),
            rows,
        ],
        out_specs=[rows, rows],
        out_shape=[
            jax.ShapeDtypeStruct((length, width), F32),
            jax.ShapeDtypeStruct((length, width), BF),
        ],
        name="queries_side",
    )(queries, key_unit, decay, solved, before, grown)


def mixed_kernel(me_ref, o_ref, q1_ref, state_ref, gates_ref, gain_ref, w_ref, *rest):
    out_refs, mixed_ref = rest[:-1], rest[-1]
    row, col = places()
    same = (col < HEAD_DIM) == (row < HEAD_DIM)
    ones = jnp.where(same, 1.0, 0.0).astype(BF)
    length, width = o_ref.shape
    for c in range(length // CHUNK):
        rows = slice(c * CHUNK, (c + 1) * CHUNK)
        for p in range(width // PAIR):
            lanes = slice(p * PAIR, (p + 1) * PAIR)
            out = o_ref[rows, lanes] + dot(q1_ref[rows, lanes], state_ref[p])
            mean = half_sums(out * out, ones) * (1.0 / HEAD_DIM)
            out = out * lax.rsqrt(mean + EPSILON) * gain_ref[...]
            mixed_ref[rows, lanes] = (out * silu(gates_ref[rows, lanes].astype(F32))).astype(BF)
    size = len(out_refs)
    block = length // size
    for k, out_ref in enumerate(out_refs):
        start = lax.rem(me_ref[0] + k, size) * block
        rows = mixed_ref[pl.ds(pl.multiple_of(start, 32), block), :]
        out_ref[...] = dot(rows, w_ref[...]).astype(out_ref.dtype)


def mixed_and_projected(me, size, local, query, state, gates, gain, w_out):
    length, width = local.shape
    block = length // size
    full = pl.BlockSpec(memory_space=pltpu.VMEM)
    return pl.pallas_call(
        mixed_kernel,
        in_specs=[pl.BlockSpec(memory_space=pltpu.SMEM)] + [full] * 6,
        out_specs=[full] * size,
        out_shape=[
            jax.ShapeDtypeStruct((block, w_out.shape[1]), F32 if k == 0 else BF)
            for k in range(size)
        ],
        scratch_shapes=[pltpu.VMEM((length, width), BF)],
        name="mixed_and_projected",
    )(me, local, query, state, gates, jnp.tile(gain, 2).reshape(1, PAIR), w_out)


def norm_kernel(stream_ref, gain_ref, *rest):
    parts, middle_ref, normed_ref = rest[:-2], rest[-2], rest[-1]
    total = stream_ref[...].astype(F32)
    projected = parts[0][...].astype(F32)
    for part in parts[1:]:
        projected = projected + part[...].astype(F32)
    middle = (total + projected).astype(BF)
    middle_ref[...] = middle
    middle = middle.astype(F32)
    mean = jnp.mean(middle * middle, axis=-1, keepdims=True)
    normed_ref[...] = (middle * lax.rsqrt(mean + EPSILON) * gain_ref[...]).astype(BF)


def normed_rows(stream, gain, parts):
    full = pl.BlockSpec(memory_space=pltpu.VMEM)
    return pl.pallas_call(
        norm_kernel,
        in_specs=[full] * (2 + len(parts)),
        out_specs=[full] * 2,
        out_shape=[jax.ShapeDtypeStruct(stream.shape, BF)] * 2,
        name="normed_rows",
    )(stream, gain.reshape(1, -1), *parts)


def hidden_kernel(wg_ref, wu_ref, *rest):
    parts, out_ref, rows_ref = rest[:-2], rest[-2], rest[-1]
    block = parts[0].shape[0]

    @pl.when(pl.program_id(0) == 0)
    def _():
        for k, part in enumerate(parts):
            rows_ref[k * block : (k + 1) * block, :] = part[...]

    both = jnp.concatenate([wg_ref[...], wu_ref[...]], axis=1)
    got = dot(rows_ref[...], both)
    width = out_ref.shape[1]
    out_ref[...] = (silu(got[:, :width]) * got[:, width:]).astype(BF)


def hidden_units(weights, parts, hidden):
    tile = 128
    steps = hidden // tile
    block, width = parts[0].shape
    length = block * len(parts)
    rows = pl.BlockSpec((block, width), lambda j: (0, 0))
    return pl.pallas_call(
        hidden_kernel,
        grid=(steps,),
        in_specs=[
            pl.BlockSpec((width, tile), lambda j: (0, j)),
            pl.BlockSpec((width, tile), lambda j: (0, steps + j)),
        ]
        + [rows] * len(parts),
        out_specs=pl.BlockSpec((length, tile), lambda j: (0, j)),
        out_shape=jax.ShapeDtypeStruct((length, hidden), BF),
        scratch_shapes=[pltpu.VMEM((length, width), BF)],
        name="hidden_units",
    )(weights, weights, *parts)


def down_kernel(h_ref, w_ref, *out_refs):
    got = dot_nt(h_ref[...], w_ref[...])
    block = out_refs[0].shape[0]
    for k, out_ref in enumerate(out_refs):
        out_ref[...] = got[k * block : (k + 1) * block, :].astype(BF)


def down_products(hidden, weights, size):
    tile = 256
    length, units = hidden.shape
    width = weights.shape[0]
    block = length // size
    return pl.pallas_call(
        down_kernel,
        grid=(width // tile,),
        in_specs=[
            pl.BlockSpec((length, units), lambda n: (0, 0)),
            pl.BlockSpec((tile, units), lambda n: (n, 2)),
        ],
        out_specs=[pl.BlockSpec((block, tile), lambda n: (0, n))] * size,
        out_shape=[jax.ShapeDtypeStruct((block, width), BF)] * size,
        name="down_products",
    )(hidden, weights)


def last_kernel(middle_ref, *rest):
    parts, out_ref = rest[:-1], rest[-1]
    total = parts[0][...].astype(F32)
    for part in parts[1:]:
        total = total + part[...].astype(F32)
    out_ref[...] = (middle_ref[...].astype(F32) + 0.5 * total).astype(BF)


def last_sum(middle, parts):
    full = pl.BlockSpec(memory_space=pltpu.VMEM)
    return pl.pallas_call(
        last_kernel,
        in_specs=[full] * (1 + len(parts)),
        out_specs=full,
        out_shape=jax.ShapeDtypeStruct(middle.shape, BF),
        name="last_sum",
    )(middle, *parts)


def blocks_same():
    half = jnp.arange(PAIR) // HEAD_DIM
    return half[:, None] == half[None, :]


def chain(earlier, later):
    same = blocks_same()
    step = jnp.where(same, jnp.roll(later, HEAD_DIM, axis=-1), 0.0).astype(BF)
    moved = jnp.einsum("pij,pjk->pik", step, earlier.astype(BF), preferred_element_type=F32)
    return moved + jnp.where(same, later, 0.0).astype(F32)


def carried_in(total, axes):
    shift = (jnp.arange(PAIR)[:, None] ^ jnp.arange(PAIR)[None, :]) == HEAD_DIM
    start = jnp.broadcast_to(jnp.where(shift, 1.0, 0.0).astype(F32), total.shape)
    before = start
    subtotal = total
    for axis in reversed(axes):
        size, index = lax.axis_size(axis), lax.axis_index(axis)
        pieces = lax.all_gather(subtotal.astype(BF), axis)
        inside, subtotal = start, start
        for k in range(size):
            subtotal = chain(subtotal, pieces[k])
            inside = jnp.where(k + 1 == index, subtotal, inside)
        before = chain(inside, before)
    return jnp.where(blocks_same(), before, 0.0).astype(BF)


def ring(size, k):
    return [(i, (i + k) % size) for i in range(size)]


def per_device(
    queries,
    keys,
    values,
    gates,
    decay_pre,
    beta_pre,
    out_gain,
    w_out,
    stream,
    norm_gain,
    w_gate,
    w_up,
    w_down,
):
    hidden = w_gate.shape[1]
    weights = jnp.concatenate([w_gate, w_up, w_down.T], axis=1)
    weights = lax.all_gather(weights, SP, axis=0, tiled=True)
    size = lax.axis_size("tp")
    me = lax.axis_index("tp").astype(jnp.int32).reshape(1)
    before, total, solved, decay, key_unit, grown = keys_side(keys, values, beta_pre, decay_pre)
    local, query = queries_side(queries, key_unit, decay, solved, before, grown)
    state = carried_in(total, SP)
    parts = mixed_and_projected(me, size, local, query, state, gates, out_gain, w_out)
    got = [lax.ppermute(parts[k], "tp", ring(size, k)) for k in range(1, size)]
    middle, normed = normed_rows(stream, norm_gain, [parts[0]] + got)
    rows = [normed] + [lax.ppermute(normed, "tp", ring(size, k)) for k in range(1, size)]
    sums = down_products(hidden_units(weights, rows, hidden), weights, size)
    back = [lax.ppermute(sums[k], "tp", ring(size, -k)) for k in range(1, size)]
    return last_sum(middle, [sums[0]] + back)


def solution(mesh):
    finer = Mesh(mesh.devices.reshape(4, 4, 2, mesh.shape["tp"]), SP_TP)
    placed = (
        P(SP, "tp"),
        P(SP, "tp"),
        P(SP, "tp"),
        P(SP, "tp"),
        P("tp", SP),
        P("tp", SP),
        P(),
        P("tp", None),
        P(SP_TP, None),
        P(),
        P(SP, "tp"),
        P(SP, "tp"),
        P("tp", SP),
    )
    return jax.shard_map(
        per_device, mesh=finer, in_specs=placed, out_specs=P(SP_TP, None), check_vma=False
    )
```

```python
import jax
import jax.numpy as jnp
from jax import lax
from jax.experimental import pallas as pl
from jax.experimental.pallas import tpu as pltpu
from jax.sharding import Mesh
from jax.sharding import PartitionSpec as P

HEAD_DIM = 64
PAIR = 2 * HEAD_DIM
CHUNK = 128
SP = ("sp_0", "sp_1", "sp_2")
SP_TP = ("sp_0", "sp_1", "sp_2", "tp")
EPSILON = 1e-06
BF = jnp.bfloat16
F32 = jnp.float32
NT = (((1,), (1,)), ((), ()))


def ring(size, k):
    return [(i, (i + k) % size) for i in range(size)]


def dot(a, b):
    return jnp.dot(a, b, preferred_element_type=F32)


def dot_nt(a, b):
    return lax.dot_general(a, b, NT, preferred_element_type=F32)


def silu(x):
    return x / (1.0 + jnp.exp(-x))


def places():
    row = lax.broadcasted_iota(jnp.int32, (PAIR, PAIR), 0)
    col = lax.broadcasted_iota(jnp.int32, (PAIR, PAIR), 1)
    return row, col


def half_sums(squares, ones):
    high = squares.astype(BF)
    low = (squares - high.astype(F32)).astype(BF)
    return dot(high, ones) + dot(low, ones)


def softplus(x):
    small = jnp.exp(-jnp.abs(x))
    series = small * (1.0 - small * (0.5 - small * (1.0 / 3.0 - 0.25 * small)))
    return jnp.maximum(x, 0.0) + jnp.where(small < 0.015, series, jnp.log(1.0 + small))


def turned(z):
    return pltpu.roll(z, HEAD_DIM, 1)


def split_three(x):
    high = x.astype(BF)
    rest = x - high.astype(F32)
    middle = rest.astype(BF)
    return jnp.concatenate([high, middle], axis=1), (rest - middle.astype(F32)).astype(BF)


def side_by_side(pair):
    zero = jnp.zeros_like(pair[0])
    upper = jnp.concatenate([pair[0], zero], axis=1)
    lower = jnp.concatenate([zero, pair[1]], axis=1)
    return jnp.concatenate([upper, lower], axis=0)


def halves(x):
    return x[:, :CHUNK], x[:, CHUNK:]


def keys_kernel(
    k_ref, v_ref, beta_ref, decay_ref,
    before_ref, total_ref, y_ref, d_ref, kb_ref, ec_ref,
    l_ref, x_ref, r_ref, f_ref,
):
    row, col = places()
    left = col < HEAD_DIM
    top = row < HEAD_DIM
    same = left == top
    ones = jnp.where(same, 1.0, 0.0).astype(BF)
    inclusive = row >= col
    strict = row > col
    differ = row ^ col
    eye = jnp.where(row == col, 1.0, 0.0)
    off_eye = differ == HEAD_DIM
    length, width = k_ref.shape
    pairs = width // PAIR
    heads = 2 * pairs
    steps = length // CHUNK

    def stacked(x):
        return jnp.concatenate([x[:, c * CHUNK : (c + 1) * CHUNK] for c in range(steps)], axis=0)

    rates = split_three(stacked(-softplus(decay_ref[...])))
    strength = split_three(stacked(1.0 / (1.0 + jnp.exp(-beta_ref[...]))))
    triangle = jnp.where(inclusive, 1.0, 0.0).astype(BF)
    eye_bf = eye.astype(BF)
    triangle_two = jnp.concatenate([triangle, triangle], axis=1)
    cum_row = dot_nt(rates[0], triangle_two) + dot_nt(rates[1], triangle)
    cum_col = dot_nt(triangle_two, rates[0]) + dot_nt(triangle, rates[1])
    beta_col = dot_nt(jnp.concatenate([eye_bf, eye_bf], axis=1), strength[0])
    beta_col = beta_col + dot_nt(eye_bf, strength[1])

    ends = []
    for c in range(steps):
        rows = slice(c * CHUNK, (c + 1) * CHUNK)
        for p in range(pairs):
            lanes = slice(p * PAIR, (p + 1) * PAIR)
            item = c * pairs + p
            key = silu(k_ref[rows, lanes].astype(F32))
            key = (key * lax.rsqrt(half_sums(key * key, ones) + EPSILON)).astype(BF)
            kb_ref[rows, lanes] = key
            key_f = key.astype(F32)
            first = c * heads + 2 * p
            cums = [cum_col[:, h : h + 1] for h in (first, first + 1)]
            betas = [beta_col[:, h : h + 1] for h in (first, first + 1)]
            cum = jnp.where(left, cums[0], cums[1])
            beta = jnp.where(left, betas[0], betas[1])
            grown = jnp.exp(cum)
            ec_ref[rows, lanes] = grown
            strong = turned(key_f * (beta * grown))
            value = silu(v_ref[rows, lanes].astype(F32)) * beta
            r_ref[item, :, :CHUNK] = jnp.where(left, value, strong).astype(BF)
            r_ref[item, :, CHUNK:] = jnp.where(left, strong, value).astype(BF)
            fade = jnp.exp(cum[CHUNK - 1 : CHUNK, :] - cum)
            f_ref[item] = (key_f * fade).T.astype(BF)
            last = [jnp.exp(x[CHUNK - 1 : CHUNK, :]) for x in cums]
            ends.append(jnp.where(off_eye, jnp.where(top, last[0], last[1]), 0.0))
            owns = [jnp.where(left, key_f, 0.0), jnp.where(left, 0.0, key_f)]
            inner = dot_nt(key, jnp.concatenate(owns, axis=0).astype(BF))
            for s in range(2):
                part = slice(s * CHUNK, (s + 1) * CHUNK)
                gap = cums[s] - cum_row[first + s : first + s + 1, :]
                decay = jnp.where(inclusive, jnp.exp(gap), 0.0)
                d_ref[item, :, part] = decay.astype(BF)
                lower = jnp.where(strict, inner[:, part] * decay * betas[s], 0.0)
                l_ref[item, :, part] = lower.astype(BF)
                x_ref[item, :, part] = (eye - jnp.where(differ == 1, lower, 0.0)).astype(BF)

    items = steps * pairs

    def level(power, carry):
        mask = jnp.where((differ >> power) == 1, 1.0, 0.0).astype(BF)
        parts = []
        for i in range(items):
            block = side_by_side([part * mask for part in halves(l_ref[i])])
            parts.append(dot(x_ref[i], block).astype(BF))
        for i in range(items):
            x = x_ref[i]
            x_ref[i] = x - dot(parts[i], side_by_side(halves(x))).astype(BF)
        return carry

    lax.fori_loop(1, 7, level, 0)

    runs = [None] * pairs
    for c in range(steps):
        for p in range(pairs):
            item = c * pairs + p
            y = dot(x_ref[item], side_by_side(halves(r_ref[item]))).astype(BF)
            y_ref[item] = y
            z = jnp.where(top, *halves(dot(f_ref[item], y)))
            z = jnp.where(same, z, ends[item] - z)
            if c == 0:
                before_ref[c, p] = jnp.where(off_eye, 1.0, 0.0).astype(BF)
                runs[p] = z.astype(BF)
            else:
                before_ref[c, p] = runs[p]
                step = jnp.where(same, turned(z), 0.0).astype(BF)
                runs[p] = (dot(step, runs[p]) + jnp.where(same, z, 0.0)).astype(BF)
    for p in range(pairs):
        total_ref[p] = runs[p]


def keys_side(keys, values, beta_pre, decay_pre):
    length, width = keys.shape
    pairs = width // PAIR
    steps = length // CHUNK
    items = steps * pairs
    full = pl.BlockSpec(memory_space=pltpu.VMEM)
    return pl.pallas_call(
        keys_kernel,
        in_specs=[full] * 4,
        out_specs=[full] * 6,
        out_shape=[
            jax.ShapeDtypeStruct((steps, pairs, PAIR, PAIR), BF),
            jax.ShapeDtypeStruct((pairs, PAIR, PAIR), BF),
            jax.ShapeDtypeStruct((items, CHUNK, 2 * PAIR), BF),
            jax.ShapeDtypeStruct((items, CHUNK, 2 * CHUNK), BF),
            jax.ShapeDtypeStruct((length, width), BF),
            jax.ShapeDtypeStruct((length, width), F32),
        ],
        scratch_shapes=[
            pltpu.VMEM((items, CHUNK, 2 * CHUNK), BF),
            pltpu.VMEM((items, CHUNK, 2 * CHUNK), BF),
            pltpu.VMEM((items, CHUNK, 2 * PAIR), BF),
            pltpu.VMEM((items, PAIR, CHUNK), BF),
        ],
        name="keys_side",
    )(keys, values, beta_pre, decay_pre)


def queries_kernel(
    q_ref, kb_ref, d_ref, y_ref, before_ref, ec_ref, gates_ref, gain_ref, o_ref, q1_ref, gate_ref
):
    row, col = places()
    left = col < HEAD_DIM
    same = left == (row < HEAD_DIM)
    ones = jnp.where(same, 1.0, 0.0).astype(BF)
    gain = jnp.concatenate([gain_ref[...], gain_ref[...]], axis=1)
    for p in range(q_ref.shape[1] // PAIR):
        lanes = slice(p * PAIR, (p + 1) * PAIR)
        gate_ref[:, lanes] = silu(gates_ref[:, lanes].astype(F32)) * gain
        query = silu(q_ref[:, lanes].astype(F32))
        query = query * lax.rsqrt(half_sums(query * query, ones) + EPSILON)
        query = (query * HEAD_DIM ** (-0.5)).astype(BF)
        key_f = kb_ref[:, lanes].astype(F32)
        owns = [jnp.where(left, key_f, 0.0), jnp.where(left, 0.0, key_f)]
        inside = dot_nt(query, jnp.concatenate(owns, axis=0).astype(BF))
        inside = (inside * d_ref[p].astype(F32)).astype(BF)
        got = halves(dot(inside, side_by_side(halves(y_ref[p]))))
        local = jnp.where(left, got[0], got[1])
        crossed = turned(jnp.where(left, got[1], got[0]))
        query = (query.astype(F32) * ec_ref[:, lanes] - crossed).astype(BF)
        before = before_ref[p].astype(F32)
        both = [jnp.where(same, before, 0.0), jnp.where(same, turned(before), 0.0)]
        moved = halves(dot(query, jnp.concatenate(both, axis=1).astype(BF)))
        o_ref[:, lanes] = local + moved[0]
        q1_ref[:, lanes] = moved[1].astype(BF)


def queries_side(queries, key_unit, decay, solved, before, grown, gates, gain):
    length, width = queries.shape
    pairs = width // PAIR
    rows = pl.BlockSpec((CHUNK, width), lambda c: (c, 0))
    per_pair = pl.BlockSpec((pairs, CHUNK, 2 * PAIR), lambda c: (c, 0, 0))
    return pl.pallas_call(
        queries_kernel,
        grid=(length // CHUNK,),
        in_specs=[
            rows,
            rows,
            per_pair,
            per_pair,
            pl.BlockSpec((None, pairs, PAIR, PAIR), lambda c: (c, 0, 0, 0)),
            rows,
            rows,
            pl.BlockSpec((1, HEAD_DIM), lambda c: (0, 0)),
        ],
        out_specs=[rows] * 3,
        out_shape=[
            jax.ShapeDtypeStruct((length, width), F32),
            jax.ShapeDtypeStruct((length, width), BF),
            jax.ShapeDtypeStruct((length, width), F32),
        ],
        name="queries_side",
    )(queries, key_unit, decay, solved, before, grown, gates, gain.reshape(1, HEAD_DIM))


def chained(earlier, later, same):
    later = later.astype(F32)
    step = jnp.where(same, turned(later), 0.0).astype(BF)
    return dot(step, earlier.astype(BF)) + jnp.where(same, later, 0.0)


def chip_kernel(at_ref, own_ref, other_ref, out_ref):
    row, col = places()
    same = (col < HEAD_DIM) == (row < HEAD_DIM)
    core = at_ref[1]
    count = out_ref.shape[0]
    for p in range(count):
        mine = own_ref[core * count + p]
        theirs = other_ref[core * count + p]
        first = jnp.where(core == 0, mine, theirs)
        second = jnp.where(core == 0, theirs, mine)
        out_ref[p] = chained(first, second, same).astype(BF)


def row_kernel(at_ref, *rest):
    parts, (total_ref, before_ref, all_ref) = rest[:-3], rest[-3:]
    row, col = places()
    same = (col < HEAD_DIM) == (row < HEAD_DIM)
    place = at_ref[2]
    size = len(parts)
    for k, part in enumerate(parts):
        all_ref[lax.rem(place - k + size, size)] = part[...]
    for p in range(total_ref.shape[0]):
        run = all_ref[0, p].astype(F32)
        inside = jnp.where(place == 0, jnp.where((row ^ col) == HEAD_DIM, 1.0, 0.0), run)
        for k in range(1, size):
            run = chained(run, all_ref[k, p], same)
            inside = jnp.where(k < place, run, inside)
        before_ref[p] = inside.astype(BF)
        total_ref[p] = run.astype(BF)


def plane_kernel(at_ref, before_ref, *rest):
    parts, out_ref = rest[:-1], rest[-1]
    row, col = places()
    same = (col < HEAD_DIM) == (row < HEAD_DIM)
    place = at_ref[3]
    for p in range(out_ref.shape[0]):
        state = jnp.zeros((PAIR, PAIR), F32)
        for k in range(len(parts), 0, -1):
            later = jnp.where(same, chained(state, parts[k - 1][p], same), 0.0)
            state = jnp.where(k <= place, later, state)
        state = chained(state, before_ref[p], same)
        out_ref[p] = jnp.where(same, state, 0.0).astype(BF)


def small_call(kernel, name, at, arrays, shapes, scratch=()):
    full = pl.BlockSpec(memory_space=pltpu.VMEM)
    return pl.pallas_call(
        kernel,
        in_specs=[pl.BlockSpec(memory_space=pltpu.SMEM)] + [full] * len(arrays),
        out_specs=[full] * len(shapes),
        out_shape=[jax.ShapeDtypeStruct(shape, BF) for shape in shapes],
        scratch_shapes=[pltpu.VMEM(shape, BF) for shape in scratch],
        name=name,
    )(at, *arrays)


def state_ahead(at, total):
    plane, line, core = SP
    swap = [(0, 1), (1, 0)]
    half = (total.shape[0] // 2, PAIR, PAIR)
    other = lax.ppermute(total, core, swap)
    (chip,) = small_call(chip_kernel, "chip_total", at, [total, other], [half])
    size = lax.axis_size(line)
    lines = [chip] + [lax.ppermute(chip, line, ring(size, k)) for k in range(1, size)]
    whole, before = small_call(
        row_kernel, "line_total", at, lines, [half, half], [(size, *half)]
    )
    size = lax.axis_size(plane)
    planes = [lax.ppermute(whole, plane, ring(size, k)) for k in range(1, size)]
    (state,) = small_call(plane_kernel, "plane_state", at, [before] + planes, [half])
    return other, state, lax.ppermute(state, core, swap)


def mixed_kernel(
    at_ref, o_ref, q1_ref, first_ref, mine_ref, theirs_ref, gate_ref, w_ref, *rest
):
    out_refs, (mixed_ref, state_ref) = rest[:-2], rest[-2:]
    row, col = places()
    same = (col < HEAD_DIM) == (row < HEAD_DIM)
    ones = jnp.where(same, 1.0, 0.0).astype(BF)
    length, width = o_ref.shape
    core = at_ref[1]
    half = mine_ref.shape[0]
    state_ref[pl.ds(core * half, half)] = mine_ref[...]
    state_ref[pl.ds((1 - core) * half, half)] = theirs_ref[...]
    for p in range(width // PAIR):
        lanes = slice(p * PAIR, (p + 1) * PAIR)
        state = state_ref[p].astype(F32)
        later = jnp.where(same, chained(state, first_ref[p], same), 0.0)
        state = jnp.where(core == 0, state, later).astype(BF)
        out = o_ref[:, lanes] + dot(q1_ref[:, lanes], state)
        mean = half_sums(out * out, ones) * (1.0 / HEAD_DIM)
        out = out * lax.rsqrt(mean + EPSILON) * gate_ref[:, lanes]
        mixed_ref[:, lanes] = out.astype(BF)
    size = len(out_refs)
    block = length // size
    for k, out_ref in enumerate(out_refs):
        start = lax.rem(at_ref[0] + k, size) * block
        rows = mixed_ref[pl.ds(pl.multiple_of(start, 32), block), :]
        out_ref[...] = dot(rows, w_ref[...]).astype(out_ref.dtype)


def mixed_and_projected(at, size, local, query, states, gate, w_out):
    length, width = local.shape
    block = length // size
    full = pl.BlockSpec(memory_space=pltpu.VMEM)
    return pl.pallas_call(
        mixed_kernel,
        in_specs=[pl.BlockSpec(memory_space=pltpu.SMEM)] + [full] * 7,
        out_specs=[full] * size,
        out_shape=[
            jax.ShapeDtypeStruct((block, w_out.shape[1]), F32 if k == 0 else BF)
            for k in range(size)
        ],
        scratch_shapes=[
            pltpu.VMEM((length, width), BF),
            pltpu.VMEM((width // PAIR, PAIR, PAIR), BF),
        ],
        name="mixed_and_projected",
    )(at, local, query, *states, gate, w_out)


def norm_kernel(stream_ref, gain_ref, *rest):
    parts, middle_ref, normed_ref = rest[:-2], rest[-2], rest[-1]
    total = stream_ref[...].astype(F32)
    projected = parts[0][...].astype(F32)
    for part in parts[1:]:
        projected = projected + part[...].astype(F32)
    middle = (total + projected).astype(BF)
    middle_ref[...] = middle
    middle = middle.astype(F32)
    mean = jnp.mean(middle * middle, axis=-1, keepdims=True)
    normed_ref[...] = (middle * lax.rsqrt(mean + EPSILON) * gain_ref[...]).astype(BF)


def normed_rows(stream, gain, parts):
    full = pl.BlockSpec(memory_space=pltpu.VMEM)
    return pl.pallas_call(
        norm_kernel,
        in_specs=[full] * (2 + len(parts)),
        out_specs=[full] * 2,
        out_shape=[jax.ShapeDtypeStruct(stream.shape, BF)] * 2,
        name="normed_rows",
    )(stream, gain.reshape(1, -1), *parts)


def channels_kernel(w_ref, *rest):
    size = (len(rest) - 7) // 2
    parts, out_refs = rest[:size], rest[size : 2 * size]
    gate_ref, up_ref, down_ref, rows_ref, hidden_ref, in_sems, down_sems = rest[2 * size :]
    width, hidden = gate_ref.shape
    block = parts[0].shape[0]
    tile, strip = 128, 256
    tiles, strips = hidden // tile, width // strip
    copies, downs = [], []
    for j in range(tiles):
        here = pl.ds(j * tile, tile)
        for k, ref in enumerate((gate_ref, up_ref)):
            from_ref = w_ref.at[:, pl.ds(k * hidden + j * tile, tile)]
            copies.append(pltpu.make_async_copy(from_ref, ref.at[:, here], in_sems.at[k, j]))
    for n in range(strips):
        here = pl.ds(n * strip, strip)
        from_ref = w_ref.at[here, pl.ds(2 * hidden, hidden)]
        downs.append(pltpu.make_async_copy(from_ref, down_ref.at[here, :], down_sems.at[n]))
    for copy in copies + downs:
        copy.start()
    for k, part in enumerate(parts):
        rows_ref[k * block : (k + 1) * block, :] = part[...]
    for j in range(tiles):
        copies[2 * j].wait()
        copies[2 * j + 1].wait()
        here = slice(j * tile, (j + 1) * tile)
        both = jnp.concatenate([gate_ref[:, here], up_ref[:, here]], axis=1)
        got = dot(rows_ref[...], both)
        hidden_ref[:, here] = (silu(got[:, :tile]) * got[:, tile:]).astype(BF)
    for n in range(strips):
        downs[n].wait()
        here = slice(n * strip, (n + 1) * strip)
        got = dot_nt(hidden_ref[...], down_ref[here, :])
        for k, out_ref in enumerate(out_refs):
            out_ref[:, here] = got[k * block : (k + 1) * block, :].astype(BF)


def channel_sums(weights, parts, hidden):
    block, width = parts[0].shape
    size = len(parts)
    length = block * size
    full = pl.BlockSpec(memory_space=pltpu.VMEM)
    return pl.pallas_call(
        channels_kernel,
        in_specs=[pl.BlockSpec(memory_space=pl.ANY)] + [full] * size,
        out_specs=[full] * size,
        out_shape=[jax.ShapeDtypeStruct((block, width), BF)] * size,
        scratch_shapes=[
            pltpu.VMEM((width, hidden), BF),
            pltpu.VMEM((width, hidden), BF),
            pltpu.VMEM((width, hidden), BF),
            pltpu.VMEM((length, width), BF),
            pltpu.VMEM((length, hidden), BF),
            pltpu.SemaphoreType.DMA((2, hidden // 128)),
            pltpu.SemaphoreType.DMA((width // 256,)),
        ],
        name="channel_sums",
    )(weights, *parts)


def last_kernel(middle_ref, *rest):
    parts, out_ref = rest[:-1], rest[-1]
    total = parts[0][...].astype(F32)
    for part in parts[1:]:
        total = total + part[...].astype(F32)
    out_ref[...] = (middle_ref[...].astype(F32) + 0.5 * total).astype(BF)


def last_sum(middle, parts):
    full = pl.BlockSpec(memory_space=pltpu.VMEM)
    return pl.pallas_call(
        last_kernel,
        in_specs=[full] * (1 + len(parts)),
        out_specs=full,
        out_shape=jax.ShapeDtypeStruct(middle.shape, BF),
        name="last_sum",
    )(middle, *parts)


def per_device(
    queries,
    keys,
    values,
    gates,
    decay_pre,
    beta_pre,
    out_gain,
    w_out,
    stream,
    norm_gain,
    w_gate,
    w_up,
    w_down,
):
    hidden = w_gate.shape[1]
    weights = jnp.concatenate([w_gate, w_up, w_down.T], axis=1)
    weights = lax.all_gather(weights, SP, axis=0, tiled=True)
    size = lax.axis_size("tp")
    at = jnp.stack([lax.axis_index(a).astype(jnp.int32) for a in ("tp", *reversed(SP))])
    before, total, solved, decay, key_unit, grown = keys_side(keys, values, beta_pre, decay_pre)
    local, query, gate = queries_side(
        queries, key_unit, decay, solved, before, grown, gates, out_gain
    )
    states = state_ahead(at, total)
    parts = mixed_and_projected(at, size, local, query, states, gate, w_out)
    got = [lax.ppermute(parts[k], "tp", ring(size, k)) for k in range(1, size)]
    middle, normed = normed_rows(stream, norm_gain, [parts[0]] + got)
    rows = [normed] + [lax.ppermute(normed, "tp", ring(size, k)) for k in range(1, size)]
    sums = channel_sums(weights, rows, hidden)
    back = [lax.ppermute(sums[k], "tp", ring(size, -k)) for k in range(1, size)]
    return last_sum(middle, [sums[0]] + back)


def solution(mesh):
    finer = Mesh(mesh.devices.reshape(4, 4, 2, mesh.shape["tp"]), SP_TP)
    placed = (
        P(SP, "tp"),
        P(SP, "tp"),
        P(SP, "tp"),
        P(SP, "tp"),
        P("tp", SP),
        P("tp", SP),
        P(),
        P("tp", None),
        P(SP_TP, None),
        P(),
        P(SP, "tp"),
        P(SP, "tp"),
        P("tp", SP),
    )
    return jax.shard_map(
        per_device, mesh=finer, in_specs=placed, out_specs=P(SP_TP, None), check_vma=False
    )
```

```python
import jax
import jax.numpy as jnp
from jax import lax
from jax.experimental import pallas as pl
from jax.experimental.pallas import tpu as pltpu
from jax.sharding import Mesh
from jax.sharding import PartitionSpec as P

HEAD_DIM = 64
PAIR = 2 * HEAD_DIM
CHUNK = 128
SP = ("sp_0", "sp_1", "sp_2")
SP_TP = ("sp_0", "sp_1", "sp_2", "tp")
EPSILON = 1e-06
BF = jnp.bfloat16
F32 = jnp.float32
NT = (((1,), (1,)), ((), ()))


FULL = pl.BlockSpec(memory_space=pltpu.VMEM)
FAR = pl.BlockSpec(memory_space=pl.ANY)
TABLE = pl.BlockSpec(memory_space=pltpu.SMEM)


def call(kernel, name, arrays, shapes, scratch=(), table=None, far=(), mib=16):
    near = [pltpu.with_memory_space_constraint(x, pltpu.VMEM) for x in arrays]
    tables = [] if table is None else [table]
    return pl.pallas_call(
        kernel,
        in_specs=[TABLE] * len(tables) + [FAR] * len(far) + [FULL] * len(near),
        out_specs=[FULL] * len(shapes),
        out_shape=[pltpu.VMEM(shape, dtype) for shape, dtype in shapes],
        scratch_shapes=scratch,
        compiler_params=pltpu.CompilerParams(vmem_limit_bytes=mib << 20),
        name=name,
    )(*tables, *far, *near)


def ring(size, k):
    return [(i, (i + k) % size) for i in range(size)]


def dot(a, b):
    return jnp.dot(a, b, preferred_element_type=F32)


def dot_nt(a, b):
    return lax.dot_general(a, b, NT, preferred_element_type=F32)


def silu(x):
    return x / (1.0 + jnp.exp(-x))


def places():
    row = lax.broadcasted_iota(jnp.int32, (PAIR, PAIR), 0)
    col = lax.broadcasted_iota(jnp.int32, (PAIR, PAIR), 1)
    return row, col


def half_sums(squares, ones):
    high = squares.astype(BF)
    low = (squares - high.astype(F32)).astype(BF)
    return dot(high, ones) + dot(low, ones)


def softplus(x):
    small = jnp.exp(-jnp.abs(x))
    series = small * (1.0 - small * (0.5 - small * (1.0 / 3.0 - 0.25 * small)))
    return jnp.maximum(x, 0.0) + jnp.where(small < 0.015, series, jnp.log(1.0 + small))


def turned(z):
    return pltpu.roll(z, HEAD_DIM, 1)


def split_three(x):
    high = x.astype(BF)
    rest = x - high.astype(F32)
    middle = rest.astype(BF)
    return jnp.concatenate([high, middle], axis=1), (rest - middle.astype(F32)).astype(BF)


def side_by_side(pair):
    zero = jnp.zeros_like(pair[0])
    upper = jnp.concatenate([pair[0], zero], axis=1)
    lower = jnp.concatenate([zero, pair[1]], axis=1)
    return jnp.concatenate([upper, lower], axis=0)


def halves(x):
    return x[:, :CHUNK], x[:, CHUNK:]


def keys_kernel(
    k_ref, v_ref, beta_ref, decay_ref,
    before_ref, total_ref, y_ref, d_ref, kb_ref, ec_ref,
    l_ref, x_ref, r_ref, f_ref,
):
    row, col = places()
    left = col < HEAD_DIM
    top = row < HEAD_DIM
    same = left == top
    ones = jnp.where(same, 1.0, 0.0).astype(BF)
    inclusive = row >= col
    strict = row > col
    differ = row ^ col
    eye = jnp.where(row == col, 1.0, 0.0)
    off_eye = differ == HEAD_DIM
    length, width = k_ref.shape
    pairs = width // PAIR
    heads = 2 * pairs
    steps = length // CHUNK

    def stacked(x):
        return jnp.concatenate([x[:, c * CHUNK : (c + 1) * CHUNK] for c in range(steps)], axis=0)

    rates = split_three(stacked(-softplus(decay_ref[...])))
    strength = split_three(stacked(1.0 / (1.0 + jnp.exp(-beta_ref[...]))))
    triangle = jnp.where(inclusive, 1.0, 0.0).astype(BF)
    eye_bf = eye.astype(BF)
    triangle_two = jnp.concatenate([triangle, triangle], axis=1)
    cum_row = dot_nt(rates[0], triangle_two) + dot_nt(rates[1], triangle)
    cum_col = dot_nt(triangle_two, rates[0]) + dot_nt(triangle, rates[1])
    beta_col = dot_nt(jnp.concatenate([eye_bf, eye_bf], axis=1), strength[0])
    beta_col = beta_col + dot_nt(eye_bf, strength[1])

    ends = []
    for c in range(steps):
        rows = slice(c * CHUNK, (c + 1) * CHUNK)
        for p in range(pairs):
            lanes = slice(p * PAIR, (p + 1) * PAIR)
            item = c * pairs + p
            key = silu(k_ref[rows, lanes].astype(F32))
            key = (key * lax.rsqrt(half_sums(key * key, ones) + EPSILON)).astype(BF)
            kb_ref[rows, lanes] = key
            key_f = key.astype(F32)
            first = c * heads + 2 * p
            cums = [cum_col[:, h : h + 1] for h in (first, first + 1)]
            betas = [beta_col[:, h : h + 1] for h in (first, first + 1)]
            cum = jnp.where(left, cums[0], cums[1])
            beta = jnp.where(left, betas[0], betas[1])
            grown = jnp.exp(cum)
            ec_ref[rows, lanes] = grown
            strong = turned(key_f * (beta * grown))
            value = silu(v_ref[rows, lanes].astype(F32)) * beta
            r_ref[item, :, :CHUNK] = jnp.where(left, value, strong).astype(BF)
            r_ref[item, :, CHUNK:] = jnp.where(left, strong, value).astype(BF)
            fade = jnp.exp(cum[CHUNK - 1 : CHUNK, :] - cum)
            f_ref[item] = (key_f * fade).T.astype(BF)
            last = [jnp.exp(x[CHUNK - 1 : CHUNK, :]) for x in cums]
            ends.append(jnp.where(off_eye, jnp.where(top, last[0], last[1]), 0.0))
            owns = [jnp.where(left, key_f, 0.0), jnp.where(left, 0.0, key_f)]
            inner = dot_nt(key, jnp.concatenate(owns, axis=0).astype(BF))
            for s in range(2):
                part = slice(s * CHUNK, (s + 1) * CHUNK)
                gap = cums[s] - cum_row[first + s : first + s + 1, :]
                decay = jnp.where(inclusive, jnp.exp(gap), 0.0)
                d_ref[item, :, part] = decay.astype(BF)
                lower = jnp.where(strict, inner[:, part] * decay * betas[s], 0.0)
                l_ref[item, :, part] = lower.astype(BF)
                x_ref[item, :, part] = (eye - jnp.where(differ == 1, lower, 0.0)).astype(BF)

    items = steps * pairs

    def level(power, carry):
        mask = jnp.where((differ >> power) == 1, 1.0, 0.0).astype(BF)
        parts = []
        for i in range(items):
            block = side_by_side([part * mask for part in halves(l_ref[i])])
            parts.append(dot(x_ref[i], block).astype(BF))
        for i in range(items):
            x = x_ref[i]
            x_ref[i] = x - dot(parts[i], side_by_side(halves(x))).astype(BF)
        return carry

    lax.fori_loop(1, 7, level, 0)

    runs = [None] * pairs
    for c in range(steps):
        for p in range(pairs):
            item = c * pairs + p
            y = dot(x_ref[item], side_by_side(halves(r_ref[item]))).astype(BF)
            y_ref[item] = y
            z = jnp.where(top, *halves(dot(f_ref[item], y)))
            z = jnp.where(same, z, ends[item] - z)
            if c == 0:
                before_ref[item] = jnp.where(off_eye, 1.0, 0.0).astype(BF)
                runs[p] = z.astype(BF)
            else:
                before_ref[item] = runs[p]
                step = jnp.where(same, turned(z), 0.0).astype(BF)
                runs[p] = (dot(step, runs[p]) + jnp.where(same, z, 0.0)).astype(BF)
    for p in range(pairs):
        total_ref[p] = runs[p]


def keys_side(keys, values, beta_pre, decay_pre):
    length, width = keys.shape
    pairs = width // PAIR
    steps = length // CHUNK
    items = steps * pairs
    wide = pltpu.VMEM((items, CHUNK, 2 * CHUNK), BF)
    return call(
        keys_kernel,
        "keys_side",
        [keys, values, beta_pre, decay_pre],
        [
            ((items, PAIR, PAIR), BF),
            ((pairs, PAIR, PAIR), BF),
            ((items, CHUNK, 2 * PAIR), BF),
            ((items, CHUNK, 2 * CHUNK), BF),
            ((length, width), BF),
            ((length, width), F32),
        ],
        [wide, wide, wide, pltpu.VMEM((items, PAIR, CHUNK), BF)],
    )


def gates_kernel(gates_ref, gain_ref, gate_ref):
    gain = jnp.concatenate([gain_ref[...], gain_ref[...]], axis=1)
    for p in range(gates_ref.shape[1] // PAIR):
        lanes = slice(p * PAIR, (p + 1) * PAIR)
        gate_ref[:, lanes] = silu(gates_ref[:, lanes].astype(F32)) * gain


def queries_kernel(after_ref, q_ref, kb_ref, d_ref, y_ref, before_ref, ec_ref, o_ref, q1_ref):
    row, col = places()
    left = col < HEAD_DIM
    same = left == (row < HEAD_DIM)
    ones = jnp.where(same, 1.0, 0.0).astype(BF)
    length, width = q_ref.shape
    pairs = width // PAIR

    def chunk(c, carry):
        rows = pl.ds(pl.multiple_of(c * CHUNK, CHUNK), CHUNK)
        for p in range(pairs):
            lanes = slice(p * PAIR, (p + 1) * PAIR)
            item = c * pairs + p
            query = silu(q_ref[rows, lanes].astype(F32))
            query = query * lax.rsqrt(half_sums(query * query, ones) + EPSILON)
            query = (query * HEAD_DIM ** (-0.5)).astype(BF)
            key_f = kb_ref[rows, lanes].astype(F32)
            owns = [jnp.where(left, key_f, 0.0), jnp.where(left, 0.0, key_f)]
            inside = dot_nt(query, jnp.concatenate(owns, axis=0).astype(BF))
            inside = (inside * d_ref[item].astype(F32)).astype(BF)
            got = halves(dot(inside, side_by_side(halves(y_ref[item]))))
            local = jnp.where(left, got[0], got[1])
            crossed = turned(jnp.where(left, got[1], got[0]))
            query = (query.astype(F32) * ec_ref[rows, lanes] - crossed).astype(BF)
            before = before_ref[item].astype(F32)
            both = [jnp.where(same, before, 0.0), jnp.where(same, turned(before), 0.0)]
            moved = halves(dot(query, jnp.concatenate(both, axis=1).astype(BF)))
            o_ref[rows, lanes] = local + moved[0]
            q1_ref[rows, lanes] = moved[1].astype(BF)
        return carry

    lax.fori_loop(0, length // CHUNK, chunk, 0)


def gates_side(gates, gain):
    return call(
        gates_kernel, "gates_side", [gates, gain.reshape(1, HEAD_DIM)], [(gates.shape, F32)]
    )[0]


def queries_side(after, queries, key_unit, decay, solved, before, grown):
    return call(
        queries_kernel,
        "queries_side",
        [queries, key_unit, decay, solved, before, grown],
        [(queries.shape, F32), (queries.shape, BF)],
        far=[after],
    )


def chained(earlier, later, same):
    later = later.astype(F32)
    step = jnp.where(same, turned(later), 0.0).astype(BF)
    return dot(step, earlier.astype(BF)) + jnp.where(same, later, 0.0)


def chip_kernel(at_ref, own_ref, other_ref, out_ref):
    row, col = places()
    same = (col < HEAD_DIM) == (row < HEAD_DIM)
    core = at_ref[1]
    count = out_ref.shape[0]
    for p in range(count):
        mine = own_ref[core * count + p]
        theirs = other_ref[core * count + p]
        first = jnp.where(core == 0, mine, theirs)
        second = jnp.where(core == 0, theirs, mine)
        out_ref[p] = chained(first, second, same).astype(BF)


def row_kernel(at_ref, after_ref, *rest):
    parts, (total_ref, before_ref, all_ref) = rest[:-3], rest[-3:]
    row, col = places()
    same = (col < HEAD_DIM) == (row < HEAD_DIM)
    place = at_ref[2]
    size = len(parts)
    for k, part in enumerate(parts):
        all_ref[lax.rem(place - k + size, size)] = part[...]
    for p in range(total_ref.shape[0]):
        run = all_ref[0, p].astype(F32)
        inside = jnp.where(place == 0, jnp.where((row ^ col) == HEAD_DIM, 1.0, 0.0), run)
        for k in range(1, size):
            run = chained(run, all_ref[k, p], same)
            inside = jnp.where(k < place, run, inside)
        before_ref[p] = inside.astype(BF)
        total_ref[p] = run.astype(BF)


def plane_kernel(at_ref, after_ref, before_ref, *rest):
    parts, out_ref = rest[:-1], rest[-1]
    row, col = places()
    same = (col < HEAD_DIM) == (row < HEAD_DIM)
    place = at_ref[3]
    for p in range(out_ref.shape[0]):
        state = jnp.zeros((PAIR, PAIR), F32)
        for k in range(len(parts), 0, -1):
            later = jnp.where(same, chained(state, parts[k - 1][p], same), 0.0)
            state = jnp.where(k <= place, later, state)
        state = chained(state, before_ref[p], same)
        out_ref[p] = jnp.where(same, state, 0.0).astype(BF)


def state_ahead(at, total, meanwhile, then):
    plane, line, core = SP
    swap = [(0, 1), (1, 0)]
    half = (total.shape[0] // 2, PAIR, PAIR)
    other = lax.ppermute(total, core, swap)
    (chip,) = call(chip_kernel, "chip_total", [total, other], [(half, BF)], table=at)
    size = lax.axis_size(line)
    lines = [chip] + [lax.ppermute(chip, line, ring(size, k)) for k in range(1, size)]
    local, query = meanwhile(chip)
    whole, before = call(
        row_kernel,
        "line_total",
        lines,
        [(half, BF), (half, BF)],
        [pltpu.VMEM((size, *half), BF)],
        table=at,
        far=[query],
    )
    size = lax.axis_size(plane)
    planes = [lax.ppermute(whole, plane, ring(size, k)) for k in range(1, size)]
    gate = then()
    (state,) = call(
        plane_kernel, "plane_state", [before] + planes, [(half, BF)], table=at, far=[gate]
    )
    return local, query, gate, (other, state, lax.ppermute(state, core, swap))


def mixed_kernel(
    at_ref, o_ref, q1_ref, first_ref, mine_ref, theirs_ref, gate_ref, w_ref, *rest
):
    out_refs, (mixed_ref, state_ref) = rest[:-2], rest[-2:]
    row, col = places()
    same = (col < HEAD_DIM) == (row < HEAD_DIM)
    ones = jnp.where(same, 1.0, 0.0).astype(BF)
    length, width = o_ref.shape
    core = at_ref[1]
    half = mine_ref.shape[0]
    state_ref[pl.ds(core * half, half)] = mine_ref[...]
    state_ref[pl.ds((1 - core) * half, half)] = theirs_ref[...]
    for p in range(width // PAIR):
        lanes = slice(p * PAIR, (p + 1) * PAIR)
        state = state_ref[p].astype(F32)
        later = jnp.where(same, chained(state, first_ref[p], same), 0.0)
        state = jnp.where(core == 0, state, later).astype(BF)
        out = o_ref[:, lanes] + dot(q1_ref[:, lanes], state)
        mean = half_sums(out * out, ones) * (1.0 / HEAD_DIM)
        out = out * lax.rsqrt(mean + EPSILON) * gate_ref[:, lanes]
        mixed_ref[:, lanes] = out.astype(BF)
    size = len(out_refs)
    block = length // size
    for k, out_ref in enumerate(out_refs):
        start = lax.rem(at_ref[0] + k, size) * block
        rows = mixed_ref[pl.ds(pl.multiple_of(start, 32), block), :]
        out_ref[...] = dot(rows, w_ref[...]).astype(out_ref.dtype)


def mixed_and_projected(at, size, local, query, states, gate, w_out):
    length, width = local.shape
    block = (length // size, w_out.shape[1])
    return call(
        mixed_kernel,
        "mixed_and_projected",
        [local, query, *states, gate, w_out],
        [(block, F32 if k == 0 else BF) for k in range(size)],
        [pltpu.VMEM((length, width), BF), pltpu.VMEM((width // PAIR, PAIR, PAIR), BF)],
        table=at,
    )


def norm_kernel(stream_ref, gain_ref, *rest):
    parts, middle_ref, normed_ref = rest[:-2], rest[-2], rest[-1]
    total = stream_ref[...].astype(F32)
    projected = parts[0][...].astype(F32)
    for part in parts[1:]:
        projected = projected + part[...].astype(F32)
    middle = (total + projected).astype(BF)
    middle_ref[...] = middle
    middle = middle.astype(F32)
    mean = jnp.mean(middle * middle, axis=-1, keepdims=True)
    normed_ref[...] = (middle * lax.rsqrt(mean + EPSILON) * gain_ref[...]).astype(BF)


def normed_rows(stream, gain, parts):
    return call(
        norm_kernel,
        "normed_rows",
        [stream, gain.reshape(1, -1), *parts],
        [(stream.shape, BF), (stream.shape, BF)],
    )


def channels_kernel(w_ref, *rest):
    size = (len(rest) - 7) // 2
    parts, out_refs = rest[:size], rest[size : 2 * size]
    gate_ref, up_ref, down_ref, rows_ref, hidden_ref, in_sems, down_sems = rest[2 * size :]
    width, hidden = gate_ref.shape
    block = parts[0].shape[0]
    tile, strip = 128, 256
    tiles, strips = hidden // tile, width // strip
    even = hidden // strip * strip
    copies, downs = [], []
    for j in range(tiles):
        here = pl.ds(j * tile, tile)
        for k, ref in enumerate((gate_ref, up_ref)):
            from_ref = w_ref.at[:, pl.ds(k * hidden + j * tile, tile)]
            copies.append(pltpu.make_async_copy(from_ref, ref.at[:, here], in_sems.at[k, j]))
    for n in range(strips):
        here = pl.ds(n * strip, strip)
        from_ref = w_ref.at[here, pl.ds(2 * hidden, hidden)]
        downs.append(pltpu.make_async_copy(from_ref, down_ref.at[here, :], down_sems.at[n]))
    for copy in copies + downs:
        copy.start()
    for k, part in enumerate(parts):
        rows_ref[k * block : (k + 1) * block, :] = part[...]
    for j in range(tiles):
        copies[2 * j].wait()
        copies[2 * j + 1].wait()
        here = slice(j * tile, (j + 1) * tile)
        both = jnp.concatenate([gate_ref[:, here], up_ref[:, here]], axis=1)
        got = dot(rows_ref[...], both)
        hidden_ref[:, here] = (silu(got[:, :tile]) * got[:, tile:]).astype(BF)
    for n in range(strips):
        downs[n].wait()
        here = slice(n * strip, (n + 1) * strip)
        got = dot_nt(hidden_ref[:, :even], down_ref[here, :even])
        got = got + dot_nt(hidden_ref[:, even:], down_ref[here, even:])
        for k, out_ref in enumerate(out_refs):
            out_ref[:, here] = got[k * block : (k + 1) * block, :].astype(BF)


def channel_sums(weights, parts, hidden):
    block, width = parts[0].shape
    size = len(parts)
    weight = pltpu.VMEM((width, hidden), BF)
    return call(
        channels_kernel,
        "channel_sums",
        parts,
        [((block, width), BF)] * size,
        [
            weight,
            weight,
            weight,
            pltpu.VMEM((block * size, width), BF),
            pltpu.VMEM((block * size, hidden), BF),
            pltpu.SemaphoreType.DMA((2, hidden // 128)),
            pltpu.SemaphoreType.DMA((width // 256,)),
        ],
        far=[weights],
        mib=32,
    )


def last_kernel(middle_ref, *rest):
    parts, out_ref = rest[:-1], rest[-1]
    total = parts[0][...].astype(F32)
    for part in parts[1:]:
        total = total + part[...].astype(F32)
    out_ref[...] = (middle_ref[...].astype(F32) + 0.5 * total).astype(BF)


def last_sum(middle, parts):
    near = [pltpu.with_memory_space_constraint(x, pltpu.VMEM) for x in [middle, *parts]]
    return pl.pallas_call(
        last_kernel,
        in_specs=[FULL] * len(near),
        out_specs=FULL,
        out_shape=jax.ShapeDtypeStruct(middle.shape, BF),
        compiler_params=pltpu.CompilerParams(vmem_limit_bytes=16 << 20),
        name="last_sum",
    )(*near)


def per_device(
    queries,
    keys,
    values,
    gates,
    decay_pre,
    beta_pre,
    out_gain,
    w_out,
    stream,
    norm_gain,
    w_gate,
    w_up,
    w_down,
):
    hidden = w_gate.shape[1]
    weights = jnp.concatenate([w_gate, w_up, w_down.T], axis=1)
    weights = lax.all_gather(weights, SP, axis=0, tiled=True)
    size = lax.axis_size("tp")
    at = jnp.stack([lax.axis_index(a).astype(jnp.int32) for a in ("tp", *reversed(SP))])
    before, total, solved, decay, key_unit, grown = keys_side(keys, values, beta_pre, decay_pre)
    local, query, gate, states = state_ahead(
        at,
        total,
        lambda chip: queries_side(chip, queries, key_unit, decay, solved, before, grown),
        lambda: gates_side(gates, out_gain),
    )
    parts = mixed_and_projected(at, size, local, query, states, gate, w_out)
    got = [lax.ppermute(parts[k], "tp", ring(size, k)) for k in range(1, size)]
    middle, normed = normed_rows(stream, norm_gain, [parts[0]] + got)
    rows = [normed] + [lax.ppermute(normed, "tp", ring(size, k)) for k in range(1, size)]
    sums = channel_sums(weights, rows, hidden)
    back = [lax.ppermute(sums[k], "tp", ring(size, -k)) for k in range(1, size)]
    return last_sum(middle, [sums[0]] + back)


def solution(mesh):
    finer = Mesh(mesh.devices.reshape(4, 4, 2, mesh.shape["tp"]), SP_TP)
    placed = (
        P(SP, "tp"),
        P(SP, "tp"),
        P(SP, "tp"),
        P(SP, "tp"),
        P("tp", SP),
        P("tp", SP),
        P(),
        P("tp", None),
        P(SP_TP, None),
        P(),
        P(SP, "tp"),
        P(SP, "tp"),
        P("tp", SP),
    )
    return jax.shard_map(
        per_device, mesh=finer, in_specs=placed, out_specs=P(SP_TP, None), check_vma=False
    )
```

```python
import functools

import jax
import jax.numpy as jnp
from jax import lax
from jax.experimental import pallas as pl
from jax.experimental.pallas import tpu as pltpu
from jax.sharding import Mesh
from jax.sharding import PartitionSpec as P

HEAD_DIM = 64
PAIR = 2 * HEAD_DIM
CHUNK = 128
SP = ("sp_0", "sp_1", "sp_2")
SP_TP = ("sp_0", "sp_1", "sp_2", "tp")
EPSILON = 1e-06
BF = jnp.bfloat16
F32 = jnp.float32
NT = (((1,), (1,)), ((), ()))


FULL = pl.BlockSpec(memory_space=pltpu.VMEM)
FAR = pl.BlockSpec(memory_space=pl.ANY)
TABLE = pl.BlockSpec(memory_space=pltpu.SMEM)


def call(kernel, name, arrays, shapes, scratch=(), table=None, far=(), mib=16, pinned=True):
    near = [pltpu.with_memory_space_constraint(x, pltpu.VMEM) if pinned else x for x in arrays]
    tables = [] if table is None else [table]
    return pl.pallas_call(
        kernel,
        in_specs=[TABLE] * len(tables) + [FAR] * len(far) + [FULL] * len(near),
        out_specs=[FULL] * len(shapes),
        out_shape=[pltpu.VMEM(shape, dtype) for shape, dtype in shapes],
        scratch_shapes=scratch,
        compiler_params=pltpu.CompilerParams(vmem_limit_bytes=mib << 20),
        name=name,
    )(*tables, *far, *near)


def ring(size, k):
    return [(i, (i + k) % size) for i in range(size)]


def dot(a, b):
    return jnp.dot(a, b, preferred_element_type=F32)


def dot_nt(a, b):
    return lax.dot_general(a, b, NT, preferred_element_type=F32)


def silu(x):
    return x / (1.0 + jnp.exp(-x))


def places():
    row = lax.broadcasted_iota(jnp.int32, (PAIR, PAIR), 0)
    col = lax.broadcasted_iota(jnp.int32, (PAIR, PAIR), 1)
    return row, col


def half_sums(squares, ones):
    high = squares.astype(BF)
    low = (squares - high.astype(F32)).astype(BF)
    return dot(high, ones) + dot(low, ones)


def softplus(x):
    small = jnp.exp(-jnp.abs(x))
    series = small * (1.0 - small * (0.5 - small * (1.0 / 3.0 - 0.25 * small)))
    return jnp.maximum(x, 0.0) + jnp.where(small < 0.015, series, jnp.log(1.0 + small))


def turned(z):
    return pltpu.roll(z, HEAD_DIM, 1)


def split_three(x):
    high = x.astype(BF)
    rest = x - high.astype(F32)
    middle = rest.astype(BF)
    return jnp.concatenate([high, middle], axis=1), (rest - middle.astype(F32)).astype(BF)


def side_by_side(pair):
    zero = jnp.zeros_like(pair[0])
    upper = jnp.concatenate([pair[0], zero], axis=1)
    lower = jnp.concatenate([zero, pair[1]], axis=1)
    return jnp.concatenate([upper, lower], axis=0)


def halves(x):
    return x[:, :CHUNK], x[:, CHUNK:]


def keys_kernel(
    k_ref, v_ref, beta_ref, decay_ref,
    before_ref, total_ref, y_ref, d_ref, ec_ref,
    l_ref, x_ref, r_ref, f_ref,
):
    row, col = places()
    left = col < HEAD_DIM
    top = row < HEAD_DIM
    same = left == top
    ones = jnp.where(same, 1.0, 0.0).astype(BF)
    inclusive = row >= col
    strict = row > col
    differ = row ^ col
    eye = jnp.where(row == col, 1.0, 0.0)
    off_eye = differ == HEAD_DIM
    length, width = k_ref.shape
    pairs = width // PAIR
    heads = 2 * pairs
    steps = length // CHUNK

    def stacked(x):
        return jnp.concatenate([x[:, c * CHUNK : (c + 1) * CHUNK] for c in range(steps)], axis=0)

    rates = split_three(stacked(-softplus(decay_ref[...])))
    strength = split_three(stacked(1.0 / (1.0 + jnp.exp(-beta_ref[...]))))
    triangle = jnp.where(inclusive, 1.0, 0.0).astype(BF)
    eye_bf = eye.astype(BF)
    triangle_two = jnp.concatenate([triangle, triangle], axis=1)
    cum_row = dot_nt(rates[0], triangle_two) + dot_nt(rates[1], triangle)
    cum_col = dot_nt(triangle_two, rates[0]) + dot_nt(triangle, rates[1])
    beta_col = dot_nt(jnp.concatenate([eye_bf, eye_bf], axis=1), strength[0])
    beta_col = beta_col + dot_nt(eye_bf, strength[1])

    ends = []
    for c in range(steps):
        rows = slice(c * CHUNK, (c + 1) * CHUNK)
        for p in range(pairs):
            lanes = slice(p * PAIR, (p + 1) * PAIR)
            item = c * pairs + p
            key = silu(k_ref[rows, lanes].astype(F32))
            key = (key * lax.rsqrt(half_sums(key * key, ones) + EPSILON)).astype(BF)
            y_ref[item, :, 2 * PAIR :] = key
            key_f = key.astype(F32)
            first = c * heads + 2 * p
            cums = [cum_col[:, h : h + 1] for h in (first, first + 1)]
            betas = [beta_col[:, h : h + 1] for h in (first, first + 1)]
            cum = jnp.where(left, cums[0], cums[1])
            beta = jnp.where(left, betas[0], betas[1])
            grown = jnp.exp(cum)
            ec_ref[rows, lanes] = grown
            strong = turned(key_f * (beta * grown))
            value = silu(v_ref[rows, lanes].astype(F32)) * beta
            r_ref[item, :, :CHUNK] = jnp.where(left, value, strong).astype(BF)
            r_ref[item, :, CHUNK:] = jnp.where(left, strong, value).astype(BF)
            fade = jnp.exp(cum[CHUNK - 1 : CHUNK, :] - cum)
            f_ref[item] = (key_f * fade).T.astype(BF)
            last = [jnp.exp(x[CHUNK - 1 : CHUNK, :]) for x in cums]
            ends.append(jnp.where(off_eye, jnp.where(top, last[0], last[1]), 0.0))
            owns = [jnp.where(left, key_f, 0.0), jnp.where(left, 0.0, key_f)]
            inner = dot_nt(key, jnp.concatenate(owns, axis=0).astype(BF))
            for s in range(2):
                part = slice(s * CHUNK, (s + 1) * CHUNK)
                gap = cums[s] - cum_row[first + s : first + s + 1, :]
                decay = jnp.where(inclusive, jnp.exp(gap), 0.0)
                d_ref[item, :, part] = decay.astype(BF)
                lower = jnp.where(strict, inner[:, part] * decay * betas[s], 0.0)
                l_ref[item, :, part] = lower.astype(BF)
                x_ref[item, :, part] = (eye - jnp.where(differ == 1, lower, 0.0)).astype(BF)

    items = steps * pairs

    def level(power, carry):
        mask = jnp.where((differ >> power) == 1, 1.0, 0.0).astype(BF)
        parts = []
        for i in range(items):
            block = side_by_side([part * mask for part in halves(l_ref[i])])
            parts.append(dot(x_ref[i], block).astype(BF))
        for i in range(items):
            x = x_ref[i]
            x_ref[i] = x - dot(parts[i], side_by_side(halves(x))).astype(BF)
        return carry

    lax.fori_loop(1, 7, level, 0)

    runs = [None] * pairs
    for c in range(steps):
        for p in range(pairs):
            item = c * pairs + p
            y = dot(x_ref[item], side_by_side(halves(r_ref[item]))).astype(BF)
            y_ref[item, :, : 2 * PAIR] = y
            z = jnp.where(top, *halves(dot(f_ref[item], y)))
            z = jnp.where(same, z, ends[item] - z)
            if c == 0:
                before_ref[item] = jnp.where(off_eye, 1.0, 0.0).astype(BF)
                runs[p] = z.astype(BF)
            else:
                before_ref[item] = runs[p]
                step = jnp.where(same, turned(z), 0.0).astype(BF)
                runs[p] = (dot(step, runs[p]) + jnp.where(same, z, 0.0)).astype(BF)
    for p in range(pairs):
        total_ref[p] = runs[p]


def keys_side(keys, values, beta_pre, decay_pre):
    length, width = keys.shape
    pairs = width // PAIR
    steps = length // CHUNK
    items = steps * pairs
    wide = pltpu.VMEM((items, CHUNK, 2 * CHUNK), BF)
    return call(
        keys_kernel,
        "keys_side",
        [keys, values, beta_pre, decay_pre],
        [
            ((items, PAIR, PAIR), BF),
            ((pairs, PAIR, PAIR), BF),
            ((items, CHUNK, 3 * PAIR), BF),
            ((items, CHUNK, 2 * CHUNK), BF),
            ((length, width), F32),
        ],
        [wide, wide, wide, pltpu.VMEM((items, PAIR, CHUNK), BF)],
        pinned=False,
    )


def gates_kernel(gates_ref, gain_ref, gate_ref):
    gain = jnp.concatenate([gain_ref[...], gain_ref[...]], axis=1)
    for p in range(gates_ref.shape[1] // PAIR):
        lanes = slice(p * PAIR, (p + 1) * PAIR)
        gate_ref[:, lanes] = silu(gates_ref[:, lanes].astype(F32)) * gain


def queries_kernel(first, after_ref, q_ref, d_ref, y_ref, before_ref, ec_ref, o_ref, q1_ref):
    row, col = places()
    left = col < HEAD_DIM
    same = left == (row < HEAD_DIM)
    ones = jnp.where(same, 1.0, 0.0).astype(BF)
    length, width = o_ref.shape
    pairs = q_ref.shape[1] // PAIR

    def chunk(c, carry):
        rows = pl.ds(pl.multiple_of(c * CHUNK, CHUNK), CHUNK)
        for p in range(first, first + width // PAIR):
            lanes = slice(p * PAIR, (p + 1) * PAIR)
            place = slice((p - first) * PAIR, (p - first + 1) * PAIR)
            item = c * pairs + p
            query = silu(q_ref[rows, lanes].astype(F32))
            query = query * lax.rsqrt(half_sums(query * query, ones) + EPSILON)
            query = (query * HEAD_DIM ** (-0.5)).astype(BF)
            key_f = y_ref[item, :, 2 * PAIR :].astype(F32)
            owns = [jnp.where(left, key_f, 0.0), jnp.where(left, 0.0, key_f)]
            inside = dot_nt(query, jnp.concatenate(owns, axis=0).astype(BF))
            inside = (inside * d_ref[item].astype(F32)).astype(BF)
            got = halves(dot(inside, side_by_side(halves(y_ref[item, :, : 2 * PAIR]))))
            local = jnp.where(left, got[0], got[1])
            crossed = turned(jnp.where(left, got[1], got[0]))
            query = (query.astype(F32) * ec_ref[rows, lanes] - crossed).astype(BF)
            before = before_ref[item].astype(F32)
            both = [jnp.where(same, before, 0.0), jnp.where(same, turned(before), 0.0)]
            moved = halves(dot(query, jnp.concatenate(both, axis=1).astype(BF)))
            o_ref[rows, place] = local + moved[0]
            q1_ref[rows, place] = moved[1].astype(BF)
        return carry

    lax.fori_loop(0, length // CHUNK, chunk, 0)


def gates_side(gates, gain):
    return call(
        gates_kernel, "gates_side", [gates, gain.reshape(1, HEAD_DIM)], [(gates.shape, F32)]
    )[0]


def queries_side(first, after, queries, decay, solved, before, grown):
    length, width = queries.shape
    shape = (length, width // 2)
    return call(
        functools.partial(queries_kernel, first),
        "queries_side",
        [queries, decay, solved, before, grown],
        [(shape, F32), (shape, BF)],
        far=[after],
    )


def chained(earlier, later, same):
    later = later.astype(F32)
    step = jnp.where(same, turned(later), 0.0).astype(BF)
    return dot(step, earlier.astype(BF)) + jnp.where(same, later, 0.0)


def chip_kernel(at_ref, own_ref, other_ref, out_ref):
    row, col = places()
    same = (col < HEAD_DIM) == (row < HEAD_DIM)
    core = at_ref[1]
    count = out_ref.shape[0]
    for p in range(count):
        mine = own_ref[core * count + p]
        theirs = other_ref[core * count + p]
        first = jnp.where(core == 0, mine, theirs)
        second = jnp.where(core == 0, theirs, mine)
        out_ref[p] = chained(first, second, same).astype(BF)


def row_kernel(at_ref, after_ref, *rest):
    parts, (total_ref, before_ref, all_ref) = rest[:-3], rest[-3:]
    row, col = places()
    same = (col < HEAD_DIM) == (row < HEAD_DIM)
    place = at_ref[2]
    size = len(parts)
    for k, part in enumerate(parts):
        all_ref[lax.rem(place - k + size, size)] = part[...]
    for p in range(total_ref.shape[0]):
        run = all_ref[0, p].astype(F32)
        inside = jnp.where(place == 0, jnp.where((row ^ col) == HEAD_DIM, 1.0, 0.0), run)
        for k in range(1, size):
            run = chained(run, all_ref[k, p], same)
            inside = jnp.where(k < place, run, inside)
        before_ref[p] = inside.astype(BF)
        total_ref[p] = run.astype(BF)


def plane_kernel(at_ref, after_ref, before_ref, *rest):
    parts, out_ref = rest[:-1], rest[-1]
    row, col = places()
    same = (col < HEAD_DIM) == (row < HEAD_DIM)
    place = at_ref[3]
    for p in range(out_ref.shape[0]):
        state = jnp.zeros((PAIR, PAIR), F32)
        for k in range(len(parts), 0, -1):
            later = jnp.where(same, chained(state, parts[k - 1][p], same), 0.0)
            state = jnp.where(k <= place, later, state)
        state = chained(state, before_ref[p], same)
        out_ref[p] = jnp.where(same, state, 0.0).astype(BF)


def state_ahead(at, total, meanwhile, then):
    plane, line, core = SP
    swap = [(0, 1), (1, 0)]
    half = (total.shape[0] // 2, PAIR, PAIR)
    other = lax.ppermute(total, core, swap)
    (chip,) = call(chip_kernel, "chip_total", [total, other], [(half, BF)], table=at)
    size = lax.axis_size(line)
    lines = [chip] + [lax.ppermute(chip, line, ring(size, k)) for k in range(1, size)]
    early = meanwhile(chip)
    whole, before = call(
        row_kernel,
        "line_total",
        lines,
        [(half, BF), (half, BF)],
        [pltpu.VMEM((size, *half), BF)],
        table=at,
        far=[early[1]],
    )
    size = lax.axis_size(plane)
    planes = [lax.ppermute(whole, plane, ring(size, k)) for k in range(1, size)]
    late = then(whole)
    (state,) = call(
        plane_kernel, "plane_state", [before] + planes, [(half, BF)], table=at, far=[late[1]]
    )
    return early, late, (other, state, lax.ppermute(state, core, swap))


def mixed_kernel(
    at_ref, o0_ref, q0_ref, o1_ref, q1_ref,
    first_ref, mine_ref, theirs_ref, gate_ref, w_ref, *rest,
):
    out_refs, (mixed_ref, state_ref) = rest[:-2], rest[-2:]
    row, col = places()
    same = (col < HEAD_DIM) == (row < HEAD_DIM)
    ones = jnp.where(same, 1.0, 0.0).astype(BF)
    length, width = gate_ref.shape
    core = at_ref[1]
    half = mine_ref.shape[0]
    state_ref[pl.ds(core * half, half)] = mine_ref[...]
    state_ref[pl.ds((1 - core) * half, half)] = theirs_ref[...]
    for p in range(width // PAIR):
        lanes = slice(p * PAIR, (p + 1) * PAIR)
        state = state_ref[p].astype(F32)
        later = jnp.where(same, chained(state, first_ref[p], same), 0.0)
        state = jnp.where(core == 0, state, later).astype(BF)
        o_ref, q_ref = ((o0_ref, q0_ref), (o1_ref, q1_ref))[p // half]
        place = slice((p % half) * PAIR, (p % half + 1) * PAIR)
        out = o_ref[:, place] + dot(q_ref[:, place], state)
        mean = half_sums(out * out, ones) * (1.0 / HEAD_DIM)
        out = out * lax.rsqrt(mean + EPSILON) * gate_ref[:, lanes]
        mixed_ref[:, lanes] = out.astype(BF)
    size = len(out_refs)
    block = length // size
    for k, out_ref in enumerate(out_refs):
        start = lax.rem(at_ref[0] + k, size) * block
        rows = mixed_ref[pl.ds(pl.multiple_of(start, 32), block), :]
        out_ref[...] = dot(rows, w_ref[...]).astype(out_ref.dtype)


def mixed_and_projected(at, size, early, late, states, gate, w_out):
    length, width = gate.shape
    block = (length // size, w_out.shape[1])
    return call(
        mixed_kernel,
        "mixed_and_projected",
        [*early, *late, *states, gate, w_out],
        [(block, F32 if k == 0 else BF) for k in range(size)],
        [pltpu.VMEM((length, width), BF), pltpu.VMEM((width // PAIR, PAIR, PAIR), BF)],
        table=at,
    )


def norm_kernel(stream_ref, gain_ref, *rest):
    parts, middle_ref, normed_ref = rest[:-2], rest[-2], rest[-1]
    total = stream_ref[...].astype(F32)
    projected = parts[0][...].astype(F32)
    for part in parts[1:]:
        projected = projected + part[...].astype(F32)
    middle = (total + projected).astype(BF)
    middle_ref[...] = middle
    middle = middle.astype(F32)
    mean = jnp.mean(middle * middle, axis=-1, keepdims=True)
    normed_ref[...] = (middle * lax.rsqrt(mean + EPSILON) * gain_ref[...]).astype(BF)


def normed_rows(stream, gain, parts):
    return call(
        norm_kernel,
        "normed_rows",
        [stream, gain.reshape(1, -1), *parts],
        [(stream.shape, BF), (stream.shape, BF)],
    )


def activated(rows, gate, up):
    got = dot(rows, jnp.concatenate([gate, up], axis=1))
    width = gate.shape[1]
    return (silu(got[:, :width]) * got[:, width:]).astype(BF)


def product_nt(a, b):
    even = a.shape[1] // 256 * 256
    return dot_nt(a[:, :even], b[:, :even]) + dot_nt(a[:, even:], b[:, even:])


TILE = 128
STRIP = 256


def first_channels_kernel(count, w_ref, *rest):
    parts, out_refs = rest[:count], rest[count : 2 * count]
    gate_ref, up_ref, down_ref, rows_ref, hidden_ref, in_sems, down_sems = rest[2 * count :]
    width, hidden = gate_ref.shape
    block = parts[0].shape[0]
    copies, downs = [], []
    for j in range(hidden // TILE):
        here = pl.ds(j * TILE, TILE)
        for k, ref in enumerate((gate_ref, up_ref)):
            from_ref = w_ref.at[:, pl.ds(k * hidden + j * TILE, TILE)]
            copies.append(pltpu.make_async_copy(from_ref, ref.at[:, here], in_sems.at[k, j]))
    for n in range(width // STRIP):
        here = pl.ds(n * STRIP, STRIP)
        from_ref = w_ref.at[here, pl.ds(2 * hidden, hidden)]
        downs.append(pltpu.make_async_copy(from_ref, down_ref.at[here, :], down_sems.at[n]))
    for copy in copies + downs:
        copy.start()
    for k, part in enumerate(parts):
        rows_ref[k * block : (k + 1) * block, :] = part[...]
    for j in range(hidden // TILE):
        copies[2 * j].wait()
        copies[2 * j + 1].wait()
        here = slice(j * TILE, (j + 1) * TILE)
        hidden_ref[:, here] = activated(rows_ref[...], gate_ref[:, here], up_ref[:, here])
    for n in range(width // STRIP):
        downs[n].wait()
        here = slice(n * STRIP, (n + 1) * STRIP)
        got = product_nt(hidden_ref[...], down_ref[here, :])
        for k, out_ref in enumerate(out_refs):
            out_ref[:, here] = got[k * block : (k + 1) * block, :].astype(BF)


def first_channels(weights, parts, hidden):
    block, width = parts[0].shape
    count = len(parts)
    out = call(
        functools.partial(first_channels_kernel, count),
        "first_channels",
        parts,
        [((block, width), BF)] * count + [((width, hidden), BF)] * 3,
        [
            pltpu.VMEM((block * count, width), BF),
            pltpu.VMEM((block * count, hidden), BF),
            pltpu.SemaphoreType.DMA((2, hidden // TILE)),
            pltpu.SemaphoreType.DMA((width // STRIP,)),
        ],
        far=[pltpu.with_memory_space_constraint(weights, pltpu.HBM)],
    )
    return out[:count], out[count:]


def more_channels_kernel(rows_ref, gate_ref, up_ref, down_ref, out_ref, hidden_ref):
    for j in range(gate_ref.shape[1] // TILE):
        here = slice(j * TILE, (j + 1) * TILE)
        hidden_ref[:, here] = activated(rows_ref[...], gate_ref[:, here], up_ref[:, here])
    for n in range(down_ref.shape[0] // STRIP):
        here = slice(n * STRIP, (n + 1) * STRIP)
        out_ref[:, here] = product_nt(hidden_ref[...], down_ref[here, :]).astype(BF)


def more_channels(rows, projections):
    return call(
        more_channels_kernel,
        "more_channels",
        [rows, *projections],
        [(rows.shape, BF)],
        [pltpu.VMEM((rows.shape[0], projections[0].shape[1]), BF)],
    )[0]


def last_kernel(middle_ref, *rest):
    parts, out_ref = rest[:-1], rest[-1]
    total = parts[0][...].astype(F32)
    for part in parts[1:]:
        total = total + part[...].astype(F32)
    out_ref[...] = (middle_ref[...].astype(F32) + 0.5 * total).astype(BF)


def last_sum(middle, parts):
    near = [pltpu.with_memory_space_constraint(x, pltpu.VMEM) for x in [middle, *parts]]
    return pl.pallas_call(
        last_kernel,
        in_specs=[FULL] * len(near),
        out_specs=FULL,
        out_shape=jax.ShapeDtypeStruct(middle.shape, BF),
        compiler_params=pltpu.CompilerParams(vmem_limit_bytes=16 << 20),
        name="last_sum",
    )(*near)


def per_device(
    queries,
    keys,
    values,
    gates,
    decay_pre,
    beta_pre,
    out_gain,
    w_out,
    stream,
    norm_gain,
    w_gate,
    w_up,
    w_down,
):
    hidden = w_gate.shape[1]
    weights = jnp.concatenate([w_gate, w_up, w_down.T], axis=1)
    weights = lax.all_gather(weights, SP, axis=0, tiled=True)
    size = lax.axis_size("tp")
    at = jnp.stack([lax.axis_index(a).astype(jnp.int32) for a in ("tp", *reversed(SP))])
    before, total, solved, decay, grown = keys_side(keys, values, beta_pre, decay_pre)
    gate = gates_side(gates, out_gain)
    pairs = queries.shape[1] // PAIR
    early, late, states = state_ahead(
        at,
        total,
        lambda x: queries_side(0, x, queries, decay, solved, before, grown),
        lambda x: queries_side(pairs // 2, x, queries, decay, solved, before, grown),
    )
    parts = mixed_and_projected(at, size, early, late, states, gate, w_out)
    got = [lax.ppermute(parts[k], "tp", ring(size, k)) for k in range(1, size)]
    middle, normed = normed_rows(stream, norm_gain, [parts[0]] + got)
    right = lax.ppermute(normed, "tp", ring(size, 1))
    left = lax.ppermute(normed, "tp", ring(size, -1))
    across = lax.ppermute(normed, "tp", ring(size, 2))
    sums, projections = first_channels(weights, [normed, right, left], hidden)
    back = [lax.ppermute(sums[1], "tp", ring(size, -1)), lax.ppermute(sums[2], "tp", ring(size, 1))]
    last = more_channels(across, projections)
    back.append(lax.ppermute(last, "tp", ring(size, 2)))
    return last_sum(middle, [sums[0]] + back)


def solution(mesh):
    finer = Mesh(mesh.devices.reshape(4, 4, 2, mesh.shape["tp"]), SP_TP)
    placed = (
        P(SP, "tp"),
        P(SP, "tp"),
        P(SP, "tp"),
        P(SP, "tp"),
        P("tp", SP),
        P("tp", SP),
        P(),
        P("tp", None),
        P(SP_TP, None),
        P(),
        P(SP, "tp"),
        P(SP, "tp"),
        P("tp", SP),
    )
    return jax.shard_map(
        per_device, mesh=finer, in_specs=placed, out_specs=P(SP_TP, None), check_vma=False
    )
```

```python
import functools

import jax
import jax.numpy as jnp
from jax import lax
from jax.experimental import pallas as pl
from jax.experimental.pallas import tpu as pltpu
from jax.sharding import Mesh
from jax.sharding import PartitionSpec as P

HEAD_DIM = 64
PAIR = 2 * HEAD_DIM
CHUNK = 128
SP = ("sp_0", "sp_1", "sp_2")
SP_TP = ("sp_0", "sp_1", "sp_2", "tp")
EPSILON = 1e-06
BF = jnp.bfloat16
F32 = jnp.float32
NT = (((1,), (1,)), ((), ()))


FULL = pl.BlockSpec(memory_space=pltpu.VMEM)
FAR = pl.BlockSpec(memory_space=pl.ANY)
TABLE = pl.BlockSpec(memory_space=pltpu.SMEM)


def call(kernel, name, arrays, shapes, scratch=(), table=None, far=(), mib=16):
    near = [pltpu.with_memory_space_constraint(x, pltpu.VMEM) for x in arrays]
    tables = [] if table is None else [table]
    return pl.pallas_call(
        kernel,
        in_specs=[TABLE] * len(tables) + [FAR] * len(far) + [FULL] * len(near),
        out_specs=[FULL] * len(shapes),
        out_shape=[pltpu.VMEM(shape, dtype) for shape, dtype in shapes],
        scratch_shapes=scratch,
        compiler_params=pltpu.CompilerParams(vmem_limit_bytes=mib << 20),
        name=name,
    )(*tables, *far, *near)


def ring(size, k):
    return [(i, (i + k) % size) for i in range(size)]


def dot(a, b):
    return jnp.dot(a, b, preferred_element_type=F32)


def dot_nt(a, b):
    return lax.dot_general(a, b, NT, preferred_element_type=F32)


def silu(x):
    return x / (1.0 + jnp.exp(-x))


def places():
    row = lax.broadcasted_iota(jnp.int32, (PAIR, PAIR), 0)
    col = lax.broadcasted_iota(jnp.int32, (PAIR, PAIR), 1)
    return row, col


def half_sums(squares, ones):
    high = squares.astype(BF)
    low = (squares - high.astype(F32)).astype(BF)
    return dot(high, ones) + dot(low, ones)


def softplus(x):
    small = jnp.exp(-jnp.abs(x))
    series = small * (1.0 - small * (0.5 - small * (1.0 / 3.0 - 0.25 * small)))
    return jnp.maximum(x, 0.0) + jnp.where(small < 0.015, series, jnp.log(1.0 + small))


def turned(z):
    return pltpu.roll(z, HEAD_DIM, 1)


def split_three(x):
    high = x.astype(BF)
    rest = x - high.astype(F32)
    middle = rest.astype(BF)
    return jnp.concatenate([high, middle], axis=1), (rest - middle.astype(F32)).astype(BF)


def side_by_side(pair):
    zero = jnp.zeros_like(pair[0])
    upper = jnp.concatenate([pair[0], zero], axis=1)
    lower = jnp.concatenate([zero, pair[1]], axis=1)
    return jnp.concatenate([upper, lower], axis=0)


def halves(x):
    return x[:, :CHUNK], x[:, CHUNK:]


def keys_kernel(
    k_far_ref, v_far_ref, beta_far_ref, decay_far_ref,
    before_ref, total_ref, y_ref, d_ref, ec_ref,
    l_ref, x_ref, r_ref, f_ref, k_ref, v_ref, beta_ref, decay_ref, sems,
):
    length, width = k_ref.shape
    rate_copies = [
        pltpu.make_async_copy(decay_far_ref, decay_ref, sems.at[0]),
        pltpu.make_async_copy(beta_far_ref, beta_ref, sems.at[1]),
    ]
    row_copies = []
    for c in range(length // CHUNK):
        rows = pl.ds(c * CHUNK, CHUNK)
        for k, (far_ref, ref) in enumerate(((k_far_ref, k_ref), (v_far_ref, v_ref))):
            sem = sems.at[2 + 2 * c + k]
            row_copies.append(pltpu.make_async_copy(far_ref.at[rows], ref.at[rows], sem))
    for copy in rate_copies + row_copies:
        copy.start()
    row, col = places()
    left = col < HEAD_DIM
    top = row < HEAD_DIM
    same = left == top
    ones = jnp.where(same, 1.0, 0.0).astype(BF)
    inclusive = row >= col
    strict = row > col
    differ = row ^ col
    eye = jnp.where(row == col, 1.0, 0.0)
    off_eye = differ == HEAD_DIM
    pairs = width // PAIR
    heads = 2 * pairs
    steps = length // CHUNK

    def stacked(x):
        return jnp.concatenate([x[:, c * CHUNK : (c + 1) * CHUNK] for c in range(steps)], axis=0)

    for copy in rate_copies:
        copy.wait()
    rates = split_three(stacked(-softplus(decay_ref[...])))
    strength = split_three(stacked(1.0 / (1.0 + jnp.exp(-beta_ref[...]))))
    triangle = jnp.where(inclusive, 1.0, 0.0).astype(BF)
    eye_bf = eye.astype(BF)
    triangle_two = jnp.concatenate([triangle, triangle], axis=1)
    cum_row = dot_nt(rates[0], triangle_two) + dot_nt(rates[1], triangle)
    cum_col = dot_nt(triangle_two, rates[0]) + dot_nt(triangle, rates[1])
    beta_col = dot_nt(jnp.concatenate([eye_bf, eye_bf], axis=1), strength[0])
    beta_col = beta_col + dot_nt(eye_bf, strength[1])

    ends = []
    for c in range(steps):
        rows = slice(c * CHUNK, (c + 1) * CHUNK)
        row_copies[2 * c].wait()
        row_copies[2 * c + 1].wait()
        for p in range(pairs):
            lanes = slice(p * PAIR, (p + 1) * PAIR)
            item = c * pairs + p
            key = silu(k_ref[rows, lanes].astype(F32))
            key = (key * lax.rsqrt(half_sums(key * key, ones) + EPSILON)).astype(BF)
            y_ref[item, :, 2 * PAIR :] = key
            key_f = key.astype(F32)
            first = c * heads + 2 * p
            cums = [cum_col[:, h : h + 1] for h in (first, first + 1)]
            betas = [beta_col[:, h : h + 1] for h in (first, first + 1)]
            cum = jnp.where(left, cums[0], cums[1])
            beta = jnp.where(left, betas[0], betas[1])
            grown = jnp.exp(cum)
            ec_ref[rows, lanes] = grown
            strong = turned(key_f * (beta * grown))
            value = silu(v_ref[rows, lanes].astype(F32)) * beta
            r_ref[item, :, :CHUNK] = jnp.where(left, value, strong).astype(BF)
            r_ref[item, :, CHUNK:] = jnp.where(left, strong, value).astype(BF)
            fade = jnp.exp(cum[CHUNK - 1 : CHUNK, :] - cum)
            f_ref[item] = (key_f * fade).T.astype(BF)
            last = [jnp.exp(x[CHUNK - 1 : CHUNK, :]) for x in cums]
            ends.append(jnp.where(off_eye, jnp.where(top, last[0], last[1]), 0.0))
            owns = [jnp.where(left, key_f, 0.0), jnp.where(left, 0.0, key_f)]
            inner = dot_nt(key, jnp.concatenate(owns, axis=0).astype(BF))
            for s in range(2):
                part = slice(s * CHUNK, (s + 1) * CHUNK)
                gap = cums[s] - cum_row[first + s : first + s + 1, :]
                decay = jnp.where(inclusive, jnp.exp(gap), 0.0)
                d_ref[item, :, part] = decay.astype(BF)
                lower = jnp.where(strict, inner[:, part] * decay * betas[s], 0.0)
                l_ref[item, :, part] = lower.astype(BF)
                x_ref[item, :, part] = (eye - jnp.where(differ == 1, lower, 0.0)).astype(BF)

    items = steps * pairs

    def level(power, carry):
        mask = jnp.where((differ >> power) == 1, 1.0, 0.0).astype(BF)
        parts = []
        for i in range(items):
            block = side_by_side([part * mask for part in halves(l_ref[i])])
            parts.append(dot(x_ref[i], block).astype(BF))
        for i in range(items):
            x = x_ref[i]
            x_ref[i] = x - dot(parts[i], side_by_side(halves(x))).astype(BF)
        return carry

    lax.fori_loop(1, 7, level, 0)

    runs = [None] * pairs
    for c in range(steps):
        for p in range(pairs):
            item = c * pairs + p
            y = dot(x_ref[item], side_by_side(halves(r_ref[item]))).astype(BF)
            y_ref[item, :, : 2 * PAIR] = y
            z = jnp.where(top, *halves(dot(f_ref[item], y)))
            z = jnp.where(same, z, ends[item] - z)
            if c == 0:
                before_ref[item] = jnp.where(off_eye, 1.0, 0.0).astype(BF)
                runs[p] = z.astype(BF)
            else:
                before_ref[item] = runs[p]
                step = jnp.where(same, turned(z), 0.0).astype(BF)
                runs[p] = (dot(step, runs[p]) + jnp.where(same, z, 0.0)).astype(BF)
    for p in range(pairs):
        total_ref[p] = runs[p]


def keys_side(keys, values, beta_pre, decay_pre):
    length, width = keys.shape
    pairs = width // PAIR
    steps = length // CHUNK
    items = steps * pairs
    wide = pltpu.VMEM((items, CHUNK, 2 * CHUNK), BF)
    return call(
        keys_kernel,
        "keys_side",
        [],
        [
            ((items, PAIR, PAIR), BF),
            ((pairs, PAIR, PAIR), BF),
            ((items, CHUNK, 3 * PAIR), BF),
            ((items, CHUNK, 2 * CHUNK), BF),
            ((length, width), F32),
        ],
        [
            wide,
            wide,
            wide,
            pltpu.VMEM((items, PAIR, CHUNK), BF),
            pltpu.VMEM((length, width), BF),
            pltpu.VMEM((length, width), BF),
            pltpu.VMEM(beta_pre.shape, F32),
            pltpu.VMEM(beta_pre.shape, F32),
            pltpu.SemaphoreType.DMA((2 + 2 * steps,)),
        ],
        far=[
            pltpu.with_memory_space_constraint(x, pltpu.HBM)
            for x in (keys, values, beta_pre, decay_pre)
        ],
    )


def gates_kernel(gates_ref, gain_ref, gate_ref):
    gain = jnp.concatenate([gain_ref[...], gain_ref[...]], axis=1)
    for p in range(gates_ref.shape[1] // PAIR):
        lanes = slice(p * PAIR, (p + 1) * PAIR)
        gate_ref[:, lanes] = silu(gates_ref[:, lanes].astype(F32)) * gain


def queries_kernel(first, after_ref, q_ref, d_ref, y_ref, before_ref, ec_ref, o_ref, q1_ref):
    row, col = places()
    left = col < HEAD_DIM
    same = left == (row < HEAD_DIM)
    ones = jnp.where(same, 1.0, 0.0).astype(BF)
    length, width = o_ref.shape
    pairs = q_ref.shape[1] // PAIR

    def chunk(c, carry):
        rows = pl.ds(pl.multiple_of(c * CHUNK, CHUNK), CHUNK)
        for p in range(first, first + width // PAIR):
            lanes = slice(p * PAIR, (p + 1) * PAIR)
            place = slice((p - first) * PAIR, (p - first + 1) * PAIR)
            item = c * pairs + p
            query = silu(q_ref[rows, lanes].astype(F32))
            query = query * lax.rsqrt(half_sums(query * query, ones) + EPSILON)
            query = (query * HEAD_DIM ** (-0.5)).astype(BF)
            key_f = y_ref[item, :, 2 * PAIR :].astype(F32)
            owns = [jnp.where(left, key_f, 0.0), jnp.where(left, 0.0, key_f)]
            inside = dot_nt(query, jnp.concatenate(owns, axis=0).astype(BF))
            inside = (inside * d_ref[item].astype(F32)).astype(BF)
            got = halves(dot(inside, side_by_side(halves(y_ref[item, :, : 2 * PAIR]))))
            local = jnp.where(left, got[0], got[1])
            crossed = turned(jnp.where(left, got[1], got[0]))
            query = (query.astype(F32) * ec_ref[rows, lanes] - crossed).astype(BF)
            before = before_ref[item].astype(F32)
            both = [jnp.where(same, before, 0.0), jnp.where(same, turned(before), 0.0)]
            moved = halves(dot(query, jnp.concatenate(both, axis=1).astype(BF)))
            o_ref[rows, place] = local + moved[0]
            q1_ref[rows, place] = moved[1].astype(BF)
        return carry

    lax.fori_loop(0, length // CHUNK, chunk, 0)


def gates_side(gates, gain):
    return call(
        gates_kernel, "gates_side", [gates, gain.reshape(1, HEAD_DIM)], [(gates.shape, F32)]
    )[0]


def queries_side(first, after, queries, decay, solved, before, grown):
    length, width = queries.shape
    shape = (length, width // 2)
    return call(
        functools.partial(queries_kernel, first),
        "queries_side",
        [queries, decay, solved, before, grown],
        [(shape, F32), (shape, BF)],
        far=[after],
    )


def chained(earlier, later, same):
    later = later.astype(F32)
    step = jnp.where(same, turned(later), 0.0).astype(BF)
    return dot(step, earlier.astype(BF)) + jnp.where(same, later, 0.0)


def chip_kernel(at_ref, own_ref, other_ref, out_ref):
    row, col = places()
    same = (col < HEAD_DIM) == (row < HEAD_DIM)
    core = at_ref[1]
    count = out_ref.shape[0]
    for p in range(count):
        mine = own_ref[core * count + p]
        theirs = other_ref[core * count + p]
        first = jnp.where(core == 0, mine, theirs)
        second = jnp.where(core == 0, theirs, mine)
        out_ref[p] = chained(first, second, same).astype(BF)


def row_kernel(at_ref, after_ref, *rest):
    parts, (total_ref, before_ref, all_ref) = rest[:-3], rest[-3:]
    row, col = places()
    same = (col < HEAD_DIM) == (row < HEAD_DIM)
    place = at_ref[2]
    size = len(parts)
    for k, part in enumerate(parts):
        all_ref[lax.rem(place - k + size, size)] = part[...]
    for p in range(total_ref.shape[0]):
        run = all_ref[0, p].astype(F32)
        inside = jnp.where(place == 0, jnp.where((row ^ col) == HEAD_DIM, 1.0, 0.0), run)
        for k in range(1, size):
            run = chained(run, all_ref[k, p], same)
            inside = jnp.where(k < place, run, inside)
        before_ref[p] = inside.astype(BF)
        total_ref[p] = run.astype(BF)


def plane_kernel(at_ref, after_ref, before_ref, *rest):
    parts, out_ref = rest[:-1], rest[-1]
    row, col = places()
    same = (col < HEAD_DIM) == (row < HEAD_DIM)
    place = at_ref[3]
    for p in range(out_ref.shape[0]):
        state = jnp.zeros((PAIR, PAIR), F32)
        for k in range(len(parts), 0, -1):
            later = jnp.where(same, chained(state, parts[k - 1][p], same), 0.0)
            state = jnp.where(k <= place, later, state)
        state = chained(state, before_ref[p], same)
        out_ref[p] = jnp.where(same, state, 0.0).astype(BF)


def state_ahead(at, total, meanwhile, then):
    plane, line, core = SP
    swap = [(0, 1), (1, 0)]
    half = (total.shape[0] // 2, PAIR, PAIR)
    other = lax.ppermute(total, core, swap)
    (chip,) = call(chip_kernel, "chip_total", [total, other], [(half, BF)], table=at)
    size = lax.axis_size(line)
    lines = [chip] + [lax.ppermute(chip, line, ring(size, k)) for k in range(1, size)]
    early = meanwhile(chip)
    whole, before = call(
        row_kernel,
        "line_total",
        lines,
        [(half, BF), (half, BF)],
        [pltpu.VMEM((size, *half), BF)],
        table=at,
        far=[early[1]],
    )
    size = lax.axis_size(plane)
    planes = [lax.ppermute(whole, plane, ring(size, k)) for k in range(1, size)]
    late = then(whole)
    (state,) = call(
        plane_kernel, "plane_state", [before] + planes, [(half, BF)], table=at, far=[late[1]]
    )
    return early, late, (other, state, lax.ppermute(state, core, swap))


def mixed_kernel(
    at_ref, o0_ref, q0_ref, o1_ref, q1_ref,
    first_ref, mine_ref, theirs_ref, gate_ref, w_ref, *rest,
):
    out_ref, mixed_ref, state_ref = rest
    row, col = places()
    same = (col < HEAD_DIM) == (row < HEAD_DIM)
    ones = jnp.where(same, 1.0, 0.0).astype(BF)
    length, width = gate_ref.shape
    core = at_ref[1]
    half = mine_ref.shape[0]
    state_ref[pl.ds(core * half, half)] = mine_ref[...]
    state_ref[pl.ds((1 - core) * half, half)] = theirs_ref[...]
    for p in range(width // PAIR):
        lanes = slice(p * PAIR, (p + 1) * PAIR)
        state = state_ref[p].astype(F32)
        later = jnp.where(same, chained(state, first_ref[p], same), 0.0)
        state = jnp.where(core == 0, state, later).astype(BF)
        o_ref, q_ref = ((o0_ref, q0_ref), (o1_ref, q1_ref))[p // half]
        place = slice((p % half) * PAIR, (p % half + 1) * PAIR)
        out = o_ref[:, place] + dot(q_ref[:, place], state)
        mean = half_sums(out * out, ones) * (1.0 / HEAD_DIM)
        out = out * lax.rsqrt(mean + EPSILON) * gate_ref[:, lanes]
        mixed_ref[:, lanes] = out.astype(BF)
    for n in range(w_ref.shape[1] // STRIP):
        here = slice(n * STRIP, (n + 1) * STRIP)
        got = dot(mixed_ref[...], w_ref[:, here]).astype(BF)
        block = out_ref.shape[1]
        for k in range(out_ref.shape[0]):
            out_ref[k, :, here] = got[k * block : (k + 1) * block, :]


def mixed_and_projected(at, size, early, late, states, gate, w_out):
    length, width = gate.shape
    return call(
        mixed_kernel,
        "mixed_and_projected",
        [*early, *late, *states, gate, w_out],
        [((size, length // size, w_out.shape[1]), BF)],
        [pltpu.VMEM((length, width), BF), pltpu.VMEM((width // PAIR, PAIR, PAIR), BF)],
        table=at,
    )[0]


def norm_kernel(stream_ref, gain_ref, parts_ref, middle_ref, normed_ref):
    projected = parts_ref[0].astype(F32)
    for k in range(1, parts_ref.shape[0]):
        projected = projected + parts_ref[k].astype(F32)
    middle = (stream_ref[...].astype(F32) + projected).astype(BF)
    middle_ref[...] = middle
    middle = middle.astype(F32)
    mean = jnp.mean(middle * middle, axis=-1, keepdims=True)
    normed_ref[...] = (middle * lax.rsqrt(mean + EPSILON) * gain_ref[...]).astype(BF)


def normed_rows(stream, gain, parts):
    return call(
        norm_kernel,
        "normed_rows",
        [stream, gain.reshape(1, -1), parts],
        [(stream.shape, BF), (stream.shape, BF)],
    )


def activated(rows, gate, up):
    got = dot(rows, jnp.concatenate([gate, up], axis=1))
    width = gate.shape[1]
    return (silu(got[:, :width]) * got[:, width:]).astype(BF)


def product_nt(a, b):
    even = a.shape[1] // 256 * 256
    return dot_nt(a[:, :even], b[:, :even]) + dot_nt(a[:, even:], b[:, even:])


TILE = 128
STRIP = 256
AHEAD = 4


def first_channels_kernel(count, w_ref, *rest):
    parts, out_refs = rest[:count], rest[count : 2 * count]
    gate_ref, up_ref, down_ref, rows_ref, hidden_ref, in_sems, down_sems = rest[2 * count :]
    width, hidden = gate_ref.shape
    block = parts[0].shape[0]
    groups = []
    for j in range(hidden // TILE):
        here = pl.ds(j * TILE, TILE)
        group = []
        for k, ref in enumerate((gate_ref, up_ref)):
            from_ref = w_ref.at[:, pl.ds(k * hidden + j * TILE, TILE)]
            group.append(pltpu.make_async_copy(from_ref, ref.at[:, here], in_sems.at[k, j]))
        groups.append(group)
    for n in range(width // STRIP):
        here = pl.ds(n * STRIP, STRIP)
        from_ref = w_ref.at[here, pl.ds(2 * hidden, hidden)]
        groups.append([pltpu.make_async_copy(from_ref, down_ref.at[here, :], down_sems.at[n])])

    def begin(g):
        if g < len(groups):
            for copy in groups[g]:
                copy.start()

    def arrived(g):
        for copy in groups[g]:
            copy.wait()
        begin(g + AHEAD)

    for g in range(AHEAD):
        begin(g)
    for k, part in enumerate(parts):
        rows_ref[k * block : (k + 1) * block, :] = part[...]
    for j in range(hidden // TILE):
        arrived(j)
        here = slice(j * TILE, (j + 1) * TILE)
        hidden_ref[:, here] = activated(rows_ref[...], gate_ref[:, here], up_ref[:, here])
    for n in range(width // STRIP):
        arrived(hidden // TILE + n)
        here = slice(n * STRIP, (n + 1) * STRIP)
        got = product_nt(hidden_ref[...], down_ref[here, :])
        for k, out_ref in enumerate(out_refs):
            out_ref[:, here] = got[k * block : (k + 1) * block, :].astype(BF)


def first_channels(weights, parts, hidden):
    block, width = parts[0].shape
    count = len(parts)
    out = call(
        functools.partial(first_channels_kernel, count),
        "first_channels",
        parts,
        [((block, width), BF)] * count + [((width, hidden), BF)] * 3,
        [
            pltpu.VMEM((block * count, width), BF),
            pltpu.VMEM((block * count, hidden), BF),
            pltpu.SemaphoreType.DMA((2, hidden // TILE)),
            pltpu.SemaphoreType.DMA((width // STRIP,)),
        ],
        far=[pltpu.with_memory_space_constraint(weights, pltpu.HBM)],
    )
    return out[:count], out[count:]


def more_channels_kernel(upper_ref, lower_ref, gate_ref, up_ref, down_ref, out_ref, hidden_ref):
    rows = jnp.concatenate([upper_ref[...], lower_ref[...]], axis=0)
    for j in range(gate_ref.shape[1] // TILE):
        here = slice(j * TILE, (j + 1) * TILE)
        hidden_ref[:, here] = activated(rows, gate_ref[:, here], up_ref[:, here])
    for n in range(down_ref.shape[0] // STRIP):
        here = slice(n * STRIP, (n + 1) * STRIP)
        out_ref[:, here] = product_nt(hidden_ref[...], down_ref[here, :]).astype(BF)


def more_channels(halves_of_rows, projections):
    half, width = halves_of_rows[0].shape
    return call(
        more_channels_kernel,
        "more_channels",
        [*halves_of_rows, *projections],
        [((2 * half, width), BF)],
        [pltpu.VMEM((2 * half, projections[0].shape[1]), BF)],
    )[0]


def last_kernel(middle_ref, *rest):
    parts, out_ref = rest[:-1], rest[-1]
    total = parts[0][...].astype(F32)
    for part in parts[1:]:
        total = total + part[...].astype(F32)
    out_ref[...] = (middle_ref[...].astype(F32) + 0.5 * total).astype(BF)


def last_sum(middle, parts):
    near = [pltpu.with_memory_space_constraint(x, pltpu.VMEM) for x in [middle, *parts]]
    return pl.pallas_call(
        last_kernel,
        in_specs=[FULL] * len(near),
        out_specs=FULL,
        out_shape=jax.ShapeDtypeStruct(middle.shape, BF),
        compiler_params=pltpu.CompilerParams(vmem_limit_bytes=16 << 20),
        name="last_sum",
    )(*near)


def per_device(
    queries,
    keys,
    values,
    gates,
    decay_pre,
    beta_pre,
    out_gain,
    w_out,
    stream,
    norm_gain,
    w_gate,
    w_up,
    w_down,
):
    hidden = w_gate.shape[1]
    weights = jnp.concatenate([w_gate, w_up, w_down.T], axis=1)
    weights = lax.all_gather(weights, SP, axis=0, tiled=True)
    size = lax.axis_size("tp")
    at = jnp.stack([lax.axis_index(a).astype(jnp.int32) for a in ("tp", *reversed(SP))])
    before, total, solved, decay, grown = keys_side(keys, values, beta_pre, decay_pre)
    gate = gates_side(gates, out_gain)
    pairs = queries.shape[1] // PAIR
    early, late, states = state_ahead(
        at,
        total,
        lambda x: queries_side(0, x, queries, decay, solved, before, grown),
        lambda x: queries_side(pairs // 2, x, queries, decay, solved, before, grown),
    )
    parts = mixed_and_projected(at, size, early, late, states, gate, w_out)
    parts = lax.all_to_all(parts, "tp", 0, 0, tiled=True)
    middle, normed = normed_rows(stream, norm_gain, parts)
    right = lax.ppermute(normed, "tp", ring(size, 1))
    left = lax.ppermute(normed, "tp", ring(size, -1))
    half = normed.shape[0] // 2
    across = [
        lax.ppermute(right[:half], "tp", ring(size, 1)),
        lax.ppermute(left[half:], "tp", ring(size, -1)),
    ]
    sums, projections = first_channels(weights, [normed, right, left], hidden)
    back = [lax.ppermute(sums[1], "tp", ring(size, -1)), lax.ppermute(sums[2], "tp", ring(size, 1))]
    last = more_channels(across, projections)
    back.append(lax.ppermute(last, "tp", ring(size, 2)))
    return last_sum(middle, [sums[0]] + back)


def solution(mesh):
    finer = Mesh(mesh.devices.reshape(4, 4, 2, mesh.shape["tp"]), SP_TP)
    placed = (
        P(SP, "tp"),
        P(SP, "tp"),
        P(SP, "tp"),
        P(SP, "tp"),
        P("tp", SP),
        P("tp", SP),
        P(),
        P("tp", None),
        P(SP_TP, None),
        P(),
        P(SP, "tp"),
        P(SP, "tp"),
        P("tp", SP),
    )
    return jax.shard_map(
        per_device, mesh=finer, in_specs=placed, out_specs=P(SP_TP, None), check_vma=False
    )
```

```python
import functools

import jax
import jax.numpy as jnp
from jax import lax
from jax.experimental import pallas as pl
from jax.experimental.pallas import tpu as pltpu
from jax.sharding import Mesh
from jax.sharding import PartitionSpec as P


HEAD_DIM = 64
PAIR = 2 * HEAD_DIM
CHUNK = 128
SP = ("sp_0", "sp_1", "sp_2")
SP_TP = ("sp_0", "sp_1", "sp_2", "tp")
EPSILON = 1e-06
BF = jnp.bfloat16
F32 = jnp.float32
NT = (((1,), (1,)), ((), ()))


FULL = pl.BlockSpec(memory_space=pltpu.VMEM)
FAR = pl.BlockSpec(memory_space=pl.ANY)
TABLE = pl.BlockSpec(memory_space=pltpu.SMEM)


def call(kernel, arrays, shapes, scratch=(), table=None, far=(), mib=16):
    near = [pltpu.with_memory_space_constraint(x, pltpu.VMEM) for x in arrays]
    tables = [] if table is None else [table]
    return pl.pallas_call(
        kernel,
        in_specs=[TABLE] * len(tables) + [FAR] * len(far) + [FULL] * len(near),
        out_specs=[FULL] * len(shapes),
        out_shape=[pltpu.VMEM(shape, dtype) for shape, dtype in shapes],
        scratch_shapes=scratch,
        compiler_params=pltpu.CompilerParams(vmem_limit_bytes=mib << 20),
    )(*tables, *far, *near)


def ring(size, k):
    return [(i, (i + k) % size) for i in range(size)]


def dot(a, b):
    return jnp.dot(a, b, preferred_element_type=F32)


def dot_nt(a, b):
    return lax.dot_general(a, b, NT, preferred_element_type=F32)


def silu(x):
    return x / (1.0 + jnp.exp(-x))


def places():
    row = lax.broadcasted_iota(jnp.int32, (PAIR, PAIR), 0)
    col = lax.broadcasted_iota(jnp.int32, (PAIR, PAIR), 1)
    return row, col


def half_sums(squares, ones):
    high = squares.astype(BF)
    low = (squares - high.astype(F32)).astype(BF)
    return dot(high, ones) + dot(low, ones)


def softplus(x):
    small = jnp.exp(-jnp.abs(x))
    series = small * (1.0 - small * (0.5 - small * (1.0 / 3.0 - 0.25 * small)))
    return jnp.maximum(x, 0.0) + jnp.where(small < 0.015, series, jnp.log(1.0 + small))


def turned(z):
    return pltpu.roll(z, HEAD_DIM, 1)


def split_three(x):
    high = x.astype(BF)
    rest = x - high.astype(F32)
    middle = rest.astype(BF)
    return jnp.concatenate([high, middle], axis=1), (rest - middle.astype(F32)).astype(BF)


def side_by_side(pair):
    zero = jnp.zeros_like(pair[0])
    upper = jnp.concatenate([pair[0], zero], axis=1)
    lower = jnp.concatenate([zero, pair[1]], axis=1)
    return jnp.concatenate([upper, lower], axis=0)


def halves(x):
    return x[:, :CHUNK], x[:, CHUNK:]


def keys_kernel(
    k_far_ref, v_far_ref, beta_far_ref, decay_far_ref,
    before_ref, total_ref, y_ref, d_ref, ec_ref,
    l_ref, x_ref, r_ref, f_ref, k_ref, v_ref, beta_ref, decay_ref, sems,
):
    length, width = k_ref.shape
    rate_copies = [
        pltpu.make_async_copy(decay_far_ref, decay_ref, sems.at[0]),
        pltpu.make_async_copy(beta_far_ref, beta_ref, sems.at[1]),
    ]
    row_copies = []
    for c in range(length // CHUNK):
        rows = pl.ds(c * CHUNK, CHUNK)
        for k, (far_ref, ref) in enumerate(((k_far_ref, k_ref), (v_far_ref, v_ref))):
            sem = sems.at[2 + 2 * c + k]
            row_copies.append(pltpu.make_async_copy(far_ref.at[rows], ref.at[rows], sem))
    for copy in rate_copies + row_copies:
        copy.start()
    row, col = places()
    left = col < HEAD_DIM
    top = row < HEAD_DIM
    same = left == top
    ones = jnp.where(same, 1.0, 0.0).astype(BF)
    inclusive = row >= col
    strict = row > col
    differ = row ^ col
    eye = jnp.where(row == col, 1.0, 0.0)
    off_eye = differ == HEAD_DIM
    pairs = width // PAIR
    heads = 2 * pairs
    steps = length // CHUNK

    def stacked(x):
        return jnp.concatenate([x[:, c * CHUNK : (c + 1) * CHUNK] for c in range(steps)], axis=0)

    for copy in rate_copies:
        copy.wait()
    rates = split_three(stacked(-softplus(decay_ref[...])))
    strength = split_three(stacked(1.0 / (1.0 + jnp.exp(-beta_ref[...]))))
    triangle = jnp.where(inclusive, 1.0, 0.0).astype(BF)
    eye_bf = eye.astype(BF)
    triangle_two = jnp.concatenate([triangle, triangle], axis=1)
    cum_row = dot_nt(rates[0], triangle_two) + dot_nt(rates[1], triangle)
    cum_col = dot_nt(triangle_two, rates[0]) + dot_nt(triangle, rates[1])
    beta_col = dot_nt(jnp.concatenate([eye_bf, eye_bf], axis=1), strength[0])
    beta_col = beta_col + dot_nt(eye_bf, strength[1])

    ends = []
    for c in range(steps):
        rows = slice(c * CHUNK, (c + 1) * CHUNK)
        row_copies[2 * c].wait()
        row_copies[2 * c + 1].wait()
        for p in range(pairs):
            lanes = slice(p * PAIR, (p + 1) * PAIR)
            item = c * pairs + p
            key = silu(k_ref[rows, lanes].astype(F32))
            key = (key * lax.rsqrt(half_sums(key * key, ones) + EPSILON)).astype(BF)
            y_ref[item, :, 2 * PAIR :] = key
            key_f = key.astype(F32)
            first = c * heads + 2 * p
            cums = [cum_col[:, h : h + 1] for h in (first, first + 1)]
            betas = [beta_col[:, h : h + 1] for h in (first, first + 1)]
            cum = jnp.where(left, cums[0], cums[1])
            beta = jnp.where(left, betas[0], betas[1])
            grown = jnp.exp(cum)
            ec_ref[rows, lanes] = grown
            strong = turned(key_f * (beta * grown))
            value = silu(v_ref[rows, lanes].astype(F32)) * beta
            r_ref[item, :, :CHUNK] = jnp.where(left, value, strong).astype(BF)
            r_ref[item, :, CHUNK:] = jnp.where(left, strong, value).astype(BF)
            fade = jnp.exp(cum[CHUNK - 1 : CHUNK, :] - cum)
            f_ref[item] = (key_f * fade).T.astype(BF)
            last = [jnp.exp(x[CHUNK - 1 : CHUNK, :]) for x in cums]
            ends.append(jnp.where(off_eye, jnp.where(top, last[0], last[1]), 0.0))
            owns = [jnp.where(left, key_f, 0.0), jnp.where(left, 0.0, key_f)]
            inner = dot_nt(key, jnp.concatenate(owns, axis=0).astype(BF))
            for s in range(2):
                part = slice(s * CHUNK, (s + 1) * CHUNK)
                gap = cums[s] - cum_row[first + s : first + s + 1, :]
                decay = jnp.where(inclusive, jnp.exp(gap), 0.0)
                d_ref[item, :, part] = decay.astype(BF)
                lower = jnp.where(strict, inner[:, part] * decay * betas[s], 0.0)
                l_ref[item, :, part] = lower.astype(BF)
                x_ref[item, :, part] = (eye - jnp.where(differ == 1, lower, 0.0)).astype(BF)

    items = steps * pairs

    def level(power, carry):
        mask = jnp.where((differ >> power) == 1, 1.0, 0.0).astype(BF)
        parts = []
        for i in range(items):
            block = side_by_side([part * mask for part in halves(l_ref[i])])
            parts.append(dot(x_ref[i], block).astype(BF))
        for i in range(items):
            x = x_ref[i]
            x_ref[i] = x - dot(parts[i], side_by_side(halves(x))).astype(BF)
        return carry

    lax.fori_loop(1, 7, level, 0)

    runs = [None] * pairs
    for c in range(steps):
        for p in range(pairs):
            item = c * pairs + p
            y = dot(x_ref[item], side_by_side(halves(r_ref[item]))).astype(BF)
            y_ref[item, :, : 2 * PAIR] = y
            z = jnp.where(top, *halves(dot(f_ref[item], y)))
            z = jnp.where(same, z, ends[item] - z)
            if c == 0:
                before_ref[item] = jnp.where(off_eye, 1.0, 0.0).astype(BF)
                runs[p] = z.astype(BF)
            else:
                before_ref[item] = runs[p]
                step = jnp.where(same, turned(z), 0.0).astype(BF)
                runs[p] = (dot(step, runs[p]) + jnp.where(same, z, 0.0)).astype(BF)
    for p in range(pairs):
        total_ref[p] = runs[p]


def keys_side(keys, values, beta_pre, decay_pre):
    length, width = keys.shape
    pairs = width // PAIR
    steps = length // CHUNK
    items = steps * pairs
    wide = pltpu.VMEM((items, CHUNK, 2 * CHUNK), BF)
    return call(
        keys_kernel,
        [],
        [
            ((items, PAIR, PAIR), BF),
            ((pairs, PAIR, PAIR), BF),
            ((items, CHUNK, 3 * PAIR), BF),
            ((items, CHUNK, 2 * CHUNK), BF),
            ((length, width), F32),
        ],
        [
            wide,
            wide,
            wide,
            pltpu.VMEM((items, PAIR, CHUNK), BF),
            pltpu.VMEM((length, width), BF),
            pltpu.VMEM((length, width), BF),
            pltpu.VMEM(beta_pre.shape, F32),
            pltpu.VMEM(beta_pre.shape, F32),
            pltpu.SemaphoreType.DMA((2 + 2 * steps,)),
        ],
        far=[
            pltpu.with_memory_space_constraint(x, pltpu.HBM)
            for x in (keys, values, beta_pre, decay_pre)
        ],
    )


def gates_kernel(gates_ref, gain_ref, gate_ref):
    gain = jnp.concatenate([gain_ref[...], gain_ref[...]], axis=1)
    for p in range(gates_ref.shape[1] // PAIR):
        lanes = slice(p * PAIR, (p + 1) * PAIR)
        gate_ref[:, lanes] = silu(gates_ref[:, lanes].astype(F32)) * gain


def queries_kernel(first, after_ref, q_ref, d_ref, y_ref, before_ref, ec_ref, o_ref, q1_ref):
    row, col = places()
    left = col < HEAD_DIM
    same = left == (row < HEAD_DIM)
    ones = jnp.where(same, 1.0, 0.0).astype(BF)
    length, width = o_ref.shape
    pairs = q_ref.shape[1] // PAIR

    def chunk(c, carry):
        rows = pl.ds(pl.multiple_of(c * CHUNK, CHUNK), CHUNK)
        for p in range(first, first + width // PAIR):
            lanes = slice(p * PAIR, (p + 1) * PAIR)
            place = slice((p - first) * PAIR, (p - first + 1) * PAIR)
            item = c * pairs + p
            query = silu(q_ref[rows, lanes].astype(F32))
            query = query * lax.rsqrt(half_sums(query * query, ones) + EPSILON)
            query = (query * HEAD_DIM ** (-0.5)).astype(BF)
            key_f = y_ref[item, :, 2 * PAIR :].astype(F32)
            owns = [jnp.where(left, key_f, 0.0), jnp.where(left, 0.0, key_f)]
            inside = dot_nt(query, jnp.concatenate(owns, axis=0).astype(BF))
            inside = (inside * d_ref[item].astype(F32)).astype(BF)
            got = halves(dot(inside, side_by_side(halves(y_ref[item, :, : 2 * PAIR]))))
            local = jnp.where(left, got[0], got[1])
            crossed = turned(jnp.where(left, got[1], got[0]))
            query = (query.astype(F32) * ec_ref[rows, lanes] - crossed).astype(BF)
            before = before_ref[item].astype(F32)
            both = [jnp.where(same, before, 0.0), jnp.where(same, turned(before), 0.0)]
            moved = halves(dot(query, jnp.concatenate(both, axis=1).astype(BF)))
            o_ref[rows, place] = local + moved[0]
            q1_ref[rows, place] = moved[1].astype(BF)
        return carry

    lax.fori_loop(0, length // CHUNK, chunk, 0)


def gates_side(gates, gain):
    return call(gates_kernel, [gates, gain.reshape(1, HEAD_DIM)], [(gates.shape, F32)])[0]


def queries_side(first, after, queries, decay, solved, before, grown):
    length, width = queries.shape
    shape = (length, width // 2)
    return call(
        functools.partial(queries_kernel, first),
        [queries, decay, solved, before, grown],
        [(shape, F32), (shape, BF)],
        far=[after],
    )


def chained(earlier, later, same):
    later = later.astype(F32)
    step = jnp.where(same, turned(later), 0.0).astype(BF)
    return dot(step, earlier.astype(BF)) + jnp.where(same, later, 0.0)


def chip_kernel(at_ref, own_ref, other_ref, out_ref):
    row, col = places()
    same = (col < HEAD_DIM) == (row < HEAD_DIM)
    core = at_ref[1]
    count = out_ref.shape[0]
    for p in range(count):
        mine = own_ref[core * count + p]
        theirs = other_ref[core * count + p]
        first = jnp.where(core == 0, mine, theirs)
        second = jnp.where(core == 0, theirs, mine)
        out_ref[p] = chained(first, second, same).astype(BF)


def row_kernel(at_ref, after_ref, *rest):
    parts, (total_ref, before_ref, all_ref) = rest[:-3], rest[-3:]
    row, col = places()
    same = (col < HEAD_DIM) == (row < HEAD_DIM)
    place = at_ref[2]
    size = len(parts)
    for k, part in enumerate(parts):
        all_ref[lax.rem(place - k + size, size)] = part[...]
    for p in range(total_ref.shape[0]):
        run = all_ref[0, p].astype(F32)
        inside = jnp.where(place == 0, jnp.where((row ^ col) == HEAD_DIM, 1.0, 0.0), run)
        for k in range(1, size):
            run = chained(run, all_ref[k, p], same)
            inside = jnp.where(k < place, run, inside)
        before_ref[p] = inside.astype(BF)
        total_ref[p] = run.astype(BF)


def plane_kernel(at_ref, after_ref, before_ref, *rest):
    parts, out_ref = rest[:-1], rest[-1]
    row, col = places()
    same = (col < HEAD_DIM) == (row < HEAD_DIM)
    place = at_ref[3]
    for p in range(out_ref.shape[0]):
        state = jnp.zeros((PAIR, PAIR), F32)
        for k in range(len(parts), 0, -1):
            later = jnp.where(same, chained(state, parts[k - 1][p], same), 0.0)
            state = jnp.where(k <= place, later, state)
        state = chained(state, before_ref[p], same)
        out_ref[p] = jnp.where(same, state, 0.0).astype(BF)


def state_ahead(at, total, meanwhile, then):
    plane, line, core = SP
    swap = [(0, 1), (1, 0)]
    half = (total.shape[0] // 2, PAIR, PAIR)
    other = lax.ppermute(total, core, swap)
    (chip,) = call(chip_kernel, [total, other], [(half, BF)], table=at)
    size = lax.axis_size(line)
    lines = [chip] + [lax.ppermute(chip, line, ring(size, k)) for k in range(1, size)]
    early = meanwhile(chip)
    whole, before = call(
        row_kernel,
        lines,
        [(half, BF), (half, BF)],
        [pltpu.VMEM((size, *half), BF)],
        table=at,
        far=[early[1]],
    )
    size = lax.axis_size(plane)
    planes = [lax.ppermute(whole, plane, ring(size, k)) for k in range(1, size)]
    late = then(whole)
    (state,) = call(plane_kernel, [before] + planes, [(half, BF)], table=at, far=[late[1]])
    return early, late, (other, state, lax.ppermute(state, core, swap))


def mixed_kernel(
    at_ref, o0_ref, q0_ref, o1_ref, q1_ref,
    first_ref, mine_ref, theirs_ref, gate_ref, w_ref, *rest,
):
    out_refs, (mixed_ref, state_ref) = rest[:-2], rest[-2:]
    row, col = places()
    same = (col < HEAD_DIM) == (row < HEAD_DIM)
    ones = jnp.where(same, 1.0, 0.0).astype(BF)
    length, width = gate_ref.shape
    core = at_ref[1]
    half = mine_ref.shape[0]
    state_ref[pl.ds(core * half, half)] = mine_ref[...]
    state_ref[pl.ds((1 - core) * half, half)] = theirs_ref[...]
    for p in range(width // PAIR):
        lanes = slice(p * PAIR, (p + 1) * PAIR)
        state = state_ref[p].astype(F32)
        later = jnp.where(same, chained(state, first_ref[p], same), 0.0)
        state = jnp.where(core == 0, state, later).astype(BF)
        o_ref, q_ref = ((o0_ref, q0_ref), (o1_ref, q1_ref))[p // half]
        place = slice((p % half) * PAIR, (p % half + 1) * PAIR)
        out = o_ref[:, place] + dot(q_ref[:, place], state)
        mean = half_sums(out * out, ones) * (1.0 / HEAD_DIM)
        out = out * lax.rsqrt(mean + EPSILON) * gate_ref[:, lanes]
        mixed_ref[:, lanes] = out.astype(BF)
    size = len(out_refs)
    block = length // size
    for k, out_ref in enumerate(out_refs):
        start = lax.rem(at_ref[0] + k, size) * block
        rows = mixed_ref[pl.ds(pl.multiple_of(start, 32), block), :]
        out_ref[...] = dot(rows, w_ref[...]).astype(out_ref.dtype)


def mixed_and_projected(at, size, early, late, states, gate, w_out):
    length, width = gate.shape
    return call(
        mixed_kernel,
        [*early, *late, *states, gate, w_out],
        [((length // size, w_out.shape[1]), BF if k else F32) for k in range(size)],
        [pltpu.VMEM((length, width), BF), pltpu.VMEM((width // PAIR, PAIR, PAIR), BF)],
        table=at,
    )


def norm_kernel(stream_ref, gain_ref, *rest):
    parts, (middle_ref, normed_ref) = rest[:-2], rest[-2:]
    projected = parts[0][...]
    for part in parts[1:]:
        projected = projected + part[...].astype(F32)
    middle = (stream_ref[...].astype(F32) + projected).astype(BF)
    middle_ref[...] = middle
    middle = middle.astype(F32)
    mean = jnp.mean(middle * middle, axis=-1, keepdims=True)
    normed_ref[...] = (middle * lax.rsqrt(mean + EPSILON) * gain_ref[...]).astype(BF)


def normed_rows(stream, gain, parts):
    return call(
        norm_kernel, [stream, gain.reshape(1, -1), *parts], [(stream.shape, BF), (stream.shape, BF)]
    )


def activated(rows, gate, up):
    got = dot(rows, jnp.concatenate([gate, up], axis=1))
    width = gate.shape[1]
    return (silu(got[:, :width]) * got[:, width:]).astype(BF)


def product_nt(a, b):
    even = a.shape[1] // 256 * 256
    return dot_nt(a[:, :even], b[:, :even]) + dot_nt(a[:, even:], b[:, even:])


TILE = 128
STRIP = 256
AHEAD = 3
UP_GROUPS = (1, 2, 4, 4)
DOWN_GROUPS = (8,)


def first_channels_kernel(count, w_ref, *rest):
    parts, out_refs = rest[:count], rest[count : 2 * count]
    gate_ref, up_ref, down_ref, rows_ref, hidden_ref, in_sems, down_sems = rest[2 * count :]
    width, hidden = gate_ref.shape
    block = parts[0].shape[0]
    groups, spans = [], []
    for many, spread in ((hidden // TILE, UP_GROUPS), (width // STRIP, DOWN_GROUPS)):
        assert sum(spread) == many
        starts = [sum(spread[:k]) for k in range(len(spread))]
        spans.append([range(start, start + n) for start, n in zip(starts, spread)])
    for g, tiles in enumerate(spans[0]):
        here = pl.ds(tiles[0] * TILE, len(tiles) * TILE)
        group = []
        for k, ref in enumerate((gate_ref, up_ref)):
            from_ref = w_ref.at[:, pl.ds(k * hidden + tiles[0] * TILE, len(tiles) * TILE)]
            group.append(pltpu.make_async_copy(from_ref, ref.at[:, here], in_sems.at[k, g]))
        groups.append(group)
    for g, strips in enumerate(spans[1]):
        here = pl.ds(strips[0] * STRIP, len(strips) * STRIP)
        from_ref = w_ref.at[here, pl.ds(2 * hidden, hidden)]
        groups.append([pltpu.make_async_copy(from_ref, down_ref.at[here, :], down_sems.at[g])])

    def begin(g):
        if g < len(groups):
            for copy in groups[g]:
                copy.start()

    def arrived(g):
        for copy in groups[g]:
            copy.wait()
        begin(g + AHEAD)

    for g in range(AHEAD):
        begin(g)
    for k, part in enumerate(parts):
        rows_ref[k * block : (k + 1) * block, :] = part[...]
    for g, tiles in enumerate(spans[0]):
        arrived(g)
        for j in tiles:
            here = slice(j * TILE, (j + 1) * TILE)
            hidden_ref[:, here] = activated(rows_ref[...], gate_ref[:, here], up_ref[:, here])
    for g, strips in enumerate(spans[1]):
        arrived(len(spans[0]) + g)
        for n in strips:
            here = slice(n * STRIP, (n + 1) * STRIP)
            got = product_nt(hidden_ref[...], down_ref[here, :])
            for k, out_ref in enumerate(out_refs):
                out_ref[:, here] = got[k * block : (k + 1) * block, :].astype(BF)


def first_channels(weights, parts, hidden):
    block, width = parts[0].shape
    count = len(parts)
    out = call(
        functools.partial(first_channels_kernel, count),
        parts,
        [((block, width), BF)] * count + [((width, hidden), BF)] * 3,
        [
            pltpu.VMEM((block * count, width), BF),
            pltpu.VMEM((block * count, hidden), BF),
            pltpu.SemaphoreType.DMA((2, len(UP_GROUPS))),
            pltpu.SemaphoreType.DMA((len(DOWN_GROUPS),)),
        ],
        far=[pltpu.with_memory_space_constraint(weights, pltpu.HBM)],
    )
    return out[:count], out[count:]


def more_channels_kernel(own_ref, upper_ref, lower_ref, gate_ref, up_ref, down_ref, *rest):
    out_refs, hidden_ref = rest[:-1], rest[-1]
    block = own_ref.shape[0]
    rows = jnp.concatenate([own_ref[...], upper_ref[...], lower_ref[...]], axis=0)
    for j in range(gate_ref.shape[1] // TILE):
        here = slice(j * TILE, (j + 1) * TILE)
        hidden_ref[:, here] = activated(rows, gate_ref[:, here], up_ref[:, here])
    for n in range(down_ref.shape[0] // STRIP):
        here = slice(n * STRIP, (n + 1) * STRIP)
        got = product_nt(hidden_ref[...], down_ref[here, :])
        for k, out_ref in enumerate(out_refs):
            out_ref[:, here] = got[k * block : (k + 1) * block, :].astype(BF)


def more_channels(rows, projections):
    block, width = rows[0].shape
    return call(
        more_channels_kernel,
        [*rows, *projections],
        [((block, width), BF)] * 2,
        [pltpu.VMEM((2 * block, projections[0].shape[1]), BF)],
    )


def last_kernel(middle_ref, *rest):
    parts, out_ref = rest[:-1], rest[-1]
    total = parts[0][...].astype(F32)
    for part in parts[1:]:
        total = total + part[...].astype(F32)
    out_ref[...] = (middle_ref[...].astype(F32) + 0.5 * total).astype(BF)


def last_sum(middle, parts):
    near = [pltpu.with_memory_space_constraint(x, pltpu.VMEM) for x in [middle, *parts]]
    return pl.pallas_call(
        last_kernel,
        in_specs=[FULL] * len(near),
        out_specs=FULL,
        out_shape=jax.ShapeDtypeStruct(middle.shape, BF),
        compiler_params=pltpu.CompilerParams(vmem_limit_bytes=16 << 20),
        name="last_sum",
    )(*near)


def per_device(
    queries,
    keys,
    values,
    gates,
    decay_pre,
    beta_pre,
    out_gain,
    w_out,
    stream,
    norm_gain,
    w_gate,
    w_up,
    w_down,
):
    hidden = w_gate.shape[1]
    weights = jnp.concatenate([w_gate, w_up, w_down.T], axis=1)
    weights = lax.all_gather(weights, SP, axis=0, tiled=True)
    size = lax.axis_size("tp")
    at = jnp.stack([lax.axis_index(a).astype(jnp.int32) for a in ("tp", *reversed(SP))])
    before, total, solved, decay, grown = keys_side(keys, values, beta_pre, decay_pre)
    gate = gates_side(gates, out_gain)
    pairs = queries.shape[1] // PAIR
    early, late, states = state_ahead(
        at,
        total,
        lambda x: queries_side(0, x, queries, decay, solved, before, grown),
        lambda x: queries_side(pairs // 2, x, queries, decay, solved, before, grown),
    )
    parts = mixed_and_projected(at, size, early, late, states, gate, w_out)
    parts = [parts[0]] + [lax.ppermute(parts[k], "tp", ring(size, k)) for k in (2, 1, 3)]
    middle, normed = normed_rows(stream, norm_gain, parts)
    right = lax.ppermute(normed, "tp", ring(size, 1))
    left = lax.ppermute(normed, "tp", ring(size, -1))
    half = normed.shape[0] // 2
    across = [
        lax.ppermute(right[:half], "tp", ring(size, 1)),
        lax.ppermute(left[half:], "tp", ring(size, -1)),
    ]
    sums, projections = first_channels(weights, [right, left], hidden)
    back = [lax.ppermute(sums[0], "tp", ring(size, -1))]
    back.append(lax.ppermute(sums[1], "tp", ring(size, 1)))
    own, last = more_channels([normed, *across], projections)
    back.append(lax.ppermute(last, "tp", ring(size, 2)))
    return last_sum(middle, [own] + back)


def solution(mesh):
    finer = Mesh(mesh.devices.reshape(4, 4, 2, mesh.shape["tp"]), SP_TP)
    placed = (
        P(SP, "tp"),
        P(SP, "tp"),
        P(SP, "tp"),
        P(SP, "tp"),
        P("tp", SP),
        P("tp", SP),
        P(),
        P("tp", None),
        P(SP_TP, None),
        P(),
        P(SP, "tp"),
        P(SP, "tp"),
        P("tp", SP),
    )
    return jax.shard_map(
        per_device, mesh=finer, in_specs=placed, out_specs=P(SP_TP, None), check_vma=False
    )
```

```python
import functools

import jax
import jax.numpy as jnp
from jax import lax
from jax.experimental import pallas as pl
from jax.experimental.pallas import tpu as pltpu
from jax.sharding import Mesh
from jax.sharding import PartitionSpec as P


HEAD_DIM = 64
PAIR = 2 * HEAD_DIM
CHUNK = 128
SP = ("sp_0", "sp_1", "sp_2")
SP_TP = ("sp_0", "sp_1", "sp_2", "tp")
EPSILON = 1e-06
BF = jnp.bfloat16
F32 = jnp.float32
NT = (((1,), (1,)), ((), ()))


FULL = pl.BlockSpec(memory_space=pltpu.VMEM)
FAR = pl.BlockSpec(memory_space=pl.ANY)


def call(kernel, arrays, shapes, scratch=(), far=(), mib=16):
    near = [pltpu.with_memory_space_constraint(x, pltpu.VMEM) for x in arrays]
    return pl.pallas_call(
        kernel,
        in_specs=[FAR] * len(far) + [FULL] * len(near),
        out_specs=[FULL] * len(shapes),
        out_shape=[pltpu.VMEM(shape, dtype) for shape, dtype in shapes],
        scratch_shapes=scratch,
        compiler_params=pltpu.CompilerParams(vmem_limit_bytes=mib << 20),
    )(*far, *near)


def ring(size, k):
    return [(i, (i + k) % size) for i in range(size)]


def dot(a, b):
    return jnp.dot(a, b, preferred_element_type=F32)


def dot_nt(a, b):
    return lax.dot_general(a, b, NT, preferred_element_type=F32)


def silu(x):
    return x / (1.0 + jnp.exp(-x))


def places():
    row = lax.broadcasted_iota(jnp.int32, (PAIR, PAIR), 0)
    col = lax.broadcasted_iota(jnp.int32, (PAIR, PAIR), 1)
    return row, col


def half_sums(squares, ones):
    high = squares.astype(BF)
    low = (squares - high.astype(F32)).astype(BF)
    return dot(high, ones) + dot(low, ones)


def softplus(x):
    small = jnp.exp(-jnp.abs(x))
    series = small * (1.0 - small * (0.5 - small * (1.0 / 3.0 - 0.25 * small)))
    return jnp.maximum(x, 0.0) + jnp.where(small < 0.015, series, jnp.log(1.0 + small))


def turned(z):
    return pltpu.roll(z, HEAD_DIM, 1)


def split_three(x):
    high = x.astype(BF)
    rest = x - high.astype(F32)
    middle = rest.astype(BF)
    return jnp.concatenate([high, middle], axis=1), (rest - middle.astype(F32)).astype(BF)


def side_by_side(pair):
    zero = jnp.zeros_like(pair[0])
    upper = jnp.concatenate([pair[0], zero], axis=1)
    lower = jnp.concatenate([zero, pair[1]], axis=1)
    return jnp.concatenate([upper, lower], axis=0)


def halves(x):
    return x[:, :CHUNK], x[:, CHUNK:]


def packing_kernel(*rest):
    from_refs, packed_ref, sems = rest[:-2], rest[-2], rest[-1]
    hidden = from_refs[0].shape[1]
    copies = []
    for k, ref in enumerate(from_refs):
        here = packed_ref.at[:, pl.ds(k * hidden, hidden)]
        copies.append(pltpu.make_async_copy(ref, here, sems.at[k]))
    for copy in copies:
        copy.start()
    for copy in copies:
        copy.wait()


def packed(weights):
    rows, hidden = weights[0].shape
    far = [pltpu.with_memory_space_constraint(x, pltpu.HBM) for x in weights]
    return pl.pallas_call(
        packing_kernel,
        in_specs=[FAR] * len(far),
        out_specs=FAR,
        out_shape=pltpu.HBM((rows, len(weights) * hidden), BF),
        scratch_shapes=[pltpu.SemaphoreType.DMA((len(far),))],
        compiler_params=pltpu.CompilerParams(vmem_limit_bytes=16 << 20),
        name="packed",
    )(*far)


def keys_kernel(
    k_far_ref, v_far_ref, beta_far_ref, decay_far_ref,
    before_ref, total_ref, y_ref, d_ref, ec_ref,
    l_ref, x_ref, r_ref, f_ref, k_ref, v_ref, beta_ref, decay_ref, sems,
):
    length, width = k_ref.shape
    rate_copies = [
        pltpu.make_async_copy(decay_far_ref, decay_ref, sems.at[0]),
        pltpu.make_async_copy(beta_far_ref, beta_ref, sems.at[1]),
    ]
    row_copies = []
    for c in range(length // CHUNK):
        rows = pl.ds(c * CHUNK, CHUNK)
        for k, (far_ref, ref) in enumerate(((k_far_ref, k_ref), (v_far_ref, v_ref))):
            sem = sems.at[2 + 2 * c + k]
            row_copies.append(pltpu.make_async_copy(far_ref.at[rows], ref.at[rows], sem))
    for copy in rate_copies + row_copies:
        copy.start()
    row, col = places()
    left = col < HEAD_DIM
    top = row < HEAD_DIM
    same = left == top
    ones = jnp.where(same, 1.0, 0.0).astype(BF)
    inclusive = row >= col
    strict = row > col
    differ = row ^ col
    eye = jnp.where(row == col, 1.0, 0.0)
    off_eye = differ == HEAD_DIM
    pairs = width // PAIR
    heads = 2 * pairs
    steps = length // CHUNK

    def stacked(x):
        return jnp.concatenate([x[:, c * CHUNK : (c + 1) * CHUNK] for c in range(steps)], axis=0)

    for copy in rate_copies + row_copies:
        copy.wait()
    rates = split_three(stacked(-softplus(decay_ref[...])))
    strength = split_three(stacked(1.0 / (1.0 + jnp.exp(-beta_ref[...]))))
    triangle = jnp.where(inclusive, 1.0, 0.0).astype(BF)
    eye_bf = eye.astype(BF)
    triangle_two = jnp.concatenate([triangle, triangle], axis=1)
    cum_row = dot_nt(rates[0], triangle_two) + dot_nt(rates[1], triangle)
    cum_col = dot_nt(triangle_two, rates[0]) + dot_nt(triangle, rates[1])
    beta_col = dot_nt(jnp.concatenate([eye_bf, eye_bf], axis=1), strength[0])
    beta_col = beta_col + dot_nt(eye_bf, strength[1])

    ends = []
    for c in range(steps):
        rows = slice(c * CHUNK, (c + 1) * CHUNK)
        for p in range(pairs):
            lanes = slice(p * PAIR, (p + 1) * PAIR)
            item = c * pairs + p
            key = silu(k_ref[rows, lanes].astype(F32))
            key = (key * lax.rsqrt(half_sums(key * key, ones) + EPSILON)).astype(BF)
            y_ref[item, :, 2 * PAIR :] = key
            key_f = key.astype(F32)
            first = c * heads + 2 * p
            cums = [cum_col[:, h : h + 1] for h in (first, first + 1)]
            betas = [beta_col[:, h : h + 1] for h in (first, first + 1)]
            cum = jnp.where(left, cums[0], cums[1])
            beta = jnp.where(left, betas[0], betas[1])
            grown = jnp.exp(cum)
            ec_ref[rows, lanes] = grown
            strong = turned(key_f * (beta * grown))
            value = silu(v_ref[rows, lanes].astype(F32)) * beta
            r_ref[item, :, :CHUNK] = jnp.where(left, value, strong).astype(BF)
            r_ref[item, :, CHUNK:] = jnp.where(left, strong, value).astype(BF)
            fade = jnp.exp(cum[CHUNK - 1 : CHUNK, :] - cum)
            f_ref[item] = (key_f * fade).T.astype(BF)
            last = [jnp.exp(x[CHUNK - 1 : CHUNK, :]) for x in cums]
            ends.append(jnp.where(off_eye, jnp.where(top, last[0], last[1]), 0.0))
            owns = [jnp.where(left, key_f, 0.0), jnp.where(left, 0.0, key_f)]
            inner = dot_nt(key, jnp.concatenate(owns, axis=0).astype(BF))
            for s in range(2):
                part = slice(s * CHUNK, (s + 1) * CHUNK)
                gap = cums[s] - cum_row[first + s : first + s + 1, :]
                decay = jnp.where(inclusive, jnp.exp(gap), 0.0)
                d_ref[item, :, part] = decay.astype(BF)
                lower = jnp.where(strict, inner[:, part] * decay * betas[s], 0.0)
                l_ref[item, :, part] = lower.astype(BF)
                x_ref[item, :, part] = (eye - jnp.where(differ == 1, lower, 0.0)).astype(BF)

    items = steps * pairs

    for power in range(1, 7):
        mask = jnp.where((differ >> power) == 1, 1.0, 0.0).astype(BF)
        parts = []
        for i in range(items):
            block = side_by_side([part * mask for part in halves(l_ref[i])])
            parts.append(dot(x_ref[i], block).astype(BF))
        for i in range(items):
            x = x_ref[i]
            x_ref[i] = x - dot(parts[i], side_by_side(halves(x))).astype(BF)

    runs = [None] * pairs
    for c in range(steps):
        for p in range(pairs):
            item = c * pairs + p
            y = dot(x_ref[item], side_by_side(halves(r_ref[item]))).astype(BF)
            y_ref[item, :, : 2 * PAIR] = y
            z = jnp.where(top, *halves(dot(f_ref[item], y)))
            z = jnp.where(same, z, ends[item] - z)
            if c == 0:
                before_ref[item] = jnp.where(off_eye, 1.0, 0.0).astype(BF)
                runs[p] = z.astype(BF)
            else:
                before_ref[item] = runs[p]
                step = jnp.where(same, turned(z), 0.0).astype(BF)
                runs[p] = (dot(step, runs[p]) + jnp.where(same, z, 0.0)).astype(BF)
    for p in range(pairs):
        total_ref[p] = runs[p]


def keys_side(keys, values, beta_pre, decay_pre):
    length, width = keys.shape
    pairs = width // PAIR
    steps = length // CHUNK
    items = steps * pairs
    wide = pltpu.VMEM((items, CHUNK, 2 * CHUNK), BF)
    return call(
        keys_kernel,
        [],
        [
            ((items, PAIR, PAIR), BF),
            ((pairs, PAIR, PAIR), BF),
            ((items, CHUNK, 3 * PAIR), BF),
            ((items, CHUNK, 2 * CHUNK), BF),
            ((length, width), F32),
        ],
        [
            wide,
            wide,
            wide,
            pltpu.VMEM((items, PAIR, CHUNK), BF),
            pltpu.VMEM((length, width), BF),
            pltpu.VMEM((length, width), BF),
            pltpu.VMEM(beta_pre.shape, F32),
            pltpu.VMEM(beta_pre.shape, F32),
            pltpu.SemaphoreType.DMA((2 + 2 * steps,)),
        ],
        far=[
            pltpu.with_memory_space_constraint(x, pltpu.HBM)
            for x in (keys, values, beta_pre, decay_pre)
        ],
    )


def gates_kernel(gates_ref, gain_ref, gate_ref):
    gain = jnp.concatenate([gain_ref[...], gain_ref[...]], axis=1)
    for p in range(gates_ref.shape[1] // PAIR):
        lanes = slice(p * PAIR, (p + 1) * PAIR)
        gate_ref[:, lanes] = silu(gates_ref[:, lanes].astype(F32)) * gain


def queries_kernel(first, after_ref, q_ref, d_ref, y_ref, before_ref, ec_ref, o_ref, q1_ref):
    row, col = places()
    left = col < HEAD_DIM
    same = left == (row < HEAD_DIM)
    ones = jnp.where(same, 1.0, 0.0).astype(BF)
    length, width = o_ref.shape
    pairs = q_ref.shape[1] // PAIR

    def chunk(c, carry):
        rows = pl.ds(pl.multiple_of(c * CHUNK, CHUNK), CHUNK)
        for p in range(first, first + width // PAIR):
            lanes = slice(p * PAIR, (p + 1) * PAIR)
            place = slice((p - first) * PAIR, (p - first + 1) * PAIR)
            item = c * pairs + p
            query = silu(q_ref[rows, lanes].astype(F32))
            query = query * lax.rsqrt(half_sums(query * query, ones) + EPSILON)
            query = (query * HEAD_DIM ** (-0.5)).astype(BF)
            key_f = y_ref[item, :, 2 * PAIR :].astype(F32)
            owns = [jnp.where(left, key_f, 0.0), jnp.where(left, 0.0, key_f)]
            inside = dot_nt(query, jnp.concatenate(owns, axis=0).astype(BF))
            inside = (inside * d_ref[item].astype(F32)).astype(BF)
            got = halves(dot(inside, side_by_side(halves(y_ref[item, :, : 2 * PAIR]))))
            local = jnp.where(left, got[0], got[1])
            crossed = turned(jnp.where(left, got[1], got[0]))
            query = (query.astype(F32) * ec_ref[rows, lanes] - crossed).astype(BF)
            before = before_ref[item].astype(F32)
            both = [jnp.where(same, before, 0.0), jnp.where(same, turned(before), 0.0)]
            moved = halves(dot(query, jnp.concatenate(both, axis=1).astype(BF)))
            o_ref[rows, place] = local + moved[0]
            q1_ref[rows, place] = moved[1].astype(BF)
        return carry

    lax.fori_loop(0, length // CHUNK, chunk, 0)


def gates_side(gates, gain):
    return call(gates_kernel, [gates, gain.reshape(1, HEAD_DIM)], [(gates.shape, F32)])[0]


def queries_side(first, after, queries, decay, solved, before, grown):
    length, width = queries.shape
    shape = (length, width // 2)
    return call(
        functools.partial(queries_kernel, first),
        [queries, decay, solved, before, grown],
        [(shape, F32), (shape, BF)],
        far=[after],
    )


def chained(earlier, later, same):
    later = later.astype(F32)
    step = jnp.where(same, turned(later), 0.0).astype(BF)
    return dot(step, earlier.astype(BF)) + jnp.where(same, later, 0.0)


def chip_kernel(own_ref, other_ref, out_ref, kept_ref):
    kept_ref[...] = other_ref[...]
    row, col = places()
    same = (col < HEAD_DIM) == (row < HEAD_DIM)
    core = lax.axis_index(SP[2])
    count = out_ref.shape[0]
    for p in range(count):
        mine = own_ref[core * count + p]
        theirs = other_ref[core * count + p]
        first = jnp.where(core == 0, mine, theirs)
        second = jnp.where(core == 0, theirs, mine)
        out_ref[p] = chained(first, second, same).astype(BF)


def row_kernel(after_ref, *rest):
    parts, (total_ref, before_ref, all_ref) = rest[:-3], rest[-3:]
    row, col = places()
    same = (col < HEAD_DIM) == (row < HEAD_DIM)
    place = lax.axis_index(SP[1])
    size = len(parts)
    for k, part in enumerate(parts):
        all_ref[lax.rem(place - k + size, size)] = part[...]
    for p in range(total_ref.shape[0]):
        run = all_ref[0, p].astype(F32)
        inside = jnp.where(place == 0, jnp.where((row ^ col) == HEAD_DIM, 1.0, 0.0), run)
        for k in range(1, size):
            run = chained(run, all_ref[k, p], same)
            inside = jnp.where(k < place, run, inside)
        before_ref[p] = inside.astype(BF)
        total_ref[p] = run.astype(BF)


def plane_kernel(after_ref, before_ref, *rest):
    parts, out_ref = rest[:-1], rest[-1]
    row, col = places()
    same = (col < HEAD_DIM) == (row < HEAD_DIM)
    place = lax.axis_index(SP[0])
    for p in range(out_ref.shape[0]):
        state = jnp.zeros((PAIR, PAIR), F32)
        for k in range(len(parts), 0, -1):
            later = jnp.where(same, chained(state, parts[k - 1][p], same), 0.0)
            state = jnp.where(k <= place, later, state)
        state = chained(state, before_ref[p], same)
        out_ref[p] = jnp.where(same, state, 0.0).astype(BF)


def state_ahead(total, meanwhile, then):
    plane, line, core = SP
    swap = [(0, 1), (1, 0)]
    half = (total.shape[0] // 2, PAIR, PAIR)
    other = lax.ppermute(total, core, swap)
    chip, other = call(chip_kernel, [total, other], [(half, BF), (total.shape, BF)])
    size = lax.axis_size(line)
    lines = [chip] + [lax.ppermute(chip, line, ring(size, k)) for k in range(1, size)]
    early = meanwhile(chip)
    whole, before = call(
        row_kernel, lines, [(half, BF), (half, BF)], [pltpu.VMEM((size, *half), BF)], far=[early[1]]
    )
    size = lax.axis_size(plane)
    planes = [lax.ppermute(whole, plane, ring(size, k)) for k in range(1, size)]
    late = then(whole)
    (state,) = call(plane_kernel, [before] + planes, [(half, BF)], far=[late[1]])
    return early, late, (other, state, lax.ppermute(state, core, swap))


def mixed_kernel(
    o0_ref, q0_ref, o1_ref, q1_ref,
    first_ref, mine_ref, theirs_ref, gate_ref, w_ref, *rest,
):
    out_refs, (mixed_ref, state_ref) = rest[:-2], rest[-2:]
    row, col = places()
    same = (col < HEAD_DIM) == (row < HEAD_DIM)
    ones = jnp.where(same, 1.0, 0.0).astype(BF)
    length, width = gate_ref.shape
    size = len(out_refs)
    block = length // size
    core = lax.axis_index(SP[2])
    turn = lax.axis_index("tp")
    half = mine_ref.shape[0]
    state_ref[pl.ds(core * half, half)] = mine_ref[...]
    state_ref[pl.ds((1 - core) * half, half)] = theirs_ref[...]
    for p in range(width // PAIR):
        lanes = slice(p * PAIR, (p + 1) * PAIR)
        state = state_ref[p].astype(F32)
        later = jnp.where(same, chained(state, first_ref[p], same), 0.0)
        state = jnp.where(core == 0, state, later).astype(BF)
        o_ref, q_ref = ((o0_ref, q0_ref), (o1_ref, q1_ref))[p // half]
        place = slice((p % half) * PAIR, (p % half + 1) * PAIR)
        out = o_ref[:, place] + dot(q_ref[:, place], state)
        mean = half_sums(out * out, ones) * (1.0 / HEAD_DIM)
        out = (out * lax.rsqrt(mean + EPSILON) * gate_ref[:, lanes]).astype(BF)
        for k in range(size):
            start = pl.multiple_of(lax.rem(k - turn + size, size) * block, 32)
            mixed_ref[pl.ds(start, block), lanes] = out[k * block : (k + 1) * block, :]
    for n in range(w_ref.shape[1] // STRIP):
        here = slice(n * STRIP, (n + 1) * STRIP)
        got = dot(mixed_ref[...], w_ref[:, here])
        for k, out_ref in enumerate(out_refs):
            out_ref[:, here] = got[k * block : (k + 1) * block, :].astype(out_ref.dtype)


def mixed_and_projected(size, early, late, states, gate, w_out):
    length, width = gate.shape
    return call(
        mixed_kernel,
        [*early, *late, *states, gate, w_out],
        [((length // size, w_out.shape[1]), BF if k else F32) for k in range(size)],
        [pltpu.VMEM((length, width), BF), pltpu.VMEM((width // PAIR, PAIR, PAIR), BF)],
    )


def norm_kernel(stream_ref, gain_ref, *rest):
    parts, (middle_ref, normed_ref) = rest[:-2], rest[-2:]
    projected = parts[0][...]
    for part in parts[1:]:
        projected = projected + part[...].astype(F32)
    middle = (stream_ref[...].astype(F32) + projected).astype(BF)
    middle_ref[...] = middle
    middle = middle.astype(F32)
    mean = jnp.mean(middle * middle, axis=-1, keepdims=True)
    normed_ref[...] = (middle * lax.rsqrt(mean + EPSILON) * gain_ref[...]).astype(BF)


def normed_rows(stream, gain, parts):
    return call(
        norm_kernel, [stream, gain.reshape(1, -1), *parts], [(stream.shape, BF), (stream.shape, BF)]
    )


def activated(rows, gate, up):
    got = dot(rows, jnp.concatenate([gate, up], axis=1))
    width = gate.shape[1]
    return (silu(got[:, :width]) * got[:, width:]).astype(BF)


def product_nt(a, b):
    even = a.shape[1] // 256 * 256
    return dot_nt(a[:, :even], b[:, :even]) + dot_nt(a[:, even:], b[:, even:])


TILE = 128
STRIP = 256
AHEAD = 3
UP_GROUPS = (1, 2, 4, 4)
DOWN_GROUPS = (8,)


def first_channels_kernel(count, w_ref, *rest):
    parts, out_refs = rest[:count], rest[count : 2 * count]
    gate_ref, up_ref, down_ref, rows_ref, hidden_ref, in_sems, down_sems = rest[2 * count :]
    width, hidden = gate_ref.shape
    block = parts[0].shape[0]
    groups, spans = [], []
    for many, spread in ((hidden // TILE, UP_GROUPS), (width // STRIP, DOWN_GROUPS)):
        assert sum(spread) == many
        starts = [sum(spread[:k]) for k in range(len(spread))]
        spans.append([range(start, start + n) for start, n in zip(starts, spread)])
    for g, tiles in enumerate(spans[0]):
        here = pl.ds(tiles[0] * TILE, len(tiles) * TILE)
        group = []
        for k, ref in enumerate((gate_ref, up_ref)):
            from_ref = w_ref.at[:, pl.ds(k * hidden + tiles[0] * TILE, len(tiles) * TILE)]
            group.append(pltpu.make_async_copy(from_ref, ref.at[:, here], in_sems.at[k, g]))
        groups.append(group)
    for g, strips in enumerate(spans[1]):
        here = pl.ds(strips[0] * STRIP, len(strips) * STRIP)
        from_ref = w_ref.at[here, pl.ds(2 * hidden, hidden)]
        groups.append([pltpu.make_async_copy(from_ref, down_ref.at[here, :], down_sems.at[g])])

    def begin(g):
        if g < len(groups):
            for copy in groups[g]:
                copy.start()

    def arrived(g):
        for copy in groups[g]:
            copy.wait()
        begin(g + AHEAD)

    for g in range(AHEAD):
        begin(g)
    for k, part in enumerate(parts):
        rows_ref[k * block : (k + 1) * block, :] = part[...]
    for g, tiles in enumerate(spans[0]):
        arrived(g)
        for j in tiles:
            here = slice(j * TILE, (j + 1) * TILE)
            hidden_ref[:, here] = activated(rows_ref[...], gate_ref[:, here], up_ref[:, here])
    for g, strips in enumerate(spans[1]):
        arrived(len(spans[0]) + g)
        for n in strips:
            here = slice(n * STRIP, (n + 1) * STRIP)
            got = product_nt(hidden_ref[...], down_ref[here, :])
            for k, out_ref in enumerate(out_refs):
                out_ref[:, here] = got[k * block : (k + 1) * block, :].astype(BF)


def first_channels(weights, parts, hidden):
    block, width = parts[0].shape
    count = len(parts)
    out = call(
        functools.partial(first_channels_kernel, count),
        parts,
        [((block, width), BF)] * count + [((width, hidden), BF)] * 3,
        [
            pltpu.VMEM((block * count, width), BF),
            pltpu.VMEM((block * count, hidden), BF),
            pltpu.SemaphoreType.DMA((2, len(UP_GROUPS))),
            pltpu.SemaphoreType.DMA((len(DOWN_GROUPS),)),
        ],
        far=[pltpu.with_memory_space_constraint(weights, pltpu.HBM)],
    )
    return out[:count], out[count:]


def more_channels_kernel(own_ref, upper_ref, lower_ref, gate_ref, up_ref, down_ref, *rest):
    out_refs, hidden_ref = rest[:-1], rest[-1]
    block = own_ref.shape[0]
    rows = jnp.concatenate([own_ref[...], upper_ref[...], lower_ref[...]], axis=0)
    for j in range(gate_ref.shape[1] // TILE):
        here = slice(j * TILE, (j + 1) * TILE)
        hidden_ref[:, here] = activated(rows, gate_ref[:, here], up_ref[:, here])
    for n in range(down_ref.shape[0] // STRIP):
        here = slice(n * STRIP, (n + 1) * STRIP)
        got = product_nt(hidden_ref[...], down_ref[here, :])
        for k, out_ref in enumerate(out_refs):
            out_ref[:, here] = got[k * block : (k + 1) * block, :].astype(BF)


def more_channels(rows, projections):
    block, width = rows[0].shape
    return call(
        more_channels_kernel,
        [*rows, *projections],
        [((block, width), BF)] * 2,
        [pltpu.VMEM((2 * block, projections[0].shape[1]), BF)],
    )


def last_kernel(middle_ref, *rest):
    parts, out_ref = rest[:-1], rest[-1]
    total = parts[0][...].astype(F32)
    for part in parts[1:]:
        total = total + part[...].astype(F32)
    out_ref[...] = (middle_ref[...].astype(F32) + 0.5 * total).astype(BF)


def last_sum(middle, parts):
    near = [pltpu.with_memory_space_constraint(x, pltpu.VMEM) for x in [middle, *parts]]
    return pl.pallas_call(
        last_kernel,
        in_specs=[FULL] * len(near),
        out_specs=FULL,
        out_shape=jax.ShapeDtypeStruct(middle.shape, BF),
        compiler_params=pltpu.CompilerParams(vmem_limit_bytes=16 << 20),
        name="last_sum",
    )(*near)


def per_device(
    queries,
    keys,
    values,
    gates,
    decay_pre,
    beta_pre,
    out_gain,
    w_out,
    stream,
    norm_gain,
    w_gate,
    w_up,
    w_down,
):
    hidden = w_gate.shape[1]
    weights = packed([w_gate, w_up, w_down.T])
    weights = lax.all_gather(weights, SP, axis=0, tiled=True)
    size = lax.axis_size("tp")
    before, total, solved, decay, grown = keys_side(keys, values, beta_pre, decay_pre)
    gate = gates_side(gates, out_gain)
    pairs = queries.shape[1] // PAIR
    early, late, states = state_ahead(
        total,
        lambda x: queries_side(0, x, queries, decay, solved, before, grown),
        lambda x: queries_side(pairs // 2, x, queries, decay, solved, before, grown),
    )
    parts = mixed_and_projected(size, early, late, states, gate, w_out)
    parts = [parts[0]] + [lax.ppermute(parts[k], "tp", ring(size, k)) for k in (1, 2, 3)]
    middle, normed = normed_rows(stream, norm_gain, parts)
    right = lax.ppermute(normed, "tp", ring(size, 1))
    left = lax.ppermute(normed, "tp", ring(size, -1))
    half = normed.shape[0] // 2
    across = [
        lax.ppermute(right[:half], "tp", ring(size, 1)),
        lax.ppermute(left[half:], "tp", ring(size, -1)),
    ]
    sums, projections = first_channels(weights, [right, left], hidden)
    back = [lax.ppermute(sums[0], "tp", ring(size, -1))]
    back.append(lax.ppermute(sums[1], "tp", ring(size, 1)))
    own, last = more_channels([normed, *across], projections)
    back.append(lax.ppermute(last, "tp", ring(size, 2)))
    return last_sum(middle, [own] + back)


def solution(mesh):
    finer = Mesh(mesh.devices.reshape(4, 4, 2, mesh.shape["tp"]), SP_TP)
    placed = (
        P(SP, "tp"),
        P(SP, "tp"),
        P(SP, "tp"),
        P(SP, "tp"),
        P("tp", SP),
        P("tp", SP),
        P(),
        P("tp", None),
        P(SP_TP, None),
        P(),
        P(SP, "tp"),
        P(SP, "tp"),
        P("tp", SP),
    )
    return jax.shard_map(
        per_device, mesh=finer, in_specs=placed, out_specs=P(SP_TP, None), check_vma=False
    )
```

```python
import functools

import jax
import jax.numpy as jnp
from jax import lax
from jax.experimental import pallas as pl
from jax.experimental.pallas import tpu as pltpu
from jax.sharding import Mesh
from jax.sharding import PartitionSpec as P


HEAD_DIM = 64
PAIR = 2 * HEAD_DIM
CHUNK = 128
SP = ("sp_0", "sp_1", "sp_2")
SP_TP = ("sp_0", "sp_1", "sp_2", "tp")
EPSILON = 1e-06
BF = jnp.bfloat16
F32 = jnp.float32
NT = (((1,), (1,)), ((), ()))


FULL = pl.BlockSpec(memory_space=pltpu.VMEM)
FAR = pl.BlockSpec(memory_space=pl.ANY)


def call(kernel, arrays, shapes, scratch=(), far=(), mib=16):
    near = [pltpu.with_memory_space_constraint(x, pltpu.VMEM) for x in arrays]
    return pl.pallas_call(
        kernel,
        in_specs=[FAR] * len(far) + [FULL] * len(near),
        out_specs=[FULL] * len(shapes),
        out_shape=[pltpu.VMEM(shape, dtype) for shape, dtype in shapes],
        scratch_shapes=scratch,
        compiler_params=pltpu.CompilerParams(vmem_limit_bytes=mib << 20),
    )(*far, *near)


def ring(size, k):
    return [(i, (i + k) % size) for i in range(size)]


def dot(a, b):
    return jnp.dot(a, b, preferred_element_type=F32)


def dot_nt(a, b):
    return lax.dot_general(a, b, NT, preferred_element_type=F32)


def silu(x):
    return x / (1.0 + jnp.exp(-x))


def places():
    row = lax.broadcasted_iota(jnp.int32, (PAIR, PAIR), 0)
    col = lax.broadcasted_iota(jnp.int32, (PAIR, PAIR), 1)
    return row, col


def half_sums(squares, ones):
    high = squares.astype(BF)
    low = (squares - high.astype(F32)).astype(BF)
    return dot(high, ones) + dot(low, ones)


def softplus(x):
    small = jnp.exp(-jnp.abs(x))
    series = small * (1.0 - small * (0.5 - small * (1.0 / 3.0 - 0.25 * small)))
    return jnp.maximum(x, 0.0) + jnp.where(small < 0.015, series, jnp.log(1.0 + small))


def turned(z):
    return pltpu.roll(z, HEAD_DIM, 1)


def split_three(x):
    high = x.astype(BF)
    rest = x - high.astype(F32)
    middle = rest.astype(BF)
    return jnp.concatenate([high, middle], axis=1), (rest - middle.astype(F32)).astype(BF)


def side_by_side(pair):
    zero = jnp.zeros_like(pair[0])
    upper = jnp.concatenate([pair[0], zero], axis=1)
    lower = jnp.concatenate([zero, pair[1]], axis=1)
    return jnp.concatenate([upper, lower], axis=0)


def halves(x):
    return x[:, :CHUNK], x[:, CHUNK:]


def keys_kernel(
    k_far_ref, v_far_ref, beta_far_ref, decay_far_ref,
    before_ref, total_ref, y_ref, d_ref, ec_ref,
    l_ref, x_ref, r_ref, f_ref, k_ref, v_ref, beta_ref, decay_ref, sems,
):
    length, width = k_ref.shape
    rate_copies = [
        pltpu.make_async_copy(decay_far_ref, decay_ref, sems.at[0]),
        pltpu.make_async_copy(beta_far_ref, beta_ref, sems.at[1]),
    ]
    row_copies = []
    for c in range(length // CHUNK):
        rows = pl.ds(c * CHUNK, CHUNK)
        for k, (far_ref, ref) in enumerate(((k_far_ref, k_ref), (v_far_ref, v_ref))):
            sem = sems.at[2 + 2 * c + k]
            row_copies.append(pltpu.make_async_copy(far_ref.at[rows], ref.at[rows], sem))
    for copy in rate_copies + row_copies:
        copy.start()
    row, col = places()
    left = col < HEAD_DIM
    top = row < HEAD_DIM
    same = left == top
    ones = jnp.where(same, 1.0, 0.0).astype(BF)
    inclusive = row >= col
    strict = row > col
    differ = row ^ col
    eye = jnp.where(row == col, 1.0, 0.0)
    off_eye = differ == HEAD_DIM
    pairs = width // PAIR
    heads = 2 * pairs
    steps = length // CHUNK

    def stacked(x):
        return jnp.concatenate([x[:, c * CHUNK : (c + 1) * CHUNK] for c in range(steps)], axis=0)

    for copy in rate_copies + row_copies:
        copy.wait()
    rates = split_three(stacked(-softplus(decay_ref[...])))
    strength = split_three(stacked(1.0 / (1.0 + jnp.exp(-beta_ref[...]))))
    triangle = jnp.where(inclusive, 1.0, 0.0).astype(BF)
    eye_bf = eye.astype(BF)
    triangle_two = jnp.concatenate([triangle, triangle], axis=1)
    cum_row = dot_nt(rates[0], triangle_two) + dot_nt(rates[1], triangle)
    cum_col = dot_nt(triangle_two, rates[0]) + dot_nt(triangle, rates[1])
    beta_col = dot_nt(jnp.concatenate([eye_bf, eye_bf], axis=1), strength[0])
    beta_col = beta_col + dot_nt(eye_bf, strength[1])

    ends = []
    for c in range(steps):
        rows = slice(c * CHUNK, (c + 1) * CHUNK)
        for p in range(pairs):
            lanes = slice(p * PAIR, (p + 1) * PAIR)
            item = c * pairs + p
            key = silu(k_ref[rows, lanes].astype(F32))
            key = (key * lax.rsqrt(half_sums(key * key, ones) + EPSILON)).astype(BF)
            y_ref[item, :, 2 * PAIR :] = key
            key_f = key.astype(F32)
            first = c * heads + 2 * p
            cums = [cum_col[:, h : h + 1] for h in (first, first + 1)]
            betas = [beta_col[:, h : h + 1] for h in (first, first + 1)]
            cum = jnp.where(left, cums[0], cums[1])
            beta = jnp.where(left, betas[0], betas[1])
            grown = jnp.exp(cum)
            ec_ref[rows, lanes] = grown
            strong = turned(key_f * (beta * grown))
            value = silu(v_ref[rows, lanes].astype(F32)) * beta
            r_ref[item, :, :CHUNK] = jnp.where(left, value, strong).astype(BF)
            r_ref[item, :, CHUNK:] = jnp.where(left, strong, value).astype(BF)
            fade = jnp.exp(cum[CHUNK - 1 : CHUNK, :] - cum)
            f_ref[item] = (key_f * fade).T.astype(BF)
            last = [jnp.exp(x[CHUNK - 1 : CHUNK, :]) for x in cums]
            ends.append(jnp.where(off_eye, jnp.where(top, last[0], last[1]), 0.0))
            owns = [jnp.where(left, key_f, 0.0), jnp.where(left, 0.0, key_f)]
            inner = dot_nt(key, jnp.concatenate(owns, axis=0).astype(BF))
            for s in range(2):
                part = slice(s * CHUNK, (s + 1) * CHUNK)
                gap = cums[s] - cum_row[first + s : first + s + 1, :]
                decay = jnp.where(inclusive, jnp.exp(gap), 0.0)
                d_ref[item, :, part] = decay.astype(BF)
                lower = jnp.where(strict, inner[:, part] * decay * betas[s], 0.0)
                l_ref[item, :, part] = lower.astype(BF)
                x_ref[item, :, part] = (eye - jnp.where(differ == 1, lower, 0.0)).astype(BF)

    items = steps * pairs

    for power in range(1, 7):
        mask = jnp.where((differ >> power) == 1, 1.0, 0.0).astype(BF)
        parts = []
        for i in range(items):
            block = side_by_side([part * mask for part in halves(l_ref[i])])
            parts.append(dot(x_ref[i], block).astype(BF))
        for i in range(items):
            x = x_ref[i]
            x_ref[i] = x - dot(parts[i], side_by_side(halves(x))).astype(BF)

    runs = [None] * pairs
    for c in range(steps):
        for p in range(pairs):
            item = c * pairs + p
            y = dot(x_ref[item], side_by_side(halves(r_ref[item]))).astype(BF)
            y_ref[item, :, : 2 * PAIR] = y
            z = jnp.where(top, *halves(dot(f_ref[item], y)))
            z = jnp.where(same, z, ends[item] - z)
            if c == 0:
                before_ref[item] = jnp.where(off_eye, 1.0, 0.0).astype(BF)
                runs[p] = z.astype(BF)
            else:
                before_ref[item] = runs[p]
                step = jnp.where(same, turned(z), 0.0).astype(BF)
                runs[p] = (dot(step, runs[p]) + jnp.where(same, z, 0.0)).astype(BF)
    for p in range(pairs):
        total_ref[p] = runs[p]


def keys_side(keys, values, beta_pre, decay_pre):
    length, width = keys.shape
    pairs = width // PAIR
    steps = length // CHUNK
    items = steps * pairs
    wide = pltpu.VMEM((items, CHUNK, 2 * CHUNK), BF)
    return call(
        keys_kernel,
        [],
        [
            ((items, PAIR, PAIR), BF),
            ((pairs, PAIR, PAIR), BF),
            ((items, CHUNK, 3 * PAIR), BF),
            ((items, CHUNK, 2 * CHUNK), BF),
            ((length, width), F32),
        ],
        [
            wide,
            wide,
            wide,
            pltpu.VMEM((items, PAIR, CHUNK), BF),
            pltpu.VMEM((length, width), BF),
            pltpu.VMEM((length, width), BF),
            pltpu.VMEM(beta_pre.shape, F32),
            pltpu.VMEM(beta_pre.shape, F32),
            pltpu.SemaphoreType.DMA((2 + 2 * steps,)),
        ],
        far=[
            pltpu.with_memory_space_constraint(x, pltpu.HBM)
            for x in (keys, values, beta_pre, decay_pre)
        ],
    )


def gates_kernel(gates_ref, gain_ref, gate_ref):
    gain = jnp.concatenate([gain_ref[...], gain_ref[...]], axis=1)
    for p in range(gates_ref.shape[1] // PAIR):
        lanes = slice(p * PAIR, (p + 1) * PAIR)
        gate_ref[:, lanes] = silu(gates_ref[:, lanes].astype(F32)) * gain


def queries_kernel(first, after_ref, q_ref, d_ref, y_ref, before_ref, ec_ref, o_ref, q1_ref):
    row, col = places()
    left = col < HEAD_DIM
    same = left == (row < HEAD_DIM)
    ones = jnp.where(same, 1.0, 0.0).astype(BF)
    length, width = o_ref.shape
    pairs = q_ref.shape[1] // PAIR

    def chunk(c, carry):
        rows = pl.ds(pl.multiple_of(c * CHUNK, CHUNK), CHUNK)
        for p in range(first, first + width // PAIR):
            lanes = slice(p * PAIR, (p + 1) * PAIR)
            place = slice((p - first) * PAIR, (p - first + 1) * PAIR)
            item = c * pairs + p
            query = silu(q_ref[rows, lanes].astype(F32))
            query = query * lax.rsqrt(half_sums(query * query, ones) + EPSILON)
            query = (query * HEAD_DIM ** (-0.5)).astype(BF)
            key_f = y_ref[item, :, 2 * PAIR :].astype(F32)
            owns = [jnp.where(left, key_f, 0.0), jnp.where(left, 0.0, key_f)]
            inside = dot_nt(query, jnp.concatenate(owns, axis=0).astype(BF))
            inside = (inside * d_ref[item].astype(F32)).astype(BF)
            got = halves(dot(inside, side_by_side(halves(y_ref[item, :, : 2 * PAIR]))))
            local = jnp.where(left, got[0], got[1])
            crossed = turned(jnp.where(left, got[1], got[0]))
            query = (query.astype(F32) * ec_ref[rows, lanes] - crossed).astype(BF)
            before = before_ref[item].astype(F32)
            both = [jnp.where(same, before, 0.0), jnp.where(same, turned(before), 0.0)]
            moved = halves(dot(query, jnp.concatenate(both, axis=1).astype(BF)))
            o_ref[rows, place] = local + moved[0]
            q1_ref[rows, place] = moved[1].astype(BF)
        return carry

    lax.fori_loop(0, length // CHUNK, chunk, 0)


def gates_side(gates, gain):
    return call(gates_kernel, [gates, gain.reshape(1, HEAD_DIM)], [(gates.shape, F32)])[0]


def queries_side(first, after, queries, decay, solved, before, grown):
    length, width = queries.shape
    shape = (length, width // 2)
    return call(
        functools.partial(queries_kernel, first),
        [queries, decay, solved, before, grown],
        [(shape, F32), (shape, BF)],
        far=[after],
    )


def chained(earlier, later, same):
    later = later.astype(F32)
    step = jnp.where(same, turned(later), 0.0).astype(BF)
    return dot(step, earlier.astype(BF)) + jnp.where(same, later, 0.0)


def chip_kernel(own_ref, other_ref, out_ref, kept_ref):
    kept_ref[...] = other_ref[...]
    row, col = places()
    same = (col < HEAD_DIM) == (row < HEAD_DIM)
    core = lax.axis_index(SP[2])
    count = out_ref.shape[0]
    for p in range(count):
        mine = own_ref[core * count + p]
        theirs = other_ref[core * count + p]
        first = jnp.where(core == 0, mine, theirs)
        second = jnp.where(core == 0, theirs, mine)
        out_ref[p] = chained(first, second, same).astype(BF)


def row_kernel(after_ref, *rest):
    parts, (total_ref, before_ref, all_ref) = rest[:-3], rest[-3:]
    row, col = places()
    same = (col < HEAD_DIM) == (row < HEAD_DIM)
    place = lax.axis_index(SP[1])
    size = len(parts)
    for k, part in enumerate(parts):
        all_ref[lax.rem(place - k + size, size)] = part[...]
    for p in range(total_ref.shape[0]):
        run = all_ref[0, p].astype(F32)
        inside = jnp.where(place == 0, jnp.where((row ^ col) == HEAD_DIM, 1.0, 0.0), run)
        for k in range(1, size):
            run = chained(run, all_ref[k, p], same)
            inside = jnp.where(k < place, run, inside)
        before_ref[p] = inside.astype(BF)
        total_ref[p] = run.astype(BF)


def plane_kernel(after_ref, before_ref, *rest):
    parts, out_ref = rest[:-1], rest[-1]
    row, col = places()
    same = (col < HEAD_DIM) == (row < HEAD_DIM)
    place = lax.axis_index(SP[0])
    for p in range(out_ref.shape[0]):
        state = jnp.zeros((PAIR, PAIR), F32)
        for k in range(len(parts), 0, -1):
            later = jnp.where(same, chained(state, parts[k - 1][p], same), 0.0)
            state = jnp.where(k <= place, later, state)
        state = chained(state, before_ref[p], same)
        out_ref[p] = jnp.where(same, state, 0.0).astype(BF)


def state_ahead(total, meanwhile, then):
    plane, line, core = SP
    swap = [(0, 1), (1, 0)]
    half = (total.shape[0] // 2, PAIR, PAIR)
    other = lax.ppermute(total, core, swap)
    chip, other = call(chip_kernel, [total, other], [(half, BF), (total.shape, BF)])
    size = lax.axis_size(line)
    lines = [chip] + [lax.ppermute(chip, line, ring(size, k)) for k in range(1, size)]
    early = meanwhile(chip)
    whole, before = call(
        row_kernel, lines, [(half, BF), (half, BF)], [pltpu.VMEM((size, *half), BF)], far=[early[1]]
    )
    size = lax.axis_size(plane)
    planes = [lax.ppermute(whole, plane, ring(size, k)) for k in range(1, size)]
    late = then(whole)
    (state,) = call(plane_kernel, [before] + planes, [(half, BF)], far=[late[1]])
    return early, late, (other, state, lax.ppermute(state, core, swap))


def mixed_kernel(
    o0_ref, q0_ref, o1_ref, q1_ref,
    first_ref, mine_ref, theirs_ref, gate_ref, w_ref, *rest,
):
    out_refs, (mixed_ref, state_ref) = rest[:-2], rest[-2:]
    row, col = places()
    same = (col < HEAD_DIM) == (row < HEAD_DIM)
    ones = jnp.where(same, 1.0, 0.0).astype(BF)
    length, width = gate_ref.shape
    size = len(out_refs)
    block = length // size
    core = lax.axis_index(SP[2])
    turn = lax.axis_index("tp")
    half = mine_ref.shape[0]
    state_ref[pl.ds(core * half, half)] = mine_ref[...]
    state_ref[pl.ds((1 - core) * half, half)] = theirs_ref[...]
    for p in range(width // PAIR):
        lanes = slice(p * PAIR, (p + 1) * PAIR)
        state = state_ref[p].astype(F32)
        later = jnp.where(same, chained(state, first_ref[p], same), 0.0)
        state = jnp.where(core == 0, state, later).astype(BF)
        o_ref, q_ref = ((o0_ref, q0_ref), (o1_ref, q1_ref))[p // half]
        place = slice((p % half) * PAIR, (p % half + 1) * PAIR)
        out = o_ref[:, place] + dot(q_ref[:, place], state)
        mean = half_sums(out * out, ones) * (1.0 / HEAD_DIM)
        out = (out * lax.rsqrt(mean + EPSILON) * gate_ref[:, lanes]).astype(BF)
        for k in range(size):
            start = pl.multiple_of(lax.rem(k - turn + size, size) * block, 32)
            mixed_ref[pl.ds(start, block), lanes] = out[k * block : (k + 1) * block, :]
    for n in range(w_ref.shape[1] // STRIP):
        here = slice(n * STRIP, (n + 1) * STRIP)
        got = dot(mixed_ref[...], w_ref[:, here])
        for k, out_ref in enumerate(out_refs):
            out_ref[:, here] = got[k * block : (k + 1) * block, :].astype(out_ref.dtype)


def mixed_and_projected(size, early, late, states, gate, w_out):
    length, width = gate.shape
    return call(
        mixed_kernel,
        [*early, *late, *states, gate, w_out],
        [((length // size, w_out.shape[1]), BF if k else F32) for k in range(size)],
        [pltpu.VMEM((length, width), BF), pltpu.VMEM((width // PAIR, PAIR, PAIR), BF)],
    )


def norm_kernel(stream_ref, gain_ref, *rest):
    parts, (middle_ref, normed_ref) = rest[:-2], rest[-2:]
    projected = parts[0][...]
    for part in parts[1:]:
        projected = projected + part[...].astype(F32)
    middle = (stream_ref[...].astype(F32) + projected).astype(BF)
    middle_ref[...] = middle
    middle = middle.astype(F32)
    mean = jnp.mean(middle * middle, axis=-1, keepdims=True)
    normed_ref[...] = (middle * lax.rsqrt(mean + EPSILON) * gain_ref[...]).astype(BF)


def normed_rows(stream, gain, parts):
    return call(
        norm_kernel, [stream, gain.reshape(1, -1), *parts], [(stream.shape, BF), (stream.shape, BF)]
    )


def activated(rows, gate, up):
    got = dot(rows, jnp.concatenate([gate, up], axis=1))
    width = gate.shape[1]
    return (silu(got[:, :width]) * got[:, width:]).astype(BF)


def product_nt(a, b):
    even = a.shape[1] // 256 * 256
    return dot_nt(a[:, :even], b[:, :even]) + dot_nt(a[:, even:], b[:, even:])


TILE = 128
STRIP = 256
AHEAD = 3
UP_GROUPS = (1, 2, 4, 4)
DOWN_GROUPS = (8,)


def first_channels_kernel(count, w_ref, *rest):
    parts, out_refs = rest[:count], rest[count : 2 * count]
    gate_ref, up_ref, down_ref, rows_ref, hidden_ref, in_sems, down_sems = rest[2 * count :]
    width, hidden = gate_ref.shape
    block = parts[0].shape[0]
    groups, spans = [], []
    for many, spread in ((hidden // TILE, UP_GROUPS), (width // STRIP, DOWN_GROUPS)):
        assert sum(spread) == many
        starts = [sum(spread[:k]) for k in range(len(spread))]
        spans.append([range(start, start + n) for start, n in zip(starts, spread)])
    for g, tiles in enumerate(spans[0]):
        here = pl.ds(tiles[0] * TILE, len(tiles) * TILE)
        group = []
        for k, ref in enumerate((gate_ref, up_ref)):
            from_ref = w_ref.at[:, pl.ds(k * hidden + tiles[0] * TILE, len(tiles) * TILE)]
            group.append(pltpu.make_async_copy(from_ref, ref.at[:, here], in_sems.at[k, g]))
        groups.append(group)
    for g, strips in enumerate(spans[1]):
        here = pl.ds(strips[0] * STRIP, len(strips) * STRIP)
        from_ref = w_ref.at[here, pl.ds(2 * hidden, hidden)]
        groups.append([pltpu.make_async_copy(from_ref, down_ref.at[here, :], down_sems.at[g])])

    def begin(g):
        if g < len(groups):
            for copy in groups[g]:
                copy.start()

    def arrived(g):
        for copy in groups[g]:
            copy.wait()
        begin(g + AHEAD)

    for g in range(AHEAD):
        begin(g)
    for k, part in enumerate(parts):
        rows_ref[k * block : (k + 1) * block, :] = part[...]
    for g, tiles in enumerate(spans[0]):
        arrived(g)
        for j in tiles:
            here = slice(j * TILE, (j + 1) * TILE)
            hidden_ref[:, here] = activated(rows_ref[...], gate_ref[:, here], up_ref[:, here])
    for g, strips in enumerate(spans[1]):
        arrived(len(spans[0]) + g)
        for n in strips:
            here = slice(n * STRIP, (n + 1) * STRIP)
            got = product_nt(hidden_ref[...], down_ref[here, :])
            for k, out_ref in enumerate(out_refs):
                out_ref[:, here] = got[k * block : (k + 1) * block, :].astype(BF)


def first_channels(weights, parts, hidden):
    block, width = parts[0].shape
    count = len(parts)
    out = call(
        functools.partial(first_channels_kernel, count),
        parts,
        [((block, width), BF)] * count + [((width, hidden), BF)] * 3,
        [
            pltpu.VMEM((block * count, width), BF),
            pltpu.VMEM((block * count, hidden), BF),
            pltpu.SemaphoreType.DMA((2, len(UP_GROUPS))),
            pltpu.SemaphoreType.DMA((len(DOWN_GROUPS),)),
        ],
        far=[pltpu.with_memory_space_constraint(weights, pltpu.HBM)],
    )
    return out[:count], out[count:]


def more_channels_kernel(own_ref, upper_ref, lower_ref, gate_ref, up_ref, down_ref, *rest):
    out_refs, hidden_ref = rest[:-1], rest[-1]
    block = own_ref.shape[0]
    rows = jnp.concatenate([own_ref[...], upper_ref[...], lower_ref[...]], axis=0)
    for j in range(gate_ref.shape[1] // TILE):
        here = slice(j * TILE, (j + 1) * TILE)
        hidden_ref[:, here] = activated(rows, gate_ref[:, here], up_ref[:, here])
    for n in range(down_ref.shape[0] // STRIP):
        here = slice(n * STRIP, (n + 1) * STRIP)
        got = product_nt(hidden_ref[...], down_ref[here, :])
        for k, out_ref in enumerate(out_refs):
            out_ref[:, here] = got[k * block : (k + 1) * block, :].astype(BF)


def more_channels(rows, projections):
    block, width = rows[0].shape
    return call(
        more_channels_kernel,
        [*rows, *projections],
        [((block, width), BF)] * 2,
        [pltpu.VMEM((2 * block, projections[0].shape[1]), BF)],
    )


def last_kernel(middle_ref, *rest):
    parts, out_ref = rest[:-1], rest[-1]
    total = parts[0][...].astype(F32)
    for part in parts[1:]:
        total = total + part[...].astype(F32)
    out_ref[...] = (middle_ref[...].astype(F32) + 0.5 * total).astype(BF)


def last_sum(middle, parts):
    near = [pltpu.with_memory_space_constraint(x, pltpu.VMEM) for x in [middle, *parts]]
    return pl.pallas_call(
        last_kernel,
        in_specs=[FULL] * len(near),
        out_specs=FULL,
        out_shape=jax.ShapeDtypeStruct(middle.shape, BF),
        compiler_params=pltpu.CompilerParams(vmem_limit_bytes=16 << 20),
        name="last_sum",
    )(*near)


def per_device(
    queries,
    keys,
    values,
    gates,
    decay_pre,
    beta_pre,
    out_gain,
    w_out,
    stream,
    norm_gain,
    w_gate,
    w_up,
    w_down,
):
    hidden = w_gate.shape[1]
    weights = jnp.concatenate([w_gate, w_up, w_down.T], axis=1)
    weights = lax.all_gather(weights, SP, axis=0, tiled=True)
    size = lax.axis_size("tp")
    before, total, solved, decay, grown = keys_side(keys, values, beta_pre, decay_pre)
    gate = gates_side(gates, out_gain)
    pairs = queries.shape[1] // PAIR
    early, late, states = state_ahead(
        total,
        lambda x: queries_side(0, x, queries, decay, solved, before, grown),
        lambda x: queries_side(pairs // 2, x, queries, decay, solved, before, grown),
    )
    parts = mixed_and_projected(size, early, late, states, gate, w_out)
    parts = [parts[0]] + [lax.ppermute(parts[k], "tp", ring(size, k)) for k in (1, 2, 3)]
    middle, normed = normed_rows(stream, norm_gain, parts)
    right = lax.ppermute(normed, "tp", ring(size, 1))
    left = lax.ppermute(normed, "tp", ring(size, -1))
    half = normed.shape[0] // 2
    across = [
        lax.ppermute(right[:half], "tp", ring(size, 1)),
        lax.ppermute(left[half:], "tp", ring(size, -1)),
    ]
    sums, projections = first_channels(weights, [right, left], hidden)
    back = [lax.ppermute(sums[0], "tp", ring(size, -1))]
    back.append(lax.ppermute(sums[1], "tp", ring(size, 1)))
    own, last = more_channels([normed, *across], projections)
    back.append(lax.ppermute(last, "tp", ring(size, 2)))
    return last_sum(middle, [own] + back)


def solution(mesh):
    finer = Mesh(mesh.devices.reshape(4, 4, 2, mesh.shape["tp"]), SP_TP)
    placed = (
        P(SP, "tp"),
        P(SP, "tp"),
        P(SP, "tp"),
        P(SP, "tp"),
        P("tp", SP),
        P("tp", SP),
        P(),
        P("tp", None),
        P(SP_TP, None),
        P(),
        P(SP, "tp"),
        P(SP, "tp"),
        P("tp", SP),
    )
    return jax.shard_map(
        per_device, mesh=finer, in_specs=placed, out_specs=P(SP_TP, None), check_vma=False
    )
```

```python
import functools

import jax
import jax.numpy as jnp
from jax import lax
from jax.experimental import pallas as pl
from jax.experimental.pallas import tpu as pltpu
from jax.sharding import Mesh
from jax.sharding import PartitionSpec as P


HEAD_DIM = 64
PAIR = 2 * HEAD_DIM
CHUNK = 128
SP = ("sp_0", "sp_1", "sp_2")
SP_TP = ("sp_0", "sp_1", "sp_2", "tp")
EPSILON = 1e-06
BF = jnp.bfloat16
F32 = jnp.float32
NT = (((1,), (1,)), ((), ()))


FULL = pl.BlockSpec(memory_space=pltpu.VMEM)
FAR = pl.BlockSpec(memory_space=pl.ANY)


def call(kernel, arrays, shapes, scratch=(), far=(), mib=16):
    near = [pltpu.with_memory_space_constraint(x, pltpu.VMEM) for x in arrays]
    return pl.pallas_call(
        kernel,
        in_specs=[FAR] * len(far) + [FULL] * len(near),
        out_specs=[FULL] * len(shapes),
        out_shape=[pltpu.VMEM(shape, dtype) for shape, dtype in shapes],
        scratch_shapes=scratch,
        compiler_params=pltpu.CompilerParams(vmem_limit_bytes=mib << 20),
    )(*far, *near)


def ring(size, k):
    return [(i, (i + k) % size) for i in range(size)]


def dot(a, b):
    return jnp.dot(a, b, preferred_element_type=F32)


def dot_nt(a, b):
    return lax.dot_general(a, b, NT, preferred_element_type=F32)


def silu(x):
    return x / (1.0 + jnp.exp(-x))


def places():
    row = lax.broadcasted_iota(jnp.int32, (PAIR, PAIR), 0)
    col = lax.broadcasted_iota(jnp.int32, (PAIR, PAIR), 1)
    return row, col


def half_sums(squares, ones):
    high = squares.astype(BF)
    low = (squares - high.astype(F32)).astype(BF)
    return dot(high, ones) + dot(low, ones)


def softplus(x):
    small = jnp.exp(-jnp.abs(x))
    series = small * (1.0 - small * (0.5 - small * (1.0 / 3.0 - 0.25 * small)))
    return jnp.maximum(x, 0.0) + jnp.where(small < 0.015, series, jnp.log(1.0 + small))


def turned(z):
    return pltpu.roll(z, HEAD_DIM, 1)


def split_three(x):
    high = x.astype(BF)
    rest = x - high.astype(F32)
    middle = rest.astype(BF)
    return jnp.concatenate([high, middle], axis=1), (rest - middle.astype(F32)).astype(BF)


def side_by_side(pair):
    zero = jnp.zeros_like(pair[0])
    upper = jnp.concatenate([pair[0], zero], axis=1)
    lower = jnp.concatenate([zero, pair[1]], axis=1)
    return jnp.concatenate([upper, lower], axis=0)


def halves(x):
    return x[:, :CHUNK], x[:, CHUNK:]


def keys_kernel(
    k_far_ref, v_far_ref, beta_far_ref, decay_far_ref,
    before_ref, total_ref, y_ref, d_ref, ec_ref,
    l_ref, x_ref, r_ref, f_ref, k_ref, v_ref, beta_ref, decay_ref, sems,
):
    length, width = k_ref.shape
    rate_copies = [
        pltpu.make_async_copy(decay_far_ref, decay_ref, sems.at[0]),
        pltpu.make_async_copy(beta_far_ref, beta_ref, sems.at[1]),
    ]
    row_copies = []
    for c in range(length // CHUNK):
        rows = pl.ds(c * CHUNK, CHUNK)
        for k, (far_ref, ref) in enumerate(((k_far_ref, k_ref), (v_far_ref, v_ref))):
            sem = sems.at[2 + 2 * c + k]
            row_copies.append(pltpu.make_async_copy(far_ref.at[rows], ref.at[rows], sem))
    for copy in rate_copies + row_copies:
        copy.start()
    row, col = places()
    left = col < HEAD_DIM
    top = row < HEAD_DIM
    same = left == top
    ones = jnp.where(same, 1.0, 0.0).astype(BF)
    inclusive = row >= col
    strict = row > col
    differ = row ^ col
    eye = jnp.where(row == col, 1.0, 0.0)
    off_eye = differ == HEAD_DIM
    pairs = width // PAIR
    heads = 2 * pairs
    steps = length // CHUNK

    def stacked(x):
        return jnp.concatenate([x[:, c * CHUNK : (c + 1) * CHUNK] for c in range(steps)], axis=0)

    for copy in rate_copies + row_copies:
        copy.wait()
    rates = split_three(stacked(-softplus(decay_ref[...])))
    strength = split_three(stacked(1.0 / (1.0 + jnp.exp(-beta_ref[...]))))
    triangle = jnp.where(inclusive, 1.0, 0.0).astype(BF)
    eye_bf = eye.astype(BF)
    triangle_two = jnp.concatenate([triangle, triangle], axis=1)
    cum_row = dot_nt(rates[0], triangle_two) + dot_nt(rates[1], triangle)
    cum_col = dot_nt(triangle_two, rates[0]) + dot_nt(triangle, rates[1])
    beta_col = dot_nt(jnp.concatenate([eye_bf, eye_bf], axis=1), strength[0])
    beta_col = beta_col + dot_nt(eye_bf, strength[1])

    ends = []
    for c in range(steps):
        rows = slice(c * CHUNK, (c + 1) * CHUNK)
        for p in range(pairs):
            lanes = slice(p * PAIR, (p + 1) * PAIR)
            item = c * pairs + p
            key = silu(k_ref[rows, lanes].astype(F32))
            key = (key * lax.rsqrt(half_sums(key * key, ones) + EPSILON)).astype(BF)
            y_ref[item, :, 2 * PAIR :] = key
            key_f = key.astype(F32)
            first = c * heads + 2 * p
            cums = [cum_col[:, h : h + 1] for h in (first, first + 1)]
            betas = [beta_col[:, h : h + 1] for h in (first, first + 1)]
            cum = jnp.where(left, cums[0], cums[1])
            beta = jnp.where(left, betas[0], betas[1])
            grown = jnp.exp(cum)
            ec_ref[rows, lanes] = grown
            strong = turned(key_f * (beta * grown))
            value = silu(v_ref[rows, lanes].astype(F32)) * beta
            r_ref[item, :, :CHUNK] = jnp.where(left, value, strong).astype(BF)
            r_ref[item, :, CHUNK:] = jnp.where(left, strong, value).astype(BF)
            fade = jnp.exp(cum[CHUNK - 1 : CHUNK, :] - cum)
            f_ref[item] = (key_f * fade).T.astype(BF)
            last = [jnp.exp(x[CHUNK - 1 : CHUNK, :]) for x in cums]
            ends.append(jnp.where(off_eye, jnp.where(top, last[0], last[1]), 0.0))
            owns = [jnp.where(left, key_f, 0.0), jnp.where(left, 0.0, key_f)]
            inner = dot_nt(key, jnp.concatenate(owns, axis=0).astype(BF))
            for s in range(2):
                part = slice(s * CHUNK, (s + 1) * CHUNK)
                gap = cums[s] - cum_row[first + s : first + s + 1, :]
                decay = jnp.where(inclusive, jnp.exp(gap), 0.0)
                d_ref[item, :, part] = decay.astype(BF)
                lower = jnp.where(strict, inner[:, part] * decay * betas[s], 0.0)
                l_ref[item, :, part] = lower.astype(BF)
                x_ref[item, :, part] = (eye - jnp.where(differ == 1, lower, 0.0)).astype(BF)

    items = steps * pairs

    for power in range(1, 7):
        mask = jnp.where((differ >> power) == 1, 1.0, 0.0).astype(BF)
        parts = []
        for i in range(items):
            block = side_by_side([part * mask for part in halves(l_ref[i])])
            parts.append(dot(x_ref[i], block).astype(BF))
        for i in range(items):
            x = x_ref[i]
            x_ref[i] = x - dot(parts[i], side_by_side(halves(x))).astype(BF)

    runs = [None] * pairs
    for c in range(steps):
        for p in range(pairs):
            item = c * pairs + p
            y = dot(x_ref[item], side_by_side(halves(r_ref[item]))).astype(BF)
            y_ref[item, :, : 2 * PAIR] = y
            z = jnp.where(top, *halves(dot(f_ref[item], y)))
            z = jnp.where(same, z, ends[item] - z)
            if c == 0:
                before_ref[item] = jnp.where(off_eye, 1.0, 0.0).astype(BF)
                runs[p] = z.astype(BF)
            else:
                before_ref[item] = runs[p]
                step = jnp.where(same, turned(z), 0.0).astype(BF)
                runs[p] = (dot(step, runs[p]) + jnp.where(same, z, 0.0)).astype(BF)
    for p in range(pairs):
        total_ref[p] = runs[p]


def keys_side(keys, values, beta_pre, decay_pre):
    length, width = keys.shape
    pairs = width // PAIR
    steps = length // CHUNK
    items = steps * pairs
    wide = pltpu.VMEM((items, CHUNK, 2 * CHUNK), BF)
    return call(
        keys_kernel,
        [],
        [
            ((items, PAIR, PAIR), BF),
            ((pairs, PAIR, PAIR), BF),
            ((items, CHUNK, 3 * PAIR), BF),
            ((items, CHUNK, 2 * CHUNK), BF),
            ((length, width), F32),
        ],
        [
            wide,
            wide,
            wide,
            pltpu.VMEM((items, PAIR, CHUNK), BF),
            pltpu.VMEM((length, width), BF),
            pltpu.VMEM((length, width), BF),
            pltpu.VMEM(beta_pre.shape, F32),
            pltpu.VMEM(beta_pre.shape, F32),
            pltpu.SemaphoreType.DMA((2 + 2 * steps,)),
        ],
        far=[
            pltpu.with_memory_space_constraint(x, pltpu.HBM)
            for x in (keys, values, beta_pre, decay_pre)
        ],
    )


def gates_kernel(gates_ref, gain_ref, gate_ref):
    gain = jnp.concatenate([gain_ref[...], gain_ref[...]], axis=1)
    for p in range(gates_ref.shape[1] // PAIR):
        lanes = slice(p * PAIR, (p + 1) * PAIR)
        gate_ref[:, lanes] = silu(gates_ref[:, lanes].astype(F32)) * gain


def queries_kernel(first, after_ref, q_ref, d_ref, y_ref, before_ref, ec_ref, o_ref, q1_ref):
    row, col = places()
    left = col < HEAD_DIM
    same = left == (row < HEAD_DIM)
    ones = jnp.where(same, 1.0, 0.0).astype(BF)
    length, width = o_ref.shape
    pairs = q_ref.shape[1] // PAIR

    def chunk(c, carry):
        rows = pl.ds(pl.multiple_of(c * CHUNK, CHUNK), CHUNK)
        for p in range(first, first + width // PAIR):
            lanes = slice(p * PAIR, (p + 1) * PAIR)
            place = slice((p - first) * PAIR, (p - first + 1) * PAIR)
            item = c * pairs + p
            query = silu(q_ref[rows, lanes].astype(F32))
            query = query * lax.rsqrt(half_sums(query * query, ones) + EPSILON)
            query = (query * HEAD_DIM ** (-0.5)).astype(BF)
            key_f = y_ref[item, :, 2 * PAIR :].astype(F32)
            owns = [jnp.where(left, key_f, 0.0), jnp.where(left, 0.0, key_f)]
            inside = dot_nt(query, jnp.concatenate(owns, axis=0).astype(BF))
            inside = (inside * d_ref[item].astype(F32)).astype(BF)
            got = halves(dot(inside, side_by_side(halves(y_ref[item, :, : 2 * PAIR]))))
            local = jnp.where(left, got[0], got[1])
            crossed = turned(jnp.where(left, got[1], got[0]))
            query = (query.astype(F32) * ec_ref[rows, lanes] - crossed).astype(BF)
            before = before_ref[item].astype(F32)
            both = [jnp.where(same, before, 0.0), jnp.where(same, turned(before), 0.0)]
            moved = halves(dot(query, jnp.concatenate(both, axis=1).astype(BF)))
            o_ref[rows, place] = local + moved[0]
            q1_ref[rows, place] = moved[1].astype(BF)
        return carry

    lax.fori_loop(0, length // CHUNK, chunk, 0)


def gates_side(gates, gain):
    return call(gates_kernel, [gates, gain.reshape(1, HEAD_DIM)], [(gates.shape, F32)])[0]


def queries_side(first, after, queries, decay, solved, before, grown):
    length, width = queries.shape
    shape = (length, width // 2)
    return call(
        functools.partial(queries_kernel, first),
        [queries, decay, solved, before, grown],
        [(shape, F32), (shape, BF)],
        far=[after],
    )


def chained(earlier, later, same):
    later = later.astype(F32)
    step = jnp.where(same, turned(later), 0.0).astype(BF)
    return dot(step, earlier.astype(BF)) + jnp.where(same, later, 0.0)


def chip_kernel(own_ref, other_ref, out_ref, kept_ref):
    kept_ref[...] = other_ref[...]
    row, col = places()
    same = (col < HEAD_DIM) == (row < HEAD_DIM)
    core = lax.axis_index(SP[2])
    count = out_ref.shape[0]
    for p in range(count):
        mine = own_ref[core * count + p]
        theirs = other_ref[core * count + p]
        first = jnp.where(core == 0, mine, theirs)
        second = jnp.where(core == 0, theirs, mine)
        out_ref[p] = chained(first, second, same).astype(BF)


def row_kernel(after_ref, *rest):
    parts, (total_ref, before_ref, all_ref) = rest[:-3], rest[-3:]
    row, col = places()
    same = (col < HEAD_DIM) == (row < HEAD_DIM)
    place = lax.axis_index(SP[1])
    size = len(parts)
    for k, part in enumerate(parts):
        all_ref[lax.rem(place - k + size, size)] = part[...]
    for p in range(total_ref.shape[0]):
        run = all_ref[0, p].astype(F32)
        inside = jnp.where(place == 0, jnp.where((row ^ col) == HEAD_DIM, 1.0, 0.0), run)
        for k in range(1, size):
            run = chained(run, all_ref[k, p], same)
            inside = jnp.where(k < place, run, inside)
        before_ref[p] = inside.astype(BF)
        total_ref[p] = run.astype(BF)


def plane_kernel(after_ref, before_ref, *rest):
    parts, out_ref = rest[:-1], rest[-1]
    row, col = places()
    same = (col < HEAD_DIM) == (row < HEAD_DIM)
    place = lax.axis_index(SP[0])
    for p in range(out_ref.shape[0]):
        state = jnp.zeros((PAIR, PAIR), F32)
        for k in range(len(parts), 0, -1):
            later = jnp.where(same, chained(state, parts[k - 1][p], same), 0.0)
            state = jnp.where(k <= place, later, state)
        state = chained(state, before_ref[p], same)
        out_ref[p] = jnp.where(same, state, 0.0).astype(BF)


def state_ahead(total, meanwhile, then):
    plane, line, core = SP
    swap = [(0, 1), (1, 0)]
    half = (total.shape[0] // 2, PAIR, PAIR)
    other = lax.ppermute(total, core, swap)
    chip, other = call(chip_kernel, [total, other], [(half, BF), (total.shape, BF)])
    size = lax.axis_size(line)
    lines = [chip] + [lax.ppermute(chip, line, ring(size, k)) for k in range(1, size)]
    early = meanwhile(chip)
    whole, before = call(
        row_kernel, lines, [(half, BF), (half, BF)], [pltpu.VMEM((size, *half), BF)], far=[early[1]]
    )
    size = lax.axis_size(plane)
    planes = [lax.ppermute(whole, plane, ring(size, k)) for k in range(1, size)]
    late = then(whole)
    (state,) = call(plane_kernel, [before] + planes, [(half, BF)], far=[late[1]])
    return early, late, (other, state, lax.ppermute(state, core, swap))


def mixed_kernel(
    o0_ref, q0_ref, o1_ref, q1_ref,
    first_ref, mine_ref, theirs_ref, gate_ref, w_ref, *rest,
):
    out_refs, (mixed_ref, state_ref) = rest[:-2], rest[-2:]
    row, col = places()
    same = (col < HEAD_DIM) == (row < HEAD_DIM)
    ones = jnp.where(same, 1.0, 0.0).astype(BF)
    length, width = gate_ref.shape
    size = len(out_refs)
    block = length // size
    core = lax.axis_index(SP[2])
    turn = lax.axis_index("tp")
    half = mine_ref.shape[0]
    state_ref[pl.ds(core * half, half)] = mine_ref[...]
    state_ref[pl.ds((1 - core) * half, half)] = theirs_ref[...]
    for p in range(width // PAIR):
        lanes = slice(p * PAIR, (p + 1) * PAIR)
        state = state_ref[p].astype(F32)
        later = jnp.where(same, chained(state, first_ref[p], same), 0.0)
        state = jnp.where(core == 0, state, later).astype(BF)
        o_ref, q_ref = ((o0_ref, q0_ref), (o1_ref, q1_ref))[p // half]
        place = slice((p % half) * PAIR, (p % half + 1) * PAIR)
        out = o_ref[:, place] + dot(q_ref[:, place], state)
        mean = half_sums(out * out, ones) * (1.0 / HEAD_DIM)
        out = (out * lax.rsqrt(mean + EPSILON) * gate_ref[:, lanes]).astype(BF)
        for k in range(size):
            start = pl.multiple_of(lax.rem(k - turn + size, size) * block, 32)
            mixed_ref[pl.ds(start, block), lanes] = out[k * block : (k + 1) * block, :]
    for n in range(w_ref.shape[1] // STRIP):
        here = slice(n * STRIP, (n + 1) * STRIP)
        got = dot(mixed_ref[...], w_ref[:, here])
        for k, out_ref in enumerate(out_refs):
            out_ref[:, here] = got[k * block : (k + 1) * block, :].astype(out_ref.dtype)


def mixed_and_projected(size, early, late, states, gate, w_out):
    length, width = gate.shape
    return call(
        mixed_kernel,
        [*early, *late, *states, gate, w_out],
        [((length // size, w_out.shape[1]), BF if k else F32) for k in range(size)],
        [pltpu.VMEM((length, width), BF), pltpu.VMEM((width // PAIR, PAIR, PAIR), BF)],
    )


def norm_kernel(stream_ref, gain_ref, *rest):
    parts, (middle_ref, normed_ref) = rest[:-2], rest[-2:]
    projected = parts[0][...]
    for part in parts[1:]:
        projected = projected + part[...].astype(F32)
    middle = (stream_ref[...].astype(F32) + projected).astype(BF)
    middle_ref[...] = middle
    middle = middle.astype(F32)
    mean = jnp.mean(middle * middle, axis=-1, keepdims=True)
    normed_ref[...] = (middle * lax.rsqrt(mean + EPSILON) * gain_ref[...]).astype(BF)


def normed_rows(stream, gain, parts):
    return call(
        norm_kernel, [stream, gain.reshape(1, -1), *parts], [(stream.shape, BF), (stream.shape, BF)]
    )


def tail_kernel(after_ref, far_ref, out_ref, sem):
    head = far_ref.shape[1] - out_ref.shape[1]
    copy = pltpu.make_async_copy(far_ref.at[:, pl.ds(head, out_ref.shape[1])], out_ref, sem)
    copy.start()
    copy.wait()


def planes_kernel(*refs):
    parts, out_ref = refs[:-1], refs[-1]
    place = lax.axis_index(SP[0])
    size = len(parts)
    for k, part in enumerate(parts):
        out_ref[lax.rem(place - k + size, size)] = part[...]


def lines_kernel(*refs):
    parts, out_ref = refs[:-1], refs[-1]
    place = lax.axis_index(SP[1])
    size = len(parts)
    for k, part in enumerate(parts):
        for plane in range(part.shape[0]):
            out_ref[plane, lax.rem(place - k + size, size)] = part[plane]


def tails_of_all(after, down):
    plane, line, core = SP
    shape = (down.shape[0], TAIL)
    far = [after, pltpu.with_memory_space_constraint(down, pltpu.HBM)]
    (tail,) = call(tail_kernel, [], [(shape, BF)], [pltpu.SemaphoreType.DMA(())], far=far)
    size = lax.axis_size(plane)
    parts = [tail] + [lax.ppermute(tail, plane, ring(size, k)) for k in range(1, size)]
    (tail,) = call(planes_kernel, parts, [((size, *shape), BF)])
    size = lax.axis_size(line)
    parts = [tail] + [lax.ppermute(tail, line, ring(size, k)) for k in range(1, size)]
    shape = (tail.shape[0], size, *shape)
    (tail,) = call(lines_kernel, parts, [(shape, BF)])
    return tail, lax.ppermute(tail, core, [(0, 1), (1, 0)])


def half_kernel(which, rows_ref, out_ref):
    half = out_ref.shape[0]
    out_ref[...] = rows_ref[which * half : (which + 1) * half, :]


def half_of(rows, which):
    shape = (rows.shape[0] // 2, rows.shape[1])
    return call(functools.partial(half_kernel, which), [rows], [(shape, BF)])[0]


def activated(rows, gate, up):
    got = dot(rows, jnp.concatenate([gate, up], axis=1))
    width = gate.shape[1]
    return (silu(got[:, :width]) * got[:, width:]).astype(BF)


def product_nt(a, b):
    even = a.shape[1] // 256 * 256
    return dot_nt(a[:, :even], b[:, :even]) + dot_nt(a[:, even:], b[:, even:])


TILE = 128
STRIP = 256
AHEAD = 3
UP_GROUPS = (1, 2, 4, 4)
DOWN_GROUPS = (8,)
TAIL = 512


def first_channels_kernel(count, w_ref, *rest):
    parts, tails, out_refs = rest[:count], rest[count : count + 2], rest[count + 2 : 2 * count + 2]
    gate_ref, up_ref, down_ref, rows_ref, hidden_ref, in_sems, down_sems = rest[2 * count + 2 :]
    width, hidden = gate_ref.shape
    head = hidden - TAIL
    block = parts[0].shape[0]
    groups, spans = [], []
    for many, spread in ((hidden // TILE, UP_GROUPS), (width // STRIP, DOWN_GROUPS)):
        assert sum(spread) == many
        starts = [sum(spread[:k]) for k in range(len(spread))]
        spans.append([range(start, start + n) for start, n in zip(starts, spread)])
    for g, tiles in enumerate(spans[0]):
        here = pl.ds(tiles[0] * TILE, len(tiles) * TILE)
        group = []
        for k, ref in enumerate((gate_ref, up_ref)):
            from_ref = w_ref.at[:, pl.ds(k * hidden + tiles[0] * TILE, len(tiles) * TILE)]
            group.append(pltpu.make_async_copy(from_ref, ref.at[:, here], in_sems.at[k, g]))
        groups.append(group)
    for g, strips in enumerate(spans[1]):
        here = pl.ds(strips[0] * STRIP, len(strips) * STRIP)
        from_ref = w_ref.at[here, pl.ds(2 * hidden, head)]
        to_ref = down_ref.at[here, pl.ds(0, head)]
        groups.append([pltpu.make_async_copy(from_ref, to_ref, down_sems.at[g])])

    def begin(g):
        if g < len(groups):
            for copy in groups[g]:
                copy.start()

    def arrived(g):
        for copy in groups[g]:
            copy.wait()
        begin(g + AHEAD)

    for g in range(AHEAD):
        begin(g)
    core = lax.axis_index(SP[2])
    for c, tail in enumerate(tails):
        planes, lines, rows, _ = tail.shape
        for i in range(planes * lines):
            start = pl.multiple_of((2 * i + (core if c == 0 else 1 - core)) * rows, rows)
            down_ref[pl.ds(start, rows), head:] = tail[i // lines, i % lines]
    for k, part in enumerate(parts):
        rows_ref[k * block : (k + 1) * block, :] = part[...]
    for g, tiles in enumerate(spans[0]):
        arrived(g)
        for j in tiles:
            here = slice(j * TILE, (j + 1) * TILE)
            hidden_ref[:, here] = activated(rows_ref[...], gate_ref[:, here], up_ref[:, here])
    for g, strips in enumerate(spans[1]):
        arrived(len(spans[0]) + g)
        for n in strips:
            here = slice(n * STRIP, (n + 1) * STRIP)
            got = product_nt(hidden_ref[...], down_ref[here, :])
            for k, out_ref in enumerate(out_refs):
                out_ref[:, here] = got[k * block : (k + 1) * block, :].astype(BF)


def first_channels(weights, parts, tails, hidden):
    block, width = parts[0].shape
    count = len(parts)
    out = call(
        functools.partial(first_channels_kernel, count),
        [*parts, *tails],
        [((block, width), BF)] * count + [((width, hidden), BF)] * 3,
        [
            pltpu.VMEM((block * count, width), BF),
            pltpu.VMEM((block * count, hidden), BF),
            pltpu.SemaphoreType.DMA((2, len(UP_GROUPS))),
            pltpu.SemaphoreType.DMA((len(DOWN_GROUPS),)),
        ],
        far=[pltpu.with_memory_space_constraint(weights, pltpu.HBM)],
    )
    return out[:count], out[count:]


def more_channels_kernel(own_ref, upper_ref, lower_ref, gate_ref, up_ref, down_ref, *rest):
    out_refs, hidden_ref = rest[:-1], rest[-1]
    block = own_ref.shape[0]
    rows = jnp.concatenate([own_ref[...], upper_ref[...], lower_ref[...]], axis=0)
    for j in range(gate_ref.shape[1] // TILE):
        here = slice(j * TILE, (j + 1) * TILE)
        hidden_ref[:, here] = activated(rows, gate_ref[:, here], up_ref[:, here])
    for n in range(down_ref.shape[0] // STRIP):
        here = slice(n * STRIP, (n + 1) * STRIP)
        got = product_nt(hidden_ref[...], down_ref[here, :])
        for k, out_ref in enumerate(out_refs):
            out_ref[:, here] = got[k * block : (k + 1) * block, :].astype(BF)


def more_channels(rows, projections):
    block, width = rows[0].shape
    return call(
        more_channels_kernel,
        [*rows, *projections],
        [((block, width), BF)] * 2,
        [pltpu.VMEM((2 * block, projections[0].shape[1]), BF)],
    )


def last_kernel(middle_ref, *rest):
    parts, out_ref = rest[:-1], rest[-1]
    total = parts[0][...].astype(F32)
    for part in parts[1:]:
        total = total + part[...].astype(F32)
    out_ref[...] = (middle_ref[...].astype(F32) + 0.5 * total).astype(BF)


def last_sum(middle, parts):
    near = [pltpu.with_memory_space_constraint(x, pltpu.VMEM) for x in [middle, *parts]]
    return pl.pallas_call(
        last_kernel,
        in_specs=[FULL] * len(near),
        out_specs=FULL,
        out_shape=jax.ShapeDtypeStruct(middle.shape, BF),
        compiler_params=pltpu.CompilerParams(vmem_limit_bytes=16 << 20),
        name="last_sum",
    )(*near)


def per_device(
    queries,
    keys,
    values,
    gates,
    decay_pre,
    beta_pre,
    out_gain,
    w_out,
    stream,
    norm_gain,
    w_gate,
    w_up,
    w_down,
):
    hidden = w_gate.shape[1]
    down = w_down.T
    weights = jnp.concatenate([w_gate, w_up, down[:, : hidden - TAIL]], axis=1)
    weights = lax.all_gather(weights, SP, axis=0, tiled=True)
    size = lax.axis_size("tp")
    before, total, solved, decay, grown = keys_side(keys, values, beta_pre, decay_pre)
    gate = gates_side(gates, out_gain)
    pairs = queries.shape[1] // PAIR
    early, late, states = state_ahead(
        total,
        lambda x: queries_side(0, x, queries, decay, solved, before, grown),
        lambda x: queries_side(pairs // 2, x, queries, decay, solved, before, grown),
    )
    parts = mixed_and_projected(size, early, late, states, gate, w_out)
    return feed_forward(
        parts, size, stream, norm_gain, weights, down, hidden
    )


def feed_forward(parts, size, stream, norm_gain, weights, down, hidden):
    got = [parts[0]]
    for k in range(1, size):
        got.append(lax.ppermute(parts[k], "tp", ring(size, k)))
    tails = tails_of_all(parts[1], down)
    middle, normed = normed_rows(stream, norm_gain, got)
    right = lax.ppermute(normed, "tp", ring(size, 1))
    left = lax.ppermute(normed, "tp", ring(size, -1))
    across = [
        lax.ppermute(half_of(right, 0), "tp", ring(size, 1)),
        lax.ppermute(half_of(left, 1), "tp", ring(size, -1)),
    ]
    sums, projections = first_channels(weights, [right, left], tails, hidden)
    back = [lax.ppermute(sums[0], "tp", ring(size, -1))]
    back.append(lax.ppermute(sums[1], "tp", ring(size, 1)))
    own, last = more_channels([normed, *across], projections)
    back.append(lax.ppermute(last, "tp", ring(size, 2)))
    return last_sum(middle, [own] + back)


def solution(mesh):
    finer = Mesh(mesh.devices.reshape(4, 4, 2, mesh.shape["tp"]), SP_TP)
    placed = (
        P(SP, "tp"),
        P(SP, "tp"),
        P(SP, "tp"),
        P(SP, "tp"),
        P("tp", SP),
        P("tp", SP),
        P(),
        P("tp", None),
        P(SP_TP, None),
        P(),
        P(SP, "tp"),
        P(SP, "tp"),
        P("tp", SP),
    )
    return jax.shard_map(
        per_device, mesh=finer, in_specs=placed, out_specs=P(SP_TP, None), check_vma=False
    )
```

```python
import functools

import jax
import jax.numpy as jnp
from jax import lax
from jax.experimental import pallas as pl
from jax.experimental.pallas import tpu as pltpu
from jax.sharding import Mesh
from jax.sharding import PartitionSpec as P

HEAD_DIM = 64
PAIR = 2 * HEAD_DIM
CHUNK = 128
SP = ("sp_0", "sp_1", "sp_2")
SP_TP = ("sp_0", "sp_1", "sp_2", "tp")
EPSILON = 1e-06
BF = jnp.bfloat16
F32 = jnp.float32
NT = (((1,), (1,)), ((), ()))


FULL = pl.BlockSpec(memory_space=pltpu.VMEM)
FAR = pl.BlockSpec(memory_space=pl.ANY)


def call(kernel, name, arrays, shapes, scratch=(), far=(), mib=16):
    near = [pltpu.with_memory_space_constraint(x, pltpu.VMEM) for x in arrays]
    return pl.pallas_call(
        kernel,
        in_specs=[FAR] * len(far) + [FULL] * len(near),
        out_specs=[FULL] * len(shapes),
        out_shape=[pltpu.VMEM(shape, dtype) for shape, dtype in shapes],
        scratch_shapes=scratch,
        compiler_params=pltpu.CompilerParams(vmem_limit_bytes=mib << 20),
        name=name,
    )(*far, *near)


def ring(size, k):
    return [(i, (i + k) % size) for i in range(size)]


def dot(a, b):
    return jnp.dot(a, b, preferred_element_type=F32)


def dot_nt(a, b):
    return lax.dot_general(a, b, NT, preferred_element_type=F32)


def silu(x):
    return x / (1.0 + jnp.exp(-x))


def places():
    row = lax.broadcasted_iota(jnp.int32, (PAIR, PAIR), 0)
    col = lax.broadcasted_iota(jnp.int32, (PAIR, PAIR), 1)
    return row, col


def half_sums(squares, ones):
    high = squares.astype(BF)
    low = (squares - high.astype(F32)).astype(BF)
    return dot(high, ones) + dot(low, ones)


def softplus(x):
    small = jnp.exp(-jnp.abs(x))
    series = small * (1.0 - small * (0.5 - small * (1.0 / 3.0 - 0.25 * small)))
    return jnp.maximum(x, 0.0) + jnp.where(small < 0.015, series, jnp.log(1.0 + small))


def turned(z):
    return pltpu.roll(z, HEAD_DIM, 1)


def split_three(x):
    high = x.astype(BF)
    rest = x - high.astype(F32)
    middle = rest.astype(BF)
    return jnp.concatenate([high, middle], axis=1), (rest - middle.astype(F32)).astype(BF)


def side_by_side(pair):
    zero = jnp.zeros_like(pair[0])
    upper = jnp.concatenate([pair[0], zero], axis=1)
    lower = jnp.concatenate([zero, pair[1]], axis=1)
    return jnp.concatenate([upper, lower], axis=0)


def halves(x):
    return x[:, :CHUNK], x[:, CHUNK:]


def keys_kernel(
    k_far_ref, v_far_ref, beta_far_ref, decay_far_ref,
    before_ref, total_ref, y_ref, d_ref, ec_ref,
    l_ref, x_ref, r_ref, f_ref, k_ref, v_ref, beta_ref, decay_ref, sems,
):
    length, width = k_ref.shape
    rate_copies = [
        pltpu.make_async_copy(decay_far_ref, decay_ref, sems.at[0]),
        pltpu.make_async_copy(beta_far_ref, beta_ref, sems.at[1]),
    ]
    row_copies = []
    for c in range(length // CHUNK):
        rows = pl.ds(c * CHUNK, CHUNK)
        for k, (far_ref, ref) in enumerate(((k_far_ref, k_ref), (v_far_ref, v_ref))):
            sem = sems.at[2 + 2 * c + k]
            row_copies.append(pltpu.make_async_copy(far_ref.at[rows], ref.at[rows], sem))
    for copy in rate_copies + row_copies:
        copy.start()
    row, col = places()
    left = col < HEAD_DIM
    top = row < HEAD_DIM
    same = left == top
    ones = jnp.where(same, 1.0, 0.0).astype(BF)
    inclusive = row >= col
    strict = row > col
    differ = row ^ col
    eye = jnp.where(row == col, 1.0, 0.0)
    off_eye = differ == HEAD_DIM
    pairs = width // PAIR
    heads = 2 * pairs
    steps = length // CHUNK

    def stacked(x):
        return jnp.concatenate([x[:, c * CHUNK : (c + 1) * CHUNK] for c in range(steps)], axis=0)

    for copy in rate_copies + row_copies:
        copy.wait()
    rates = split_three(stacked(-softplus(decay_ref[...])))
    strength = split_three(stacked(1.0 / (1.0 + jnp.exp(-beta_ref[...]))))
    triangle = jnp.where(inclusive, 1.0, 0.0).astype(BF)
    eye_bf = eye.astype(BF)
    triangle_two = jnp.concatenate([triangle, triangle], axis=1)
    cum_row = dot_nt(rates[0], triangle_two) + dot_nt(rates[1], triangle)
    cum_col = dot_nt(triangle_two, rates[0]) + dot_nt(triangle, rates[1])
    beta_col = dot_nt(jnp.concatenate([eye_bf, eye_bf], axis=1), strength[0])
    beta_col = beta_col + dot_nt(eye_bf, strength[1])

    ends = []
    for c in range(steps):
        rows = slice(c * CHUNK, (c + 1) * CHUNK)
        for p in range(pairs):
            lanes = slice(p * PAIR, (p + 1) * PAIR)
            item = c * pairs + p
            key = silu(k_ref[rows, lanes].astype(F32))
            key = (key * lax.rsqrt(half_sums(key * key, ones) + EPSILON)).astype(BF)
            y_ref[item, :, 2 * PAIR :] = key
            key_f = key.astype(F32)
            first = c * heads + 2 * p
            cums = [cum_col[:, h : h + 1] for h in (first, first + 1)]
            betas = [beta_col[:, h : h + 1] for h in (first, first + 1)]
            cum = jnp.where(left, cums[0], cums[1])
            beta = jnp.where(left, betas[0], betas[1])
            grown = jnp.exp(cum)
            ec_ref[rows, lanes] = grown
            strong = turned(key_f * (beta * grown))
            value = silu(v_ref[rows, lanes].astype(F32)) * beta
            r_ref[item, :, :CHUNK] = jnp.where(left, value, strong).astype(BF)
            r_ref[item, :, CHUNK:] = jnp.where(left, strong, value).astype(BF)
            fade = jnp.exp(cum[CHUNK - 1 : CHUNK, :] - cum)
            f_ref[item] = (key_f * fade).T.astype(BF)
            last = [jnp.exp(x[CHUNK - 1 : CHUNK, :]) for x in cums]
            ends.append(jnp.where(off_eye, jnp.where(top, last[0], last[1]), 0.0))
            owns = [jnp.where(left, key_f, 0.0), jnp.where(left, 0.0, key_f)]
            inner = dot_nt(key, jnp.concatenate(owns, axis=0).astype(BF))
            for s in range(2):
                part = slice(s * CHUNK, (s + 1) * CHUNK)
                gap = cums[s] - cum_row[first + s : first + s + 1, :]
                decay = jnp.where(inclusive, jnp.exp(gap), 0.0)
                d_ref[item, :, part] = decay.astype(BF)
                lower = jnp.where(strict, inner[:, part] * decay * betas[s], 0.0)
                l_ref[item, :, part] = lower.astype(BF)
                x_ref[item, :, part] = (eye - jnp.where(differ == 1, lower, 0.0)).astype(BF)

    items = steps * pairs

    for power in range(1, 7):
        mask = jnp.where((differ >> power) == 1, 1.0, 0.0).astype(BF)
        parts = []
        for i in range(items):
            block = side_by_side([part * mask for part in halves(l_ref[i])])
            parts.append(dot(x_ref[i], block).astype(BF))
        for i in range(items):
            x = x_ref[i]
            x_ref[i] = x - dot(parts[i], side_by_side(halves(x))).astype(BF)

    runs = [None] * pairs
    for c in range(steps):
        for p in range(pairs):
            item = c * pairs + p
            y = dot(x_ref[item], side_by_side(halves(r_ref[item]))).astype(BF)
            y_ref[item, :, : 2 * PAIR] = y
            z = jnp.where(top, *halves(dot(f_ref[item], y)))
            z = jnp.where(same, z, ends[item] - z)
            if c == 0:
                before_ref[item] = jnp.where(off_eye, 1.0, 0.0).astype(BF)
                runs[p] = z.astype(BF)
            else:
                before_ref[item] = runs[p]
                step = jnp.where(same, turned(z), 0.0).astype(BF)
                runs[p] = (dot(step, runs[p]) + jnp.where(same, z, 0.0)).astype(BF)
    for p in range(pairs):
        total_ref[p] = runs[p]


def keys_side(keys, values, beta_pre, decay_pre):
    length, width = keys.shape
    pairs = width // PAIR
    steps = length // CHUNK
    items = steps * pairs
    wide = pltpu.VMEM((items, CHUNK, 2 * CHUNK), BF)
    return call(
        keys_kernel,
        "keys_side",
        [],
        [
            ((items, PAIR, PAIR), BF),
            ((pairs, PAIR, PAIR), BF),
            ((items, CHUNK, 3 * PAIR), BF),
            ((items, CHUNK, 2 * CHUNK), BF),
            ((length, width), F32),
        ],
        [
            wide,
            wide,
            wide,
            pltpu.VMEM((items, PAIR, CHUNK), BF),
            pltpu.VMEM((length, width), BF),
            pltpu.VMEM((length, width), BF),
            pltpu.VMEM(beta_pre.shape, F32),
            pltpu.VMEM(beta_pre.shape, F32),
            pltpu.SemaphoreType.DMA((2 + 2 * steps,)),
        ],
        far=[
            pltpu.with_memory_space_constraint(x, pltpu.HBM)
            for x in (keys, values, beta_pre, decay_pre)
        ],
    )


def gates_kernel(gates_ref, gain_ref, gate_ref):
    gain = jnp.concatenate([gain_ref[...], gain_ref[...]], axis=1)
    for p in range(gates_ref.shape[1] // PAIR):
        lanes = slice(p * PAIR, (p + 1) * PAIR)
        gate_ref[:, lanes] = silu(gates_ref[:, lanes].astype(F32)) * gain


def queries_kernel(first, after_ref, q_ref, d_ref, y_ref, before_ref, ec_ref, o_ref, q1_ref):
    row, col = places()
    left = col < HEAD_DIM
    same = left == (row < HEAD_DIM)
    ones = jnp.where(same, 1.0, 0.0).astype(BF)
    length, width = o_ref.shape
    pairs = q_ref.shape[1] // PAIR

    def chunk(c, carry):
        rows = pl.ds(pl.multiple_of(c * CHUNK, CHUNK), CHUNK)
        for p in range(first, first + width // PAIR):
            lanes = slice(p * PAIR, (p + 1) * PAIR)
            place = slice((p - first) * PAIR, (p - first + 1) * PAIR)
            item = c * pairs + p
            query = silu(q_ref[rows, lanes].astype(F32))
            query = query * lax.rsqrt(half_sums(query * query, ones) + EPSILON)
            query = (query * HEAD_DIM ** (-0.5)).astype(BF)
            key_f = y_ref[item, :, 2 * PAIR :].astype(F32)
            owns = [jnp.where(left, key_f, 0.0), jnp.where(left, 0.0, key_f)]
            inside = dot_nt(query, jnp.concatenate(owns, axis=0).astype(BF))
            inside = (inside * d_ref[item].astype(F32)).astype(BF)
            got = halves(dot(inside, side_by_side(halves(y_ref[item, :, : 2 * PAIR]))))
            local = jnp.where(left, got[0], got[1])
            crossed = turned(jnp.where(left, got[1], got[0]))
            query = (query.astype(F32) * ec_ref[rows, lanes] - crossed).astype(BF)
            before = before_ref[item].astype(F32)
            both = [jnp.where(same, before, 0.0), jnp.where(same, turned(before), 0.0)]
            moved = halves(dot(query, jnp.concatenate(both, axis=1).astype(BF)))
            o_ref[rows, place] = local + moved[0]
            q1_ref[rows, place] = moved[1].astype(BF)
        return carry

    lax.fori_loop(0, length // CHUNK, chunk, 0)


def gates_side(gates, gain):
    return call(
        gates_kernel, "gates_side", [gates, gain.reshape(1, HEAD_DIM)], [(gates.shape, F32)]
    )[0]


def queries_side(first, after, queries, decay, solved, before, grown):
    length, width = queries.shape
    shape = (length, width // 2)
    return call(
        functools.partial(queries_kernel, first),
        "queries_side",
        [queries, decay, solved, before, grown],
        [(shape, F32), (shape, BF)],
        far=[after],
    )


def chained(earlier, later, same):
    later = later.astype(F32)
    step = jnp.where(same, turned(later), 0.0).astype(BF)
    return dot(step, earlier.astype(BF)) + jnp.where(same, later, 0.0)


def chip_kernel(own_ref, other_ref, out_ref, kept_ref):
    kept_ref[...] = other_ref[...]
    row, col = places()
    same = (col < HEAD_DIM) == (row < HEAD_DIM)
    core = lax.axis_index(SP[2])
    count = out_ref.shape[0]
    for p in range(count):
        mine = own_ref[core * count + p]
        theirs = other_ref[core * count + p]
        first = jnp.where(core == 0, mine, theirs)
        second = jnp.where(core == 0, theirs, mine)
        out_ref[p] = chained(first, second, same).astype(BF)


def row_kernel(after_ref, *rest):
    parts, (total_ref, before_ref, all_ref) = rest[:-3], rest[-3:]
    row, col = places()
    same = (col < HEAD_DIM) == (row < HEAD_DIM)
    place = lax.axis_index(SP[1])
    size = len(parts)
    for k, part in enumerate(parts):
        all_ref[lax.rem(place - k + size, size)] = part[...]
    for p in range(total_ref.shape[0]):
        run = all_ref[0, p].astype(F32)
        inside = jnp.where(place == 0, jnp.where((row ^ col) == HEAD_DIM, 1.0, 0.0), run)
        for k in range(1, size):
            run = chained(run, all_ref[k, p], same)
            inside = jnp.where(k < place, run, inside)
        before_ref[p] = inside.astype(BF)
        total_ref[p] = run.astype(BF)


def plane_kernel(after_ref, before_ref, *rest):
    parts, out_ref = rest[:-1], rest[-1]
    row, col = places()
    same = (col < HEAD_DIM) == (row < HEAD_DIM)
    place = lax.axis_index(SP[0])
    for p in range(out_ref.shape[0]):
        state = jnp.zeros((PAIR, PAIR), F32)
        for k in range(len(parts), 0, -1):
            later = jnp.where(same, chained(state, parts[k - 1][p], same), 0.0)
            state = jnp.where(k <= place, later, state)
        state = chained(state, before_ref[p], same)
        out_ref[p] = jnp.where(same, state, 0.0).astype(BF)


def state_ahead(total, meanwhile, then):
    plane, line, core = SP
    swap = [(0, 1), (1, 0)]
    half = (total.shape[0] // 2, PAIR, PAIR)
    other = lax.ppermute(total, core, swap)
    chip, other = call(
        chip_kernel, "chip_total", [total, other], [(half, BF), (total.shape, BF)]
    )
    size = lax.axis_size(line)
    lines = [chip] + [lax.ppermute(chip, line, ring(size, k)) for k in range(1, size)]
    early = meanwhile(chip)
    whole, before = call(
        row_kernel,
        "line_total",
        lines,
        [(half, BF), (half, BF)],
        [pltpu.VMEM((size, *half), BF)],
        far=[early[1]],
    )
    size = lax.axis_size(plane)
    planes = [lax.ppermute(whole, plane, ring(size, k)) for k in range(1, size)]
    late = then(whole)
    (state,) = call(
        plane_kernel, "plane_state", [before] + planes, [(half, BF)], far=[late[1]]
    )
    return early, late, (other, state, lax.ppermute(state, core, swap))


def mixed_kernel(
    o0_ref, q0_ref, o1_ref, q1_ref,
    first_ref, mine_ref, theirs_ref, gate_ref, w_ref, *rest,
):
    out_refs, (mixed_ref, state_ref) = rest[:-2], rest[-2:]
    row, col = places()
    same = (col < HEAD_DIM) == (row < HEAD_DIM)
    ones = jnp.where(same, 1.0, 0.0).astype(BF)
    length, width = gate_ref.shape
    size = len(out_refs)
    block = length // size
    core = lax.axis_index(SP[2])
    turn = lax.axis_index("tp")
    half = mine_ref.shape[0]
    state_ref[pl.ds(core * half, half)] = mine_ref[...]
    state_ref[pl.ds((1 - core) * half, half)] = theirs_ref[...]
    for p in range(width // PAIR):
        lanes = slice(p * PAIR, (p + 1) * PAIR)
        state = state_ref[p].astype(F32)
        later = jnp.where(same, chained(state, first_ref[p], same), 0.0)
        state = jnp.where(core == 0, state, later).astype(BF)
        o_ref, q_ref = ((o0_ref, q0_ref), (o1_ref, q1_ref))[p // half]
        place = slice((p % half) * PAIR, (p % half + 1) * PAIR)
        out = o_ref[:, place] + dot(q_ref[:, place], state)
        mean = half_sums(out * out, ones) * (1.0 / HEAD_DIM)
        out = (out * lax.rsqrt(mean + EPSILON) * gate_ref[:, lanes]).astype(BF)
        for k in range(size):
            start = pl.multiple_of(lax.rem(k - turn + size, size) * block, 32)
            mixed_ref[pl.ds(start, block), lanes] = out[k * block : (k + 1) * block, :]
    for n in range(w_ref.shape[1] // STRIP):
        here = slice(n * STRIP, (n + 1) * STRIP)
        got = dot(mixed_ref[...], w_ref[:, here])
        for k, out_ref in enumerate(out_refs):
            out_ref[:, here] = got[k * block : (k + 1) * block, :].astype(out_ref.dtype)


def mixed_and_projected(size, early, late, states, gate, w_out):
    length, width = gate.shape
    return call(
        mixed_kernel,
        "mixed_and_projected",
        [*early, *late, *states, gate, w_out],
        [((length // size, w_out.shape[1]), BF if k else F32) for k in range(size)],
        [pltpu.VMEM((length, width), BF), pltpu.VMEM((width // PAIR, PAIR, PAIR), BF)],
    )


def norm_kernel(stream_ref, gain_ref, *rest):
    parts, (middle_ref, normed_ref) = rest[:-2], rest[-2:]
    projected = parts[0][...]
    for part in parts[1:]:
        projected = projected + part[...].astype(F32)
    middle = (stream_ref[...].astype(F32) + projected).astype(BF)
    middle_ref[...] = middle
    middle = middle.astype(F32)
    mean = jnp.mean(middle * middle, axis=-1, keepdims=True)
    normed_ref[...] = (middle * lax.rsqrt(mean + EPSILON) * gain_ref[...]).astype(BF)


def normed_rows(stream, gain, parts):
    return call(
        norm_kernel,
        "normed_rows",
        [stream, gain.reshape(1, -1), *parts],
        [(stream.shape, BF), (stream.shape, BF)],
    )


def activated(rows, gate, up):
    got = dot(rows, jnp.concatenate([gate, up], axis=1))
    width = gate.shape[1]
    return (silu(got[:, :width]) * got[:, width:]).astype(BF)


def product_nt(a, b):
    even = a.shape[1] // 256 * 256
    return dot_nt(a[:, :even], b[:, :even]) + dot_nt(a[:, even:], b[:, even:])


TILE = 128
STRIP = 256
AHEAD = 3
UP_GROUPS = (1, 2, 4, 4)
DOWN_GROUPS = (8,)


def channels_kernel(w_ref, *rest):
    own_ref, right_ref, left_ref, upper_ref, lower_ref, out_ref = rest[:6]
    gate_ref, up_ref, down_ref, rows_ref, hidden_ref, in_sems, down_sems = rest[6:]
    width, hidden = gate_ref.shape
    size, block = out_ref.shape[:2]
    groups, spans = [], []
    for many, spread in ((hidden // TILE, UP_GROUPS), (width // STRIP, DOWN_GROUPS)):
        assert sum(spread) == many
        starts = [sum(spread[:k]) for k in range(len(spread))]
        spans.append([range(start, start + n) for start, n in zip(starts, spread)])
    for g, tiles in enumerate(spans[0]):
        here = pl.ds(tiles[0] * TILE, len(tiles) * TILE)
        group = []
        for k, ref in enumerate((gate_ref, up_ref)):
            from_ref = w_ref.at[:, pl.ds(k * hidden + tiles[0] * TILE, len(tiles) * TILE)]
            group.append(pltpu.make_async_copy(from_ref, ref.at[:, here], in_sems.at[k, g]))
        groups.append(group)
    for g, strips in enumerate(spans[1]):
        here = pl.ds(strips[0] * STRIP, len(strips) * STRIP)
        from_ref = w_ref.at[here, pl.ds(2 * hidden, hidden)]
        groups.append([pltpu.make_async_copy(from_ref, down_ref.at[here, :], down_sems.at[g])])

    def begin(g):
        if g < len(groups):
            for copy in groups[g]:
                copy.start()

    def arrived(g):
        for copy in groups[g]:
            copy.wait()
        begin(g + AHEAD)

    for g in range(AHEAD):
        begin(g)
    rows_ref[:block, :] = own_ref[...]
    rows_ref[block : 2 * block, :] = right_ref[...]
    rows_ref[2 * block : 3 * block, :] = left_ref[...]
    half = block // 2
    rows_ref[3 * block : 3 * block + half, :] = upper_ref[...]
    rows_ref[3 * block + half :, :] = lower_ref[...]
    place = lax.axis_index("tp")
    owners = [lax.rem(place + k, size) for k in (0, size - 1, 1, 2)]
    for g, tiles in enumerate(spans[0]):
        arrived(g)
        for j in tiles:
            here = slice(j * TILE, (j + 1) * TILE)
            hidden_ref[:, here] = activated(rows_ref[...], gate_ref[:, here], up_ref[:, here])
    for g, strips in enumerate(spans[1]):
        arrived(len(spans[0]) + g)
        for n in strips:
            here = slice(n * STRIP, (n + 1) * STRIP)
            got = product_nt(hidden_ref[...], down_ref[here, :]).astype(BF)
            for k, owner in enumerate(owners):
                out_ref[owner, :, here] = got[k * block : (k + 1) * block, :]


def channel_sums(weights, parts, hidden, size):
    block, width = parts[0].shape
    weight = pltpu.VMEM((width, hidden), BF)
    return call(
        channels_kernel,
        "channel_sums",
        parts,
        [((size, block, width), BF)],
        [
            weight,
            weight,
            weight,
            pltpu.VMEM((block * size, width), BF),
            pltpu.VMEM((block * size, hidden), BF),
            pltpu.SemaphoreType.DMA((2, len(UP_GROUPS))),
            pltpu.SemaphoreType.DMA((len(DOWN_GROUPS),)),
        ],
        far=[pltpu.with_memory_space_constraint(weights, pltpu.HBM)],
        mib=32,
    )[0]


def last_kernel(middle_ref, parts_ref, out_ref):
    total = parts_ref[0].astype(F32)
    for k in range(1, parts_ref.shape[0]):
        total = total + parts_ref[k].astype(F32)
    out_ref[...] = (middle_ref[...].astype(F32) + 0.5 * total).astype(BF)


def last_sum(middle, parts):
    near = [pltpu.with_memory_space_constraint(x, pltpu.VMEM) for x in (middle, parts)]
    return pl.pallas_call(
        last_kernel,
        in_specs=[FULL] * len(near),
        out_specs=FULL,
        out_shape=jax.ShapeDtypeStruct(middle.shape, BF),
        compiler_params=pltpu.CompilerParams(vmem_limit_bytes=16 << 20),
        name="last_sum",
    )(*near)


def per_device(
    queries,
    keys,
    values,
    gates,
    decay_pre,
    beta_pre,
    out_gain,
    w_out,
    stream,
    norm_gain,
    w_gate,
    w_up,
    w_down,
):
    hidden = w_gate.shape[1]
    weights = jnp.concatenate([w_gate, w_up, w_down.T], axis=1)
    weights = lax.all_gather(weights, SP, axis=0, tiled=True)
    size = lax.axis_size("tp")
    before, total, solved, decay, grown = keys_side(keys, values, beta_pre, decay_pre)
    gate = gates_side(gates, out_gain)
    pairs = queries.shape[1] // PAIR
    early, late, states = state_ahead(
        total,
        lambda x: queries_side(0, x, queries, decay, solved, before, grown),
        lambda x: queries_side(pairs // 2, x, queries, decay, solved, before, grown),
    )
    parts = mixed_and_projected(size, early, late, states, gate, w_out)
    parts = [parts[0]] + [lax.ppermute(parts[k], "tp", ring(size, k)) for k in (1, 2, 3)]
    middle, normed = normed_rows(stream, norm_gain, parts)
    right = lax.ppermute(normed, "tp", ring(size, 1))
    left = lax.ppermute(normed, "tp", ring(size, -1))
    half = normed.shape[0] // 2
    across = [
        lax.ppermute(right[:half], "tp", ring(size, 1)),
        lax.ppermute(left[half:], "tp", ring(size, -1)),
    ]
    sums = channel_sums(weights, [normed, right, left, *across], hidden, size)
    sums = lax.all_to_all(sums, "tp", 0, 0, tiled=True)
    return last_sum(middle, sums)


def solution(mesh):
    finer = Mesh(mesh.devices.reshape(4, 4, 2, mesh.shape["tp"]), SP_TP)
    placed = (
        P(SP, "tp"),
        P(SP, "tp"),
        P(SP, "tp"),
        P(SP, "tp"),
        P("tp", SP),
        P("tp", SP),
        P(),
        P("tp", None),
        P(SP_TP, None),
        P(),
        P(SP, "tp"),
        P(SP, "tp"),
        P("tp", SP),
    )
    return jax.shard_map(
        per_device, mesh=finer, in_specs=placed, out_specs=P(SP_TP, None), check_vma=False
    )
```

```python
import functools

import jax
import jax.numpy as jnp
from jax import lax
from jax.experimental import pallas as pl
from jax.experimental.pallas import tpu as pltpu
from jax.sharding import Mesh
from jax.sharding import PartitionSpec as P


HEAD_DIM = 64
PAIR = 2 * HEAD_DIM
CHUNK = 128
SP = ("sp_0", "sp_1", "sp_2")
SP_TP = ("sp_0", "sp_1", "sp_2", "tp")
EPSILON = 1e-06
BF = jnp.bfloat16
F32 = jnp.float32
NT = (((1,), (1,)), ((), ()))


FULL = pl.BlockSpec(memory_space=pltpu.VMEM)
FAR = pl.BlockSpec(memory_space=pl.ANY)


def call(kernel, arrays, shapes, scratch=(), far=(), mib=16):
    near = [pltpu.with_memory_space_constraint(x, pltpu.VMEM) for x in arrays]
    return pl.pallas_call(
        kernel,
        in_specs=[FAR] * len(far) + [FULL] * len(near),
        out_specs=[FULL] * len(shapes),
        out_shape=[pltpu.VMEM(shape, dtype) for shape, dtype in shapes],
        scratch_shapes=scratch,
        compiler_params=pltpu.CompilerParams(vmem_limit_bytes=mib << 20),
    )(*far, *near)


def ring(size, k):
    return [(i, (i + k) % size) for i in range(size)]


def dot(a, b):
    return jnp.dot(a, b, preferred_element_type=F32)


def dot_nt(a, b):
    return lax.dot_general(a, b, NT, preferred_element_type=F32)


def silu(x):
    return x / (1.0 + jnp.exp(-x))


def places():
    row = lax.broadcasted_iota(jnp.int32, (PAIR, PAIR), 0)
    col = lax.broadcasted_iota(jnp.int32, (PAIR, PAIR), 1)
    return row, col


def half_sums(squares, ones):
    high = squares.astype(BF)
    low = (squares - high.astype(F32)).astype(BF)
    return dot(high, ones) + dot(low, ones)


def softplus(x):
    small = jnp.exp(-jnp.abs(x))
    series = small * (1.0 - small * (0.5 - small * (1.0 / 3.0 - 0.25 * small)))
    return jnp.maximum(x, 0.0) + jnp.where(small < 0.015, series, jnp.log(1.0 + small))


def turned(z):
    return pltpu.roll(z, HEAD_DIM, 1)


def split_three(x):
    high = x.astype(BF)
    rest = x - high.astype(F32)
    middle = rest.astype(BF)
    return jnp.concatenate([high, middle], axis=1), (rest - middle.astype(F32)).astype(BF)


def side_by_side(pair):
    zero = jnp.zeros_like(pair[0])
    upper = jnp.concatenate([pair[0], zero], axis=1)
    lower = jnp.concatenate([zero, pair[1]], axis=1)
    return jnp.concatenate([upper, lower], axis=0)


def halves(x):
    return x[:, :CHUNK], x[:, CHUNK:]


def keys_kernel(
    k_far_ref, v_far_ref, beta_far_ref, decay_far_ref,
    before_ref, total_ref, y_ref, d_ref, ec_ref,
    l_ref, x_ref, r_ref, f_ref, k_ref, v_ref, beta_ref, decay_ref, sems,
):
    length, width = k_ref.shape
    rate_copies = [
        pltpu.make_async_copy(decay_far_ref, decay_ref, sems.at[0]),
        pltpu.make_async_copy(beta_far_ref, beta_ref, sems.at[1]),
    ]
    row_copies = []
    for c in range(length // CHUNK):
        rows = pl.ds(c * CHUNK, CHUNK)
        for k, (far_ref, ref) in enumerate(((k_far_ref, k_ref), (v_far_ref, v_ref))):
            sem = sems.at[2 + 2 * c + k]
            row_copies.append(pltpu.make_async_copy(far_ref.at[rows], ref.at[rows], sem))
    for copy in rate_copies + row_copies:
        copy.start()
    row, col = places()
    left = col < HEAD_DIM
    top = row < HEAD_DIM
    same = left == top
    ones = jnp.where(same, 1.0, 0.0).astype(BF)
    inclusive = row >= col
    strict = row > col
    differ = row ^ col
    eye = jnp.where(row == col, 1.0, 0.0)
    off_eye = differ == HEAD_DIM
    pairs = width // PAIR
    heads = 2 * pairs
    steps = length // CHUNK

    def stacked(x):
        return jnp.concatenate([x[:, c * CHUNK : (c + 1) * CHUNK] for c in range(steps)], axis=0)

    for copy in rate_copies + row_copies:
        copy.wait()
    rates = split_three(stacked(-softplus(decay_ref[...])))
    strength = split_three(stacked(1.0 / (1.0 + jnp.exp(-beta_ref[...]))))
    triangle = jnp.where(inclusive, 1.0, 0.0).astype(BF)
    eye_bf = eye.astype(BF)
    triangle_two = jnp.concatenate([triangle, triangle], axis=1)
    cum_row = dot_nt(rates[0], triangle_two) + dot_nt(rates[1], triangle)
    cum_col = dot_nt(triangle_two, rates[0]) + dot_nt(triangle, rates[1])
    beta_col = dot_nt(jnp.concatenate([eye_bf, eye_bf], axis=1), strength[0])
    beta_col = beta_col + dot_nt(eye_bf, strength[1])

    ends = []
    for c in range(steps):
        rows = slice(c * CHUNK, (c + 1) * CHUNK)
        for p in range(pairs):
            lanes = slice(p * PAIR, (p + 1) * PAIR)
            item = c * pairs + p
            key = silu(k_ref[rows, lanes].astype(F32))
            key = (key * lax.rsqrt(half_sums(key * key, ones) + EPSILON)).astype(BF)
            y_ref[item, :, 2 * PAIR :] = key
            key_f = key.astype(F32)
            first = c * heads + 2 * p
            cums = [cum_col[:, h : h + 1] for h in (first, first + 1)]
            betas = [beta_col[:, h : h + 1] for h in (first, first + 1)]
            cum = jnp.where(left, cums[0], cums[1])
            beta = jnp.where(left, betas[0], betas[1])
            grown = jnp.exp(cum)
            ec_ref[rows, lanes] = grown
            strong = turned(key_f * (beta * grown))
            value = silu(v_ref[rows, lanes].astype(F32)) * beta
            r_ref[item, :, :CHUNK] = jnp.where(left, value, strong).astype(BF)
            r_ref[item, :, CHUNK:] = jnp.where(left, strong, value).astype(BF)
            fade = jnp.exp(cum[CHUNK - 1 : CHUNK, :] - cum)
            f_ref[item] = (key_f * fade).T.astype(BF)
            last = [jnp.exp(x[CHUNK - 1 : CHUNK, :]) for x in cums]
            ends.append(jnp.where(off_eye, jnp.where(top, last[0], last[1]), 0.0))
            owns = [jnp.where(left, key_f, 0.0), jnp.where(left, 0.0, key_f)]
            inner = dot_nt(key, jnp.concatenate(owns, axis=0).astype(BF))
            for s in range(2):
                part = slice(s * CHUNK, (s + 1) * CHUNK)
                gap = cums[s] - cum_row[first + s : first + s + 1, :]
                decay = jnp.where(inclusive, jnp.exp(gap), 0.0)
                d_ref[item, :, part] = decay.astype(BF)
                lower = jnp.where(strict, inner[:, part] * decay * betas[s], 0.0)
                l_ref[item, :, part] = lower.astype(BF)
                x_ref[item, :, part] = (eye - jnp.where(differ == 1, lower, 0.0)).astype(BF)

    items = steps * pairs

    for power in range(1, 7):
        mask = jnp.where((differ >> power) == 1, 1.0, 0.0).astype(BF)
        parts = []
        for i in range(items):
            block = side_by_side([part * mask for part in halves(l_ref[i])])
            parts.append(dot(x_ref[i], block).astype(BF))
        for i in range(items):
            x = x_ref[i]
            x_ref[i] = x - dot(parts[i], side_by_side(halves(x))).astype(BF)

    runs = [None] * pairs
    for c in range(steps):
        for p in range(pairs):
            item = c * pairs + p
            y = dot(x_ref[item], side_by_side(halves(r_ref[item]))).astype(BF)
            y_ref[item, :, : 2 * PAIR] = y
            z = jnp.where(top, *halves(dot(f_ref[item], y)))
            z = jnp.where(same, z, ends[item] - z)
            if c == 0:
                before_ref[item] = jnp.where(off_eye, 1.0, 0.0).astype(BF)
                runs[p] = z.astype(BF)
            else:
                before_ref[item] = runs[p]
                step = jnp.where(same, turned(z), 0.0).astype(BF)
                runs[p] = (dot(step, runs[p]) + jnp.where(same, z, 0.0)).astype(BF)
    for p in range(pairs):
        total_ref[p] = runs[p]


def keys_side(keys, values, beta_pre, decay_pre):
    length, width = keys.shape
    pairs = width // PAIR
    steps = length // CHUNK
    items = steps * pairs
    wide = pltpu.VMEM((items, CHUNK, 2 * CHUNK), BF)
    return call(
        keys_kernel,
        [],
        [
            ((items, PAIR, PAIR), BF),
            ((pairs, PAIR, PAIR), BF),
            ((items, CHUNK, 3 * PAIR), BF),
            ((items, CHUNK, 2 * CHUNK), BF),
            ((length, width), F32),
        ],
        [
            wide,
            wide,
            wide,
            pltpu.VMEM((items, PAIR, CHUNK), BF),
            pltpu.VMEM((length, width), BF),
            pltpu.VMEM((length, width), BF),
            pltpu.VMEM(beta_pre.shape, F32),
            pltpu.VMEM(beta_pre.shape, F32),
            pltpu.SemaphoreType.DMA((2 + 2 * steps,)),
        ],
        far=[
            pltpu.with_memory_space_constraint(x, pltpu.HBM)
            for x in (keys, values, beta_pre, decay_pre)
        ],
    )


def gates_kernel(gates_ref, gain_ref, gate_ref):
    gain = jnp.concatenate([gain_ref[...], gain_ref[...]], axis=1)
    for p in range(gates_ref.shape[1] // PAIR):
        lanes = slice(p * PAIR, (p + 1) * PAIR)
        gate_ref[:, lanes] = silu(gates_ref[:, lanes].astype(F32)) * gain


def queries_kernel(first, after_ref, q_ref, d_ref, y_ref, before_ref, ec_ref, o_ref, q1_ref):
    row, col = places()
    left = col < HEAD_DIM
    same = left == (row < HEAD_DIM)
    ones = jnp.where(same, 1.0, 0.0).astype(BF)
    length, width = o_ref.shape
    pairs = q_ref.shape[1] // PAIR

    def chunk(c, carry):
        rows = pl.ds(pl.multiple_of(c * CHUNK, CHUNK), CHUNK)
        for p in range(first, first + width // PAIR):
            lanes = slice(p * PAIR, (p + 1) * PAIR)
            place = slice((p - first) * PAIR, (p - first + 1) * PAIR)
            item = c * pairs + p
            query = silu(q_ref[rows, lanes].astype(F32))
            query = query * lax.rsqrt(half_sums(query * query, ones) + EPSILON)
            query = (query * HEAD_DIM ** (-0.5)).astype(BF)
            key_f = y_ref[item, :, 2 * PAIR :].astype(F32)
            owns = [jnp.where(left, key_f, 0.0), jnp.where(left, 0.0, key_f)]
            inside = dot_nt(query, jnp.concatenate(owns, axis=0).astype(BF))
            inside = (inside * d_ref[item].astype(F32)).astype(BF)
            got = halves(dot(inside, side_by_side(halves(y_ref[item, :, : 2 * PAIR]))))
            local = jnp.where(left, got[0], got[1])
            crossed = turned(jnp.where(left, got[1], got[0]))
            query = (query.astype(F32) * ec_ref[rows, lanes] - crossed).astype(BF)
            before = before_ref[item].astype(F32)
            both = [jnp.where(same, before, 0.0), jnp.where(same, turned(before), 0.0)]
            moved = halves(dot(query, jnp.concatenate(both, axis=1).astype(BF)))
            o_ref[rows, place] = local + moved[0]
            q1_ref[rows, place] = moved[1].astype(BF)
        return carry

    lax.fori_loop(0, length // CHUNK, chunk, 0)


def gates_side(gates, gain):
    return call(gates_kernel, [gates, gain.reshape(1, HEAD_DIM)], [(gates.shape, F32)])[0]


def queries_side(first, after, queries, decay, solved, before, grown):
    length, width = queries.shape
    shape = (length, width // 2)
    return call(
        functools.partial(queries_kernel, first),
        [queries, decay, solved, before, grown],
        [(shape, F32), (shape, BF)],
        far=[after],
    )


def chained(earlier, later, same):
    later = later.astype(F32)
    step = jnp.where(same, turned(later), 0.0).astype(BF)
    return dot(step, earlier.astype(BF)) + jnp.where(same, later, 0.0)


def chip_kernel(own_ref, other_ref, out_ref, kept_ref):
    kept_ref[...] = other_ref[...]
    row, col = places()
    same = (col < HEAD_DIM) == (row < HEAD_DIM)
    core = lax.axis_index(SP[2])
    count = out_ref.shape[0]
    for p in range(count):
        mine = own_ref[core * count + p]
        theirs = other_ref[core * count + p]
        first = jnp.where(core == 0, mine, theirs)
        second = jnp.where(core == 0, theirs, mine)
        out_ref[p] = chained(first, second, same).astype(BF)


def row_kernel(after_ref, *rest):
    parts, (total_ref, before_ref, all_ref) = rest[:-3], rest[-3:]
    row, col = places()
    same = (col < HEAD_DIM) == (row < HEAD_DIM)
    place = lax.axis_index(SP[1])
    size = len(parts)
    for k, part in enumerate(parts):
        all_ref[lax.rem(place - k + size, size)] = part[...]
    for p in range(total_ref.shape[0]):
        run = all_ref[0, p].astype(F32)
        inside = jnp.where(place == 0, jnp.where((row ^ col) == HEAD_DIM, 1.0, 0.0), run)
        for k in range(1, size):
            run = chained(run, all_ref[k, p], same)
            inside = jnp.where(k < place, run, inside)
        before_ref[p] = inside.astype(BF)
        total_ref[p] = run.astype(BF)


def plane_kernel(after_ref, before_ref, *rest):
    parts, out_ref = rest[:-1], rest[-1]
    row, col = places()
    same = (col < HEAD_DIM) == (row < HEAD_DIM)
    place = lax.axis_index(SP[0])
    for p in range(out_ref.shape[0]):
        state = jnp.zeros((PAIR, PAIR), F32)
        for k in range(len(parts), 0, -1):
            later = jnp.where(same, chained(state, parts[k - 1][p], same), 0.0)
            state = jnp.where(k <= place, later, state)
        state = chained(state, before_ref[p], same)
        out_ref[p] = jnp.where(same, state, 0.0).astype(BF)


def state_ahead(total, meanwhile, then):
    plane, line, core = SP
    swap = [(0, 1), (1, 0)]
    half = (total.shape[0] // 2, PAIR, PAIR)
    other = lax.ppermute(total, core, swap)
    chip, other = call(chip_kernel, [total, other], [(half, BF), (total.shape, BF)])
    size = lax.axis_size(line)
    lines = [chip] + [lax.ppermute(chip, line, ring(size, k)) for k in range(1, size)]
    early = meanwhile(chip)
    whole, before = call(
        row_kernel, lines, [(half, BF), (half, BF)], [pltpu.VMEM((size, *half), BF)], far=[early[1]]
    )
    size = lax.axis_size(plane)
    planes = [lax.ppermute(whole, plane, ring(size, k)) for k in range(1, size)]
    late = then(whole)
    (state,) = call(plane_kernel, [before] + planes, [(half, BF)], far=[late[1]])
    return early, late, (other, state, lax.ppermute(state, core, swap))


def mixed_kernel(
    o0_ref, q0_ref, o1_ref, q1_ref,
    first_ref, mine_ref, theirs_ref, gate_ref, w_ref, *rest,
):
    out_refs, (mixed_ref, state_ref) = rest[:-2], rest[-2:]
    row, col = places()
    same = (col < HEAD_DIM) == (row < HEAD_DIM)
    ones = jnp.where(same, 1.0, 0.0).astype(BF)
    length, width = gate_ref.shape
    size = len(out_refs)
    block = length // size
    core = lax.axis_index(SP[2])
    turn = lax.axis_index("tp")
    half = mine_ref.shape[0]
    state_ref[pl.ds(core * half, half)] = mine_ref[...]
    state_ref[pl.ds((1 - core) * half, half)] = theirs_ref[...]
    for p in range(width // PAIR):
        lanes = slice(p * PAIR, (p + 1) * PAIR)
        state = state_ref[p].astype(F32)
        later = jnp.where(same, chained(state, first_ref[p], same), 0.0)
        state = jnp.where(core == 0, state, later).astype(BF)
        o_ref, q_ref = ((o0_ref, q0_ref), (o1_ref, q1_ref))[p // half]
        place = slice((p % half) * PAIR, (p % half + 1) * PAIR)
        out = o_ref[:, place] + dot(q_ref[:, place], state)
        mean = half_sums(out * out, ones) * (1.0 / HEAD_DIM)
        out = (out * lax.rsqrt(mean + EPSILON) * gate_ref[:, lanes]).astype(BF)
        for k in range(size):
            start = pl.multiple_of(lax.rem(k - turn + size, size) * block, 32)
            mixed_ref[pl.ds(start, block), lanes] = out[k * block : (k + 1) * block, :]
    for n in range(w_ref.shape[1] // STRIP):
        here = slice(n * STRIP, (n + 1) * STRIP)
        got = dot(mixed_ref[...], w_ref[:, here])
        for k, out_ref in enumerate(out_refs):
            out_ref[:, here] = got[k * block : (k + 1) * block, :].astype(out_ref.dtype)


def mixed_and_projected(size, early, late, states, gate, w_out):
    length, width = gate.shape
    return call(
        mixed_kernel,
        [*early, *late, *states, gate, w_out],
        [((length // size, w_out.shape[1]), BF if k else F32) for k in range(size)],
        [pltpu.VMEM((length, width), BF), pltpu.VMEM((width // PAIR, PAIR, PAIR), BF)],
    )


def norm_kernel(stream_ref, gain_ref, *rest):
    parts, (middle_ref, normed_ref) = rest[:-2], rest[-2:]
    projected = parts[0][...]
    for part in parts[1:]:
        projected = projected + part[...].astype(F32)
    middle = (stream_ref[...].astype(F32) + projected).astype(BF)
    middle_ref[...] = middle
    middle = middle.astype(F32)
    mean = jnp.mean(middle * middle, axis=-1, keepdims=True)
    normed_ref[...] = (middle * lax.rsqrt(mean + EPSILON) * gain_ref[...]).astype(BF)


def normed_rows(stream, gain, parts):
    return call(
        norm_kernel, [stream, gain.reshape(1, -1), *parts], [(stream.shape, BF), (stream.shape, BF)]
    )


def activated(rows, gate, up):
    got = dot(rows, jnp.concatenate([gate, up], axis=1))
    width = gate.shape[1]
    return (silu(got[:, :width]) * got[:, width:]).astype(BF)


def product_nt(a, b):
    even = a.shape[1] // 256 * 256
    return dot_nt(a[:, :even], b[:, :even]) + dot_nt(a[:, even:], b[:, even:])


TILE = 128
STRIP = 256
AHEAD = 3
UP_GROUPS = (5, 6)
DOWN_GROUPS = (5, 3)


def first_channels_kernel(w_ref, rows_ref, *rest):
    out_refs = rest[:2]
    gate_ref, up_ref, down_ref, hidden_ref, in_sems, down_sems = rest[2:]
    width, hidden = gate_ref.shape
    block = out_refs[0].shape[0]
    groups, spans = [], []
    for many, spread in ((hidden // TILE, UP_GROUPS), (width // STRIP, DOWN_GROUPS)):
        assert sum(spread) == many
        starts = [sum(spread[:k]) for k in range(len(spread))]
        spans.append([range(start, start + n) for start, n in zip(starts, spread)])
    for g, tiles in enumerate(spans[0]):
        here = pl.ds(tiles[0] * TILE, len(tiles) * TILE)
        group = []
        for k, ref in enumerate((gate_ref, up_ref)):
            from_ref = w_ref.at[:, pl.ds(k * hidden + tiles[0] * TILE, len(tiles) * TILE)]
            group.append(pltpu.make_async_copy(from_ref, ref.at[:, here], in_sems.at[k, g]))
        groups.append(group)
    for g, strips in enumerate(spans[1]):
        here = pl.ds(strips[0] * STRIP, len(strips) * STRIP)
        from_ref = w_ref.at[here, pl.ds(2 * hidden, hidden)]
        groups.append([pltpu.make_async_copy(from_ref, down_ref.at[here, :], down_sems.at[g])])

    def begin(g):
        if g < len(groups):
            for copy in groups[g]:
                copy.start()

    def arrived(g):
        for copy in groups[g]:
            copy.wait()
        begin(g + AHEAD)

    for g in range(AHEAD):
        begin(g)
    for g, tiles in enumerate(spans[0]):
        arrived(g)
        for j in tiles:
            here = slice(j * TILE, (j + 1) * TILE)
            hidden_ref[:, here] = activated(rows_ref[...], gate_ref[:, here], up_ref[:, here])
    for g, strips in enumerate(spans[1]):
        arrived(len(spans[0]) + g)
        for n in strips:
            here = slice(n * STRIP, (n + 1) * STRIP)
            got = product_nt(hidden_ref[...], down_ref[here, :])
            for k, out_ref in enumerate(out_refs):
                out_ref[:, here] = got[k * block : (k + 1) * block, :].astype(BF)


def first_channels(weights, rows, hidden):
    block, width = rows.shape
    half = ((block // 2, width), BF)
    out = call(
        first_channels_kernel,
        [rows],
        [half, half] + [((width, hidden), BF)] * 3,
        [
            pltpu.VMEM((block, hidden), BF),
            pltpu.SemaphoreType.DMA((2, len(UP_GROUPS))),
            pltpu.SemaphoreType.DMA((len(DOWN_GROUPS),)),
        ],
        far=[pltpu.with_memory_space_constraint(weights, pltpu.HBM)],
    )
    return out[:2], out[2:]


def more_channels_kernel(count, *refs):
    parts, (gate_ref, up_ref, down_ref) = refs[:count], refs[count : count + 3]
    out_refs, hidden_ref = refs[count + 3 : -1], refs[-1]
    block = parts[0].shape[0]
    rows = jnp.concatenate([part[...] for part in parts], axis=0)
    for j in range(gate_ref.shape[1] // TILE):
        here = slice(j * TILE, (j + 1) * TILE)
        hidden_ref[:, here] = activated(rows, gate_ref[:, here], up_ref[:, here])
    for n in range(down_ref.shape[0] // STRIP):
        here = slice(n * STRIP, (n + 1) * STRIP)
        got = product_nt(hidden_ref[...], down_ref[here, :])
        for k, out_ref in enumerate(out_refs):
            out_ref[:, here] = got[k * block : (k + 1) * block, :].astype(BF)


def more_channels(rows, projections):
    block, width = rows[0].shape
    count = len(rows)
    return call(
        functools.partial(more_channels_kernel, count),
        [*rows, *projections],
        [((block, width), BF)] * count,
        [pltpu.VMEM((count * block, projections[0].shape[1]), BF)],
    )


def joined_kernel(right_ref, left_ref, upper_ref, lower_ref, right_out_ref, left_out_ref):
    half = upper_ref.shape[0]
    right_out_ref[:half, :] = right_ref[:half, :]
    low = right_ref[half:, :].astype(F32) + lower_ref[...].astype(F32)
    right_out_ref[half:, :] = low.astype(BF)
    high = left_ref[:half, :].astype(F32) + upper_ref[...].astype(F32)
    left_out_ref[:half, :] = high.astype(BF)
    left_out_ref[half:, :] = left_ref[half:, :]


def joined(right, left, upper, lower):
    shapes = [(right.shape, BF), (left.shape, BF)]
    return call(joined_kernel, [right, left, upper, lower], shapes)


def last_kernel(middle_ref, *rest):
    parts, out_ref = rest[:-1], rest[-1]
    total = parts[0][...].astype(F32)
    for part in parts[1:]:
        total = total + part[...].astype(F32)
    out_ref[...] = (middle_ref[...].astype(F32) + 0.5 * total).astype(BF)


def last_sum(middle, parts):
    near = [pltpu.with_memory_space_constraint(x, pltpu.VMEM) for x in [middle, *parts]]
    return pl.pallas_call(
        last_kernel,
        in_specs=[FULL] * len(near),
        out_specs=FULL,
        out_shape=jax.ShapeDtypeStruct(middle.shape, BF),
        compiler_params=pltpu.CompilerParams(vmem_limit_bytes=16 << 20),
        name="last_sum",
    )(*near)


def per_device(
    queries,
    keys,
    values,
    gates,
    decay_pre,
    beta_pre,
    out_gain,
    w_out,
    stream,
    norm_gain,
    w_gate,
    w_up,
    w_down,
):
    hidden = w_gate.shape[1]
    weights = jnp.concatenate([w_gate, w_up, w_down.T], axis=1)
    weights = lax.all_gather(weights, SP, axis=0, tiled=True)
    size = lax.axis_size("tp")
    before, total, solved, decay, grown = keys_side(keys, values, beta_pre, decay_pre)
    gate = gates_side(gates, out_gain)
    pairs = queries.shape[1] // PAIR
    early, late, states = state_ahead(
        total,
        lambda x: queries_side(0, x, queries, decay, solved, before, grown),
        lambda x: queries_side(pairs // 2, x, queries, decay, solved, before, grown),
    )
    parts = mixed_and_projected(size, early, late, states, gate, w_out)
    parts = [parts[0]] + [lax.ppermute(parts[k], "tp", ring(size, k)) for k in (1, 2, 3)]
    middle, normed = normed_rows(stream, norm_gain, parts)
    across = lax.ppermute(normed, "tp", ring(size, 2))
    right = lax.ppermute(normed, "tp", ring(size, 1))
    left = lax.ppermute(normed, "tp", ring(size, -1))
    (upper, lower), projections = first_channels(weights, across, hidden)
    upper = lax.ppermute(upper, "tp", ring(size, 1))
    lower = lax.ppermute(lower, "tp", ring(size, -1))
    right, left = more_channels([right, left], projections)
    right, left = joined(right, left, upper, lower)
    right = lax.ppermute(right, "tp", ring(size, -1))
    left = lax.ppermute(left, "tp", ring(size, 1))
    (own,) = more_channels([normed], projections)
    return last_sum(middle, [own, right, left])


def solution(mesh):
    finer = Mesh(mesh.devices.reshape(4, 4, 2, mesh.shape["tp"]), SP_TP)
    placed = (
        P(SP, "tp"),
        P(SP, "tp"),
        P(SP, "tp"),
        P(SP, "tp"),
        P("tp", SP),
        P("tp", SP),
        P(),
        P("tp", None),
        P(SP_TP, None),
        P(),
        P(SP, "tp"),
        P(SP, "tp"),
        P("tp", SP),
    )
    return jax.shard_map(
        per_device, mesh=finer, in_specs=placed, out_specs=P(SP_TP, None), check_vma=False
    )
```

```python
import functools

import jax
import jax.numpy as jnp
from jax import lax
from jax.experimental import pallas as pl
from jax.experimental.pallas import tpu as pltpu
from jax.sharding import Mesh
from jax.sharding import PartitionSpec as P


HEAD_DIM = 64
PAIR = 2 * HEAD_DIM
CHUNK = 128
SP = ("sp_0", "sp_1", "sp_2")
SP_TP = ("sp_0", "sp_1", "sp_2", "tp")
EPSILON = 1e-06
BF = jnp.bfloat16
F32 = jnp.float32
NT = (((1,), (1,)), ((), ()))


FULL = pl.BlockSpec(memory_space=pltpu.VMEM)
FAR = pl.BlockSpec(memory_space=pl.ANY)


def call(kernel, arrays, shapes, scratch=(), far=(), mib=16):
    near = [pltpu.with_memory_space_constraint(x, pltpu.VMEM) for x in arrays]
    return pl.pallas_call(
        kernel,
        in_specs=[FAR] * len(far) + [FULL] * len(near),
        out_specs=[FULL] * len(shapes),
        out_shape=[pltpu.VMEM(shape, dtype) for shape, dtype in shapes],
        scratch_shapes=scratch,
        compiler_params=pltpu.CompilerParams(vmem_limit_bytes=mib << 20),
    )(*far, *near)


def ring(size, k):
    return [(i, (i + k) % size) for i in range(size)]


def dot(a, b):
    return jnp.dot(a, b, preferred_element_type=F32)


def dot_nt(a, b):
    return lax.dot_general(a, b, NT, preferred_element_type=F32)


def silu(x):
    return x / (1.0 + jnp.exp(-x))


def places():
    row = lax.broadcasted_iota(jnp.int32, (PAIR, PAIR), 0)
    col = lax.broadcasted_iota(jnp.int32, (PAIR, PAIR), 1)
    return row, col


def half_sums(squares, ones):
    high = squares.astype(BF)
    low = (squares - high.astype(F32)).astype(BF)
    return dot(high, ones) + dot(low, ones)


def softplus(x):
    small = jnp.exp(-jnp.abs(x))
    series = small * (1.0 - small * (0.5 - small * (1.0 / 3.0 - 0.25 * small)))
    return jnp.maximum(x, 0.0) + jnp.where(small < 0.015, series, jnp.log(1.0 + small))


def turned(z):
    return pltpu.roll(z, HEAD_DIM, 1)


def split_three(x):
    high = x.astype(BF)
    rest = x - high.astype(F32)
    middle = rest.astype(BF)
    return jnp.concatenate([high, middle], axis=1), (rest - middle.astype(F32)).astype(BF)


def side_by_side(pair):
    zero = jnp.zeros_like(pair[0])
    upper = jnp.concatenate([pair[0], zero], axis=1)
    lower = jnp.concatenate([zero, pair[1]], axis=1)
    return jnp.concatenate([upper, lower], axis=0)


def halves(x):
    return x[:, :CHUNK], x[:, CHUNK:]


def keys_kernel(
    k_far_ref, v_far_ref, beta_far_ref, decay_far_ref,
    before_ref, total_ref, y_ref, d_ref, ec_ref,
    l_ref, x_ref, r_ref, f_ref, k_ref, v_ref, beta_ref, decay_ref, sems,
):
    length, width = k_ref.shape
    rate_copies = [
        pltpu.make_async_copy(decay_far_ref, decay_ref, sems.at[0]),
        pltpu.make_async_copy(beta_far_ref, beta_ref, sems.at[1]),
    ]
    row_copies = []
    for c in range(length // CHUNK):
        rows = pl.ds(c * CHUNK, CHUNK)
        for k, (far_ref, ref) in enumerate(((k_far_ref, k_ref), (v_far_ref, v_ref))):
            sem = sems.at[2 + 2 * c + k]
            row_copies.append(pltpu.make_async_copy(far_ref.at[rows], ref.at[rows], sem))
    for copy in rate_copies + row_copies:
        copy.start()
    row, col = places()
    left = col < HEAD_DIM
    top = row < HEAD_DIM
    same = left == top
    ones = jnp.where(same, 1.0, 0.0).astype(BF)
    inclusive = row >= col
    strict = row > col
    differ = row ^ col
    eye = jnp.where(row == col, 1.0, 0.0)
    off_eye = differ == HEAD_DIM
    pairs = width // PAIR
    heads = 2 * pairs
    steps = length // CHUNK

    def stacked(x):
        return jnp.concatenate([x[:, c * CHUNK : (c + 1) * CHUNK] for c in range(steps)], axis=0)

    for copy in rate_copies + row_copies:
        copy.wait()
    rates = split_three(stacked(-softplus(decay_ref[...])))
    strength = split_three(stacked(1.0 / (1.0 + jnp.exp(-beta_ref[...]))))
    triangle = jnp.where(inclusive, 1.0, 0.0).astype(BF)
    eye_bf = eye.astype(BF)
    triangle_two = jnp.concatenate([triangle, triangle], axis=1)
    cum_row = dot_nt(rates[0], triangle_two) + dot_nt(rates[1], triangle)
    cum_col = dot_nt(triangle_two, rates[0]) + dot_nt(triangle, rates[1])
    beta_col = dot_nt(jnp.concatenate([eye_bf, eye_bf], axis=1), strength[0])
    beta_col = beta_col + dot_nt(eye_bf, strength[1])

    ends = []
    for c in range(steps):
        rows = slice(c * CHUNK, (c + 1) * CHUNK)
        for p in range(pairs):
            lanes = slice(p * PAIR, (p + 1) * PAIR)
            item = c * pairs + p
            key = silu(k_ref[rows, lanes].astype(F32))
            key = (key * lax.rsqrt(half_sums(key * key, ones) + EPSILON)).astype(BF)
            y_ref[item, :, 2 * PAIR :] = key
            key_f = key.astype(F32)
            first = c * heads + 2 * p
            cums = [cum_col[:, h : h + 1] for h in (first, first + 1)]
            betas = [beta_col[:, h : h + 1] for h in (first, first + 1)]
            cum = jnp.where(left, cums[0], cums[1])
            beta = jnp.where(left, betas[0], betas[1])
            grown = jnp.exp(cum)
            ec_ref[rows, lanes] = grown
            strong = turned(key_f * (beta * grown))
            value = silu(v_ref[rows, lanes].astype(F32)) * beta
            r_ref[item, :, :CHUNK] = jnp.where(left, value, strong).astype(BF)
            r_ref[item, :, CHUNK:] = jnp.where(left, strong, value).astype(BF)
            fade = jnp.exp(cum[CHUNK - 1 : CHUNK, :] - cum)
            f_ref[item] = (key_f * fade).T.astype(BF)
            last = [jnp.exp(x[CHUNK - 1 : CHUNK, :]) for x in cums]
            ends.append(jnp.where(off_eye, jnp.where(top, last[0], last[1]), 0.0))
            owns = [jnp.where(left, key_f, 0.0), jnp.where(left, 0.0, key_f)]
            inner = dot_nt(key, jnp.concatenate(owns, axis=0).astype(BF))
            for s in range(2):
                part = slice(s * CHUNK, (s + 1) * CHUNK)
                gap = cums[s] - cum_row[first + s : first + s + 1, :]
                decay = jnp.where(inclusive, jnp.exp(gap), 0.0)
                d_ref[item, :, part] = decay.astype(BF)
                lower = jnp.where(strict, inner[:, part] * decay * betas[s], 0.0)
                l_ref[item, :, part] = lower.astype(BF)
                x_ref[item, :, part] = (eye - jnp.where(differ == 1, lower, 0.0)).astype(BF)

    items = steps * pairs

    for power in range(1, 7):
        mask = jnp.where((differ >> power) == 1, 1.0, 0.0).astype(BF)
        parts = []
        for i in range(items):
            block = side_by_side([part * mask for part in halves(l_ref[i])])
            parts.append(dot(x_ref[i], block).astype(BF))
        for i in range(items):
            x = x_ref[i]
            x_ref[i] = x - dot(parts[i], side_by_side(halves(x))).astype(BF)

    runs = [None] * pairs
    for c in range(steps):
        for p in range(pairs):
            item = c * pairs + p
            y = dot(x_ref[item], side_by_side(halves(r_ref[item]))).astype(BF)
            y_ref[item, :, : 2 * PAIR] = y
            z = jnp.where(top, *halves(dot(f_ref[item], y)))
            z = jnp.where(same, z, ends[item] - z)
            if c == 0:
                before_ref[item] = jnp.where(off_eye, 1.0, 0.0).astype(BF)
                runs[p] = z.astype(BF)
            else:
                before_ref[item] = runs[p]
                step = jnp.where(same, turned(z), 0.0).astype(BF)
                runs[p] = (dot(step, runs[p]) + jnp.where(same, z, 0.0)).astype(BF)
    for p in range(pairs):
        total_ref[p] = runs[p]


def keys_side(keys, values, beta_pre, decay_pre):
    length, width = keys.shape
    pairs = width // PAIR
    steps = length // CHUNK
    items = steps * pairs
    wide = pltpu.VMEM((items, CHUNK, 2 * CHUNK), BF)
    return call(
        keys_kernel,
        [],
        [
            ((items, PAIR, PAIR), BF),
            ((pairs, PAIR, PAIR), BF),
            ((items, CHUNK, 3 * PAIR), BF),
            ((items, CHUNK, 2 * CHUNK), BF),
            ((length, width), F32),
        ],
        [
            wide,
            wide,
            wide,
            pltpu.VMEM((items, PAIR, CHUNK), BF),
            pltpu.VMEM((length, width), BF),
            pltpu.VMEM((length, width), BF),
            pltpu.VMEM(beta_pre.shape, F32),
            pltpu.VMEM(beta_pre.shape, F32),
            pltpu.SemaphoreType.DMA((2 + 2 * steps,)),
        ],
        far=[
            pltpu.with_memory_space_constraint(x, pltpu.HBM)
            for x in (keys, values, beta_pre, decay_pre)
        ],
    )


def gates_kernel(gates_ref, gain_ref, gate_ref):
    gain = jnp.concatenate([gain_ref[...], gain_ref[...]], axis=1)
    for p in range(gates_ref.shape[1] // PAIR):
        lanes = slice(p * PAIR, (p + 1) * PAIR)
        gate_ref[:, lanes] = silu(gates_ref[:, lanes].astype(F32)) * gain


def queries_kernel(first, after_ref, q_ref, d_ref, y_ref, before_ref, ec_ref, o_ref, q1_ref):
    row, col = places()
    left = col < HEAD_DIM
    same = left == (row < HEAD_DIM)
    ones = jnp.where(same, 1.0, 0.0).astype(BF)
    length, width = o_ref.shape
    pairs = q_ref.shape[1] // PAIR

    def chunk(c, carry):
        rows = pl.ds(pl.multiple_of(c * CHUNK, CHUNK), CHUNK)
        for p in range(first, first + width // PAIR):
            lanes = slice(p * PAIR, (p + 1) * PAIR)
            place = slice((p - first) * PAIR, (p - first + 1) * PAIR)
            item = c * pairs + p
            query = silu(q_ref[rows, lanes].astype(F32))
            query = query * lax.rsqrt(half_sums(query * query, ones) + EPSILON)
            query = (query * HEAD_DIM ** (-0.5)).astype(BF)
            key_f = y_ref[item, :, 2 * PAIR :].astype(F32)
            owns = [jnp.where(left, key_f, 0.0), jnp.where(left, 0.0, key_f)]
            inside = dot_nt(query, jnp.concatenate(owns, axis=0).astype(BF))
            inside = (inside * d_ref[item].astype(F32)).astype(BF)
            got = halves(dot(inside, side_by_side(halves(y_ref[item, :, : 2 * PAIR]))))
            local = jnp.where(left, got[0], got[1])
            crossed = turned(jnp.where(left, got[1], got[0]))
            query = (query.astype(F32) * ec_ref[rows, lanes] - crossed).astype(BF)
            before = before_ref[item].astype(F32)
            both = [jnp.where(same, before, 0.0), jnp.where(same, turned(before), 0.0)]
            moved = halves(dot(query, jnp.concatenate(both, axis=1).astype(BF)))
            o_ref[rows, place] = local + moved[0]
            q1_ref[rows, place] = moved[1].astype(BF)
        return carry

    lax.fori_loop(0, length // CHUNK, chunk, 0)


def gates_side(gates, gain):
    return call(gates_kernel, [gates, gain.reshape(1, HEAD_DIM)], [(gates.shape, F32)])[0]


def queries_side(first, after, queries, decay, solved, before, grown):
    length, width = queries.shape
    shape = (length, width // 2)
    return call(
        functools.partial(queries_kernel, first),
        [queries, decay, solved, before, grown],
        [(shape, F32), (shape, BF)],
        far=[after],
    )


def chained(earlier, later, same):
    later = later.astype(F32)
    step = jnp.where(same, turned(later), 0.0).astype(BF)
    return dot(step, earlier.astype(BF)) + jnp.where(same, later, 0.0)


def chip_kernel(own_ref, other_ref, out_ref, kept_ref):
    kept_ref[...] = other_ref[...]
    row, col = places()
    same = (col < HEAD_DIM) == (row < HEAD_DIM)
    core = lax.axis_index(SP[2])
    count = out_ref.shape[0]
    for p in range(count):
        mine = own_ref[core * count + p]
        theirs = other_ref[core * count + p]
        first = jnp.where(core == 0, mine, theirs)
        second = jnp.where(core == 0, theirs, mine)
        out_ref[p] = chained(first, second, same).astype(BF)


def row_kernel(after_ref, *rest):
    parts, (total_ref, before_ref, all_ref) = rest[:-3], rest[-3:]
    row, col = places()
    same = (col < HEAD_DIM) == (row < HEAD_DIM)
    place = lax.axis_index(SP[1])
    size = len(parts)
    for k, part in enumerate(parts):
        all_ref[lax.rem(place - k + size, size)] = part[...]
    for p in range(total_ref.shape[0]):
        run = all_ref[0, p].astype(F32)
        inside = jnp.where(place == 0, jnp.where((row ^ col) == HEAD_DIM, 1.0, 0.0), run)
        for k in range(1, size):
            run = chained(run, all_ref[k, p], same)
            inside = jnp.where(k < place, run, inside)
        before_ref[p] = inside.astype(BF)
        total_ref[p] = run.astype(BF)


def plane_kernel(after_ref, before_ref, *rest):
    parts, out_ref = rest[:-1], rest[-1]
    row, col = places()
    same = (col < HEAD_DIM) == (row < HEAD_DIM)
    place = lax.axis_index(SP[0])
    for p in range(out_ref.shape[0]):
        state = jnp.zeros((PAIR, PAIR), F32)
        for k in range(len(parts), 0, -1):
            later = jnp.where(same, chained(state, parts[k - 1][p], same), 0.0)
            state = jnp.where(k <= place, later, state)
        state = chained(state, before_ref[p], same)
        out_ref[p] = jnp.where(same, state, 0.0).astype(BF)


def state_ahead(total, meanwhile, then):
    plane, line, core = SP
    swap = [(0, 1), (1, 0)]
    half = (total.shape[0] // 2, PAIR, PAIR)
    other = lax.ppermute(total, core, swap)
    chip, other = call(chip_kernel, [total, other], [(half, BF), (total.shape, BF)])
    size = lax.axis_size(line)
    lines = [chip] + [lax.ppermute(chip, line, ring(size, k)) for k in range(1, size)]
    early = meanwhile(chip)
    whole, before = call(
        row_kernel, lines, [(half, BF), (half, BF)], [pltpu.VMEM((size, *half), BF)], far=[early[1]]
    )
    size = lax.axis_size(plane)
    planes = [lax.ppermute(whole, plane, ring(size, k)) for k in range(1, size)]
    late = then(whole)
    (state,) = call(plane_kernel, [before] + planes, [(half, BF)], far=[late[1]])
    return early, late, (other, state, lax.ppermute(state, core, swap))


def mixed_kernel(
    o0_ref, q0_ref, o1_ref, q1_ref,
    first_ref, mine_ref, theirs_ref, gate_ref, w_ref, *rest,
):
    out_refs, (mixed_ref, state_ref) = rest[:-2], rest[-2:]
    row, col = places()
    same = (col < HEAD_DIM) == (row < HEAD_DIM)
    ones = jnp.where(same, 1.0, 0.0).astype(BF)
    length, width = gate_ref.shape
    size = len(out_refs)
    block = length // size
    core = lax.axis_index(SP[2])
    turn = lax.axis_index("tp")
    half = mine_ref.shape[0]
    state_ref[pl.ds(core * half, half)] = mine_ref[...]
    state_ref[pl.ds((1 - core) * half, half)] = theirs_ref[...]
    for p in range(width // PAIR):
        lanes = slice(p * PAIR, (p + 1) * PAIR)
        state = state_ref[p].astype(F32)
        later = jnp.where(same, chained(state, first_ref[p], same), 0.0)
        state = jnp.where(core == 0, state, later).astype(BF)
        o_ref, q_ref = ((o0_ref, q0_ref), (o1_ref, q1_ref))[p // half]
        place = slice((p % half) * PAIR, (p % half + 1) * PAIR)
        out = o_ref[:, place] + dot(q_ref[:, place], state)
        mean = half_sums(out * out, ones) * (1.0 / HEAD_DIM)
        out = (out * lax.rsqrt(mean + EPSILON) * gate_ref[:, lanes]).astype(BF)
        for k in range(size):
            start = pl.multiple_of(lax.rem(k - turn + size, size) * block, 32)
            mixed_ref[pl.ds(start, block), lanes] = out[k * block : (k + 1) * block, :]
    for n in range(w_ref.shape[1] // STRIP):
        here = slice(n * STRIP, (n + 1) * STRIP)
        got = dot(mixed_ref[...], w_ref[:, here])
        for k, out_ref in enumerate(out_refs):
            out_ref[:, here] = got[k * block : (k + 1) * block, :].astype(out_ref.dtype)


def mixed_and_projected(size, early, late, states, gate, w_out):
    length, width = gate.shape
    return call(
        mixed_kernel,
        [*early, *late, *states, gate, w_out],
        [((length // size, w_out.shape[1]), BF if k else F32) for k in range(size)],
        [pltpu.VMEM((length, width), BF), pltpu.VMEM((width // PAIR, PAIR, PAIR), BF)],
    )


def norm_kernel(stream_ref, gain_ref, *rest):
    parts, (middle_ref, normed_ref) = rest[:-2], rest[-2:]
    projected = parts[0][...]
    for part in parts[1:]:
        projected = projected + part[...].astype(F32)
    middle = (stream_ref[...].astype(F32) + projected).astype(BF)
    middle_ref[...] = middle
    middle = middle.astype(F32)
    mean = jnp.mean(middle * middle, axis=-1, keepdims=True)
    normed_ref[...] = (middle * lax.rsqrt(mean + EPSILON) * gain_ref[...]).astype(BF)


def normed_rows(stream, gain, parts):
    return call(
        norm_kernel, [stream, gain.reshape(1, -1), *parts], [(stream.shape, BF), (stream.shape, BF)]
    )


def activated(rows, gate, up):
    got = dot(rows, jnp.concatenate([gate, up], axis=1))
    width = gate.shape[1]
    return (silu(got[:, :width]) * got[:, width:]).astype(BF)


def product_nt(a, b):
    even = a.shape[1] // 256 * 256
    return dot_nt(a[:, :even], b[:, :even]) + dot_nt(a[:, even:], b[:, even:])


TILE = 128
STRIP = 256
AHEAD = 3
UP_GROUPS = (3, 5, 3)
DOWN_GROUPS = (5, 3)


def first_channels_kernel(w_ref, across_ref, right_ref, left_ref, *rest):
    out_refs, kept_ref = rest[:2], rest[2]
    gate_ref, up_ref, down_ref, hidden_ref, in_sems, down_sems = rest[3:]
    width, hidden = gate_ref.shape
    block = out_refs[0].shape[0]
    rows = across_ref.shape[0]
    groups, spans = [], []
    for many, spread in ((hidden // TILE, UP_GROUPS), (width // STRIP, DOWN_GROUPS)):
        assert sum(spread) == many
        starts = [sum(spread[:k]) for k in range(len(spread))]
        spans.append([range(start, start + n) for start, n in zip(starts, spread)])
    for g, tiles in enumerate(spans[0]):
        here = pl.ds(tiles[0] * TILE, len(tiles) * TILE)
        group = []
        for k, ref in enumerate((gate_ref, up_ref)):
            from_ref = w_ref.at[:, pl.ds(k * hidden + tiles[0] * TILE, len(tiles) * TILE)]
            group.append(pltpu.make_async_copy(from_ref, ref.at[:, here], in_sems.at[k, g]))
        groups.append(group)
    for g, strips in enumerate(spans[1]):
        here = pl.ds(strips[0] * STRIP, len(strips) * STRIP)
        from_ref = w_ref.at[here, pl.ds(2 * hidden, hidden)]
        groups.append([pltpu.make_async_copy(from_ref, down_ref.at[here, :], down_sems.at[g])])

    def begin(g):
        if g < len(groups):
            for copy in groups[g]:
                copy.start()

    def arrived(g):
        for copy in groups[g]:
            copy.wait()
        begin(g + AHEAD)

    for g in range(AHEAD):
        begin(g)
    for g, tiles in enumerate(spans[0]):
        arrived(g)
        for j in tiles:
            here = slice(j * TILE, (j + 1) * TILE)
            every = [across_ref[...], right_ref[...], left_ref[...]]
            every = jnp.concatenate(every, axis=0)
            units = activated(every, gate_ref[:, here], up_ref[:, here])
            hidden_ref[:, here] = units[:rows, :]
            kept_ref[:, here] = units[rows:, :]
    for g, strips in enumerate(spans[1]):
        arrived(len(spans[0]) + g)
        for n in strips:
            here = slice(n * STRIP, (n + 1) * STRIP)
            got = product_nt(hidden_ref[...], down_ref[here, :])
            for k, out_ref in enumerate(out_refs):
                out_ref[:, here] = got[k * block : (k + 1) * block, :].astype(BF)


def first_channels(weights, across, right, left, hidden):
    block, width = across.shape
    half = ((block // 2, width), BF)
    out = call(
        first_channels_kernel,
        [across, right, left],
        [half, half, ((2 * block, hidden), BF)] + [((width, hidden), BF)] * 3,
        [
            pltpu.VMEM((block, hidden), BF),
            pltpu.SemaphoreType.DMA((2, len(UP_GROUPS))),
            pltpu.SemaphoreType.DMA((len(DOWN_GROUPS),)),
        ],
        far=[pltpu.with_memory_space_constraint(weights, pltpu.HBM)],
    )
    return out[:2], out[2], out[3:]


def neighbours_kernel(hidden_ref, down_ref, *out_refs):
    half = out_refs[0].shape[0]
    for n in range(down_ref.shape[0] // STRIP):
        here = slice(n * STRIP, (n + 1) * STRIP)
        got = product_nt(hidden_ref[...], down_ref[here, :]).astype(BF)
        for k, out_ref in enumerate(out_refs):
            out_ref[:, here] = got[k * half : (k + 1) * half, :]


def neighbours(hidden, down):
    shape = (hidden.shape[0] // 4, down.shape[0])
    return call(neighbours_kernel, [hidden, down], [(shape, BF)] * 4)


def more_channels_kernel(count, *refs):
    parts, (gate_ref, up_ref, down_ref) = refs[:count], refs[count : count + 3]
    out_refs, hidden_ref = refs[count + 3 : -1], refs[-1]
    block = parts[0].shape[0]
    rows = jnp.concatenate([part[...] for part in parts], axis=0)
    for j in range(gate_ref.shape[1] // TILE):
        here = slice(j * TILE, (j + 1) * TILE)
        hidden_ref[:, here] = activated(rows, gate_ref[:, here], up_ref[:, here])
    for n in range(down_ref.shape[0] // STRIP):
        here = slice(n * STRIP, (n + 1) * STRIP)
        got = product_nt(hidden_ref[...], down_ref[here, :])
        for k, out_ref in enumerate(out_refs):
            out_ref[:, here] = got[k * block : (k + 1) * block, :].astype(BF)


def more_channels(rows, projections):
    block, width = rows[0].shape
    count = len(rows)
    return call(
        functools.partial(more_channels_kernel, count),
        [*rows, *projections],
        [((block, width), BF)] * count,
        [pltpu.VMEM((count * block, projections[0].shape[1]), BF)],
    )


def joined_kernel(low_ref, more_low_ref, high_ref, more_high_ref, low_out_ref, high_out_ref):
    low = low_ref[...].astype(F32) + more_low_ref[...].astype(F32)
    low_out_ref[...] = low.astype(BF)
    high = high_ref[...].astype(F32) + more_high_ref[...].astype(F32)
    high_out_ref[...] = high.astype(BF)


def joined(low, more_low, high, more_high):
    shapes = [(low.shape, BF)] * 2
    return call(joined_kernel, [low, more_low, high, more_high], shapes)


def last_kernel(middle_ref, own_ref, *rest):
    parts, out_ref = rest[:-1], rest[-1]
    half = parts[0].shape[0]
    for k in range(2):
        rows = slice(k * half, (k + 1) * half)
        total = own_ref[rows, :].astype(F32)
        for part in parts[2 * k : 2 * k + 2]:
            total = total + part[...].astype(F32)
        out_ref[rows, :] = (middle_ref[rows, :].astype(F32) + 0.5 * total).astype(BF)


def last_sum(middle, parts):
    near = [pltpu.with_memory_space_constraint(x, pltpu.VMEM) for x in [middle, *parts]]
    return pl.pallas_call(
        last_kernel,
        in_specs=[FULL] * len(near),
        out_specs=FULL,
        out_shape=jax.ShapeDtypeStruct(middle.shape, BF),
        compiler_params=pltpu.CompilerParams(vmem_limit_bytes=16 << 20),
        name="last_sum",
    )(*near)


def per_device(
    queries,
    keys,
    values,
    gates,
    decay_pre,
    beta_pre,
    out_gain,
    w_out,
    stream,
    norm_gain,
    w_gate,
    w_up,
    w_down,
):
    hidden = w_gate.shape[1]
    weights = jnp.concatenate([w_gate, w_up, w_down.T], axis=1)
    weights = lax.all_gather(weights, SP, axis=0, tiled=True)
    size = lax.axis_size("tp")
    before, total, solved, decay, grown = keys_side(keys, values, beta_pre, decay_pre)
    gate = gates_side(gates, out_gain)
    pairs = queries.shape[1] // PAIR
    early, late, states = state_ahead(
        total,
        lambda x: queries_side(0, x, queries, decay, solved, before, grown),
        lambda x: queries_side(pairs // 2, x, queries, decay, solved, before, grown),
    )
    parts = mixed_and_projected(size, early, late, states, gate, w_out)
    parts = [parts[0]] + [lax.ppermute(parts[k], "tp", ring(size, k)) for k in (1, 2, 3)]
    middle, normed = normed_rows(stream, norm_gain, parts)
    across = lax.ppermute(normed, "tp", ring(size, 2))
    right = lax.ppermute(normed, "tp", ring(size, 1))
    left = lax.ppermute(normed, "tp", ring(size, -1))
    far, units, projections = first_channels(weights, across, right, left, hidden)
    upper = lax.ppermute(far[0], "tp", ring(size, 1))
    lower = lax.ppermute(far[1], "tp", ring(size, -1))
    right_up, right_low, left_up, left_low = neighbours(units, projections[2])
    right_up = lax.ppermute(right_up, "tp", ring(size, -1))
    left_low = lax.ppermute(left_low, "tp", ring(size, 1))
    right_low, left_up = joined(right_low, lower, left_up, upper)
    right_low = lax.ppermute(right_low, "tp", ring(size, -1))
    left_up = lax.ppermute(left_up, "tp", ring(size, 1))
    (own,) = more_channels([normed], projections)
    return last_sum(middle, [own, right_up, left_up, right_low, left_low])


def solution(mesh):
    finer = Mesh(mesh.devices.reshape(4, 4, 2, mesh.shape["tp"]), SP_TP)
    placed = (
        P(SP, "tp"),
        P(SP, "tp"),
        P(SP, "tp"),
        P(SP, "tp"),
        P("tp", SP),
        P("tp", SP),
        P(),
        P("tp", None),
        P(SP_TP, None),
        P(),
        P(SP, "tp"),
        P(SP, "tp"),
        P("tp", SP),
    )
    return jax.shard_map(
        per_device, mesh=finer, in_specs=placed, out_specs=P(SP_TP, None), check_vma=False
    )
```

```python
import functools

import jax
import jax.numpy as jnp
from jax import lax
from jax.experimental import pallas as pl
from jax.experimental.pallas import tpu as pltpu
from jax.sharding import Mesh
from jax.sharding import PartitionSpec as P


HEAD_DIM = 64
PAIR = 2 * HEAD_DIM
CHUNK = 128
SP = ("sp_0", "sp_1", "sp_2")
SP_TP = ("sp_0", "sp_1", "sp_2", "tp")
EPSILON = 1e-06
BF = jnp.bfloat16
F32 = jnp.float32
NT = (((1,), (1,)), ((), ()))


FULL = pl.BlockSpec(memory_space=pltpu.VMEM)
FAR = pl.BlockSpec(memory_space=pl.ANY)


def call(kernel, arrays, shapes, scratch=(), far=(), mib=16):
    near = [pltpu.with_memory_space_constraint(x, pltpu.VMEM) for x in arrays]
    return pl.pallas_call(
        kernel,
        in_specs=[FAR] * len(far) + [FULL] * len(near),
        out_specs=[FULL] * len(shapes),
        out_shape=[pltpu.VMEM(shape, dtype) for shape, dtype in shapes],
        scratch_shapes=scratch,
        compiler_params=pltpu.CompilerParams(vmem_limit_bytes=mib << 20),
    )(*far, *near)


def upward(size, k):
    return [(i, i + k) for i in range(size - k)]


def ring(size, k):
    return [(i, (i + k) % size) for i in range(size)]


def dot(a, b):
    return jnp.dot(a, b, preferred_element_type=F32)


def dot_nt(a, b):
    return lax.dot_general(a, b, NT, preferred_element_type=F32)


def silu(x):
    return x / (1.0 + jnp.exp(-x))


def places():
    row = lax.broadcasted_iota(jnp.int32, (PAIR, PAIR), 0)
    col = lax.broadcasted_iota(jnp.int32, (PAIR, PAIR), 1)
    return row, col


def half_sums(squares, ones):
    high = squares.astype(BF)
    low = (squares - high.astype(F32)).astype(BF)
    return dot(high, ones) + dot(low, ones)


def softplus(x):
    small = jnp.exp(-jnp.abs(x))
    series = small * (1.0 - small * (0.5 - small * (1.0 / 3.0 - 0.25 * small)))
    return jnp.maximum(x, 0.0) + jnp.where(small < 0.015, series, jnp.log(1.0 + small))


def turned(z):
    return pltpu.roll(z, HEAD_DIM, 1)


def split_three(x):
    high = x.astype(BF)
    rest = x - high.astype(F32)
    middle = rest.astype(BF)
    return jnp.concatenate([high, middle], axis=1), (rest - middle.astype(F32)).astype(BF)


def side_by_side(pair):
    zero = jnp.zeros_like(pair[0])
    upper = jnp.concatenate([pair[0], zero], axis=1)
    lower = jnp.concatenate([zero, pair[1]], axis=1)
    return jnp.concatenate([upper, lower], axis=0)


def halves(x):
    return x[:, :CHUNK], x[:, CHUNK:]


def keys_kernel(
    k_far_ref, v_far_ref, beta_far_ref, decay_far_ref,
    before_ref, total_ref, y_ref, d_ref, ec_ref,
    l_ref, x_ref, r_ref, f_ref, k_ref, v_ref, beta_ref, decay_ref, sems,
):
    length, width = k_ref.shape
    rate_copies = [
        pltpu.make_async_copy(decay_far_ref, decay_ref, sems.at[0]),
        pltpu.make_async_copy(beta_far_ref, beta_ref, sems.at[1]),
    ]
    row_copies = []
    for c in range(length // CHUNK):
        rows = pl.ds(c * CHUNK, CHUNK)
        for k, (far_ref, ref) in enumerate(((k_far_ref, k_ref), (v_far_ref, v_ref))):
            sem = sems.at[2 + 2 * c + k]
            row_copies.append(pltpu.make_async_copy(far_ref.at[rows], ref.at[rows], sem))
    for copy in rate_copies + row_copies:
        copy.start()
    row, col = places()
    left = col < HEAD_DIM
    top = row < HEAD_DIM
    same = left == top
    ones = jnp.where(same, 1.0, 0.0).astype(BF)
    inclusive = row >= col
    strict = row > col
    differ = row ^ col
    eye = jnp.where(row == col, 1.0, 0.0)
    off_eye = differ == HEAD_DIM
    pairs = width // PAIR
    heads = 2 * pairs
    steps = length // CHUNK

    def stacked(x):
        return jnp.concatenate([x[:, c * CHUNK : (c + 1) * CHUNK] for c in range(steps)], axis=0)

    for copy in rate_copies + row_copies:
        copy.wait()
    rates = split_three(stacked(-softplus(decay_ref[...])))
    strength = split_three(stacked(1.0 / (1.0 + jnp.exp(-beta_ref[...]))))
    triangle = jnp.where(inclusive, 1.0, 0.0).astype(BF)
    eye_bf = eye.astype(BF)
    triangle_two = jnp.concatenate([triangle, triangle], axis=1)
    cum_row = dot_nt(rates[0], triangle_two) + dot_nt(rates[1], triangle)
    cum_col = dot_nt(triangle_two, rates[0]) + dot_nt(triangle, rates[1])
    beta_col = dot_nt(jnp.concatenate([eye_bf, eye_bf], axis=1), strength[0])
    beta_col = beta_col + dot_nt(eye_bf, strength[1])

    ends = []
    for c in range(steps):
        rows = slice(c * CHUNK, (c + 1) * CHUNK)
        for p in range(pairs):
            lanes = slice(p * PAIR, (p + 1) * PAIR)
            item = c * pairs + p
            key = silu(k_ref[rows, lanes].astype(F32))
            key = (key * lax.rsqrt(half_sums(key * key, ones) + EPSILON)).astype(BF)
            y_ref[item, :, 2 * PAIR :] = key
            key_f = key.astype(F32)
            first = c * heads + 2 * p
            cums = [cum_col[:, h : h + 1] for h in (first, first + 1)]
            betas = [beta_col[:, h : h + 1] for h in (first, first + 1)]
            cum = jnp.where(left, cums[0], cums[1])
            beta = jnp.where(left, betas[0], betas[1])
            grown = jnp.exp(cum)
            ec_ref[rows, lanes] = grown
            strong = turned(key_f * (beta * grown))
            value = silu(v_ref[rows, lanes].astype(F32)) * beta
            r_ref[item, :, :CHUNK] = jnp.where(left, value, strong).astype(BF)
            r_ref[item, :, CHUNK:] = jnp.where(left, strong, value).astype(BF)
            fade = jnp.exp(cum[CHUNK - 1 : CHUNK, :] - cum)
            f_ref[item] = (key_f * fade).T.astype(BF)
            last = [jnp.exp(x[CHUNK - 1 : CHUNK, :]) for x in cums]
            ends.append(jnp.where(off_eye, jnp.where(top, last[0], last[1]), 0.0))
            owns = [jnp.where(left, key_f, 0.0), jnp.where(left, 0.0, key_f)]
            inner = dot_nt(key, jnp.concatenate(owns, axis=0).astype(BF))
            for s in range(2):
                part = slice(s * CHUNK, (s + 1) * CHUNK)
                gap = cums[s] - cum_row[first + s : first + s + 1, :]
                decay = jnp.where(inclusive, jnp.exp(gap), 0.0)
                d_ref[item, :, part] = decay.astype(BF)
                lower = jnp.where(strict, inner[:, part] * decay * betas[s], 0.0)
                l_ref[item, :, part] = lower.astype(BF)
                x_ref[item, :, part] = (eye - jnp.where(differ == 1, lower, 0.0)).astype(BF)

    items = steps * pairs

    for power in range(1, 7):
        mask = jnp.where((differ >> power) == 1, 1.0, 0.0).astype(BF)
        parts = []
        for i in range(items):
            block = side_by_side([part * mask for part in halves(l_ref[i])])
            parts.append(dot(x_ref[i], block).astype(BF))
        for i in range(items):
            x = x_ref[i]
            x_ref[i] = x - dot(parts[i], side_by_side(halves(x))).astype(BF)

    runs = [None] * pairs
    for c in range(steps):
        for p in range(pairs):
            item = c * pairs + p
            y = dot(x_ref[item], side_by_side(halves(r_ref[item]))).astype(BF)
            y_ref[item, :, : 2 * PAIR] = y
            z = jnp.where(top, *halves(dot(f_ref[item], y)))
            z = jnp.where(same, z, ends[item] - z)
            if c == 0:
                before_ref[item] = jnp.where(off_eye, 1.0, 0.0).astype(BF)
                runs[p] = z.astype(BF)
            else:
                before_ref[item] = runs[p]
                step = jnp.where(same, turned(z), 0.0).astype(BF)
                runs[p] = (dot(step, runs[p]) + jnp.where(same, z, 0.0)).astype(BF)
    for p in range(pairs):
        total_ref[p] = runs[p]


def keys_side(keys, values, beta_pre, decay_pre):
    length, width = keys.shape
    pairs = width // PAIR
    steps = length // CHUNK
    items = steps * pairs
    wide = pltpu.VMEM((items, CHUNK, 2 * CHUNK), BF)
    return call(
        keys_kernel,
        [],
        [
            ((items, PAIR, PAIR), BF),
            ((pairs, PAIR, PAIR), BF),
            ((items, CHUNK, 3 * PAIR), BF),
            ((items, CHUNK, 2 * CHUNK), BF),
            ((length, width), F32),
        ],
        [
            wide,
            wide,
            wide,
            pltpu.VMEM((items, PAIR, CHUNK), BF),
            pltpu.VMEM((length, width), BF),
            pltpu.VMEM((length, width), BF),
            pltpu.VMEM(beta_pre.shape, F32),
            pltpu.VMEM(beta_pre.shape, F32),
            pltpu.SemaphoreType.DMA((2 + 2 * steps,)),
        ],
        far=[
            pltpu.with_memory_space_constraint(x, pltpu.HBM)
            for x in (keys, values, beta_pre, decay_pre)
        ],
    )


def gates_kernel(gates_ref, gain_ref, gate_ref):
    gain = jnp.concatenate([gain_ref[...], gain_ref[...]], axis=1)
    for p in range(gates_ref.shape[1] // PAIR):
        lanes = slice(p * PAIR, (p + 1) * PAIR)
        gate_ref[:, lanes] = silu(gates_ref[:, lanes].astype(F32)) * gain


def queries_kernel(first, after_ref, q_ref, d_ref, y_ref, before_ref, ec_ref, o_ref, q1_ref):
    row, col = places()
    left = col < HEAD_DIM
    same = left == (row < HEAD_DIM)
    ones = jnp.where(same, 1.0, 0.0).astype(BF)
    length, width = o_ref.shape
    pairs = q_ref.shape[1] // PAIR

    def chunk(c, carry):
        rows = pl.ds(pl.multiple_of(c * CHUNK, CHUNK), CHUNK)
        for p in range(first, first + width // PAIR):
            lanes = slice(p * PAIR, (p + 1) * PAIR)
            place = slice((p - first) * PAIR, (p - first + 1) * PAIR)
            item = c * pairs + p
            query = silu(q_ref[rows, lanes].astype(F32))
            query = query * lax.rsqrt(half_sums(query * query, ones) + EPSILON)
            query = (query * HEAD_DIM ** (-0.5)).astype(BF)
            key_f = y_ref[item, :, 2 * PAIR :].astype(F32)
            owns = [jnp.where(left, key_f, 0.0), jnp.where(left, 0.0, key_f)]
            inside = dot_nt(query, jnp.concatenate(owns, axis=0).astype(BF))
            inside = (inside * d_ref[item].astype(F32)).astype(BF)
            got = halves(dot(inside, side_by_side(halves(y_ref[item, :, : 2 * PAIR]))))
            local = jnp.where(left, got[0], got[1])
            crossed = turned(jnp.where(left, got[1], got[0]))
            query = (query.astype(F32) * ec_ref[rows, lanes] - crossed).astype(BF)
            before = before_ref[item].astype(F32)
            both = [jnp.where(same, before, 0.0), jnp.where(same, turned(before), 0.0)]
            moved = halves(dot(query, jnp.concatenate(both, axis=1).astype(BF)))
            o_ref[rows, place] = local + moved[0]
            q1_ref[rows, place] = moved[1].astype(BF)
        return carry

    lax.fori_loop(0, length // CHUNK, chunk, 0)


def gates_side(gates, gain):
    return call(gates_kernel, [gates, gain.reshape(1, HEAD_DIM)], [(gates.shape, F32)])[0]


def queries_side(first, after, queries, decay, solved, before, grown):
    length, width = queries.shape
    shape = (length, width // 2)
    return call(
        functools.partial(queries_kernel, first),
        [queries, decay, solved, before, grown],
        [(shape, F32), (shape, BF)],
        far=[after],
    )


def chained(earlier, later, same):
    later = later.astype(F32)
    step = jnp.where(same, turned(later), 0.0).astype(BF)
    return dot(step, earlier.astype(BF)) + jnp.where(same, later, 0.0)


def chip_kernel(own_ref, other_ref, out_ref, kept_ref):
    kept_ref[...] = other_ref[...]
    row, col = places()
    same = (col < HEAD_DIM) == (row < HEAD_DIM)
    core = lax.axis_index(SP[2])
    count = out_ref.shape[0]
    for p in range(count):
        mine = own_ref[core * count + p]
        theirs = other_ref[core * count + p]
        first = jnp.where(core == 0, mine, theirs)
        second = jnp.where(core == 0, theirs, mine)
        out_ref[p] = chained(first, second, same).astype(BF)


def row_kernel(after_ref, *rest):
    parts, (total_ref, before_ref, all_ref) = rest[:-3], rest[-3:]
    row, col = places()
    same = (col < HEAD_DIM) == (row < HEAD_DIM)
    place = lax.axis_index(SP[1])
    size = len(parts)
    for k, part in enumerate(parts):
        all_ref[lax.rem(place - k + size, size)] = part[...]
    for p in range(total_ref.shape[0]):
        run = all_ref[0, p].astype(F32)
        inside = jnp.where(place == 0, jnp.where((row ^ col) == HEAD_DIM, 1.0, 0.0), run)
        for k in range(1, size):
            run = chained(run, all_ref[k, p], same)
            inside = jnp.where(k < place, run, inside)
        before_ref[p] = inside.astype(BF)
        total_ref[p] = run.astype(BF)


def plane_kernel(after_ref, before_ref, *rest):
    parts, out_ref = rest[:-1], rest[-1]
    row, col = places()
    same = (col < HEAD_DIM) == (row < HEAD_DIM)
    place = lax.axis_index(SP[0])
    for p in range(out_ref.shape[0]):
        state = jnp.zeros((PAIR, PAIR), F32)
        for k in range(len(parts), 0, -1):
            later = jnp.where(same, chained(state, parts[k - 1][p], same), 0.0)
            state = jnp.where(k <= place, later, state)
        state = chained(state, before_ref[p], same)
        out_ref[p] = jnp.where(same, state, 0.0).astype(BF)


def state_ahead(total, meanwhile, then):
    plane, line, core = SP
    swap = [(0, 1), (1, 0)]
    half = (total.shape[0] // 2, PAIR, PAIR)
    other = lax.ppermute(total, core, swap)
    chip, other = call(chip_kernel, [total, other], [(half, BF), (total.shape, BF)])
    size = lax.axis_size(line)
    lines = [chip] + [lax.ppermute(chip, line, ring(size, k)) for k in range(1, size)]
    early = meanwhile(chip)
    whole, before = call(
        row_kernel, lines, [(half, BF), (half, BF)], [pltpu.VMEM((size, *half), BF)], far=[early[1]]
    )
    size = lax.axis_size(plane)
    planes = [lax.ppermute(whole, plane, upward(size, k)) for k in range(1, size)]
    late = then(whole)
    (state,) = call(plane_kernel, [before] + planes, [(half, BF)], far=[late[1]])
    return early, late, (other, state, lax.ppermute(state, core, swap))


def mixed_kernel(
    o0_ref, q0_ref, o1_ref, q1_ref,
    first_ref, mine_ref, theirs_ref, gate_ref, w_ref, *rest,
):
    out_refs, (mixed_ref, state_ref) = rest[:-2], rest[-2:]
    row, col = places()
    same = (col < HEAD_DIM) == (row < HEAD_DIM)
    ones = jnp.where(same, 1.0, 0.0).astype(BF)
    length, width = gate_ref.shape
    size = len(out_refs)
    block = length // size
    core = lax.axis_index(SP[2])
    turn = lax.axis_index("tp")
    half = mine_ref.shape[0]
    state_ref[pl.ds(core * half, half)] = mine_ref[...]
    state_ref[pl.ds((1 - core) * half, half)] = theirs_ref[...]
    for p in range(width // PAIR):
        lanes = slice(p * PAIR, (p + 1) * PAIR)
        state = state_ref[p].astype(F32)
        later = jnp.where(same, chained(state, first_ref[p], same), 0.0)
        state = jnp.where(core == 0, state, later).astype(BF)
        o_ref, q_ref = ((o0_ref, q0_ref), (o1_ref, q1_ref))[p // half]
        place = slice((p % half) * PAIR, (p % half + 1) * PAIR)
        out = o_ref[:, place] + dot(q_ref[:, place], state)
        mean = half_sums(out * out, ones) * (1.0 / HEAD_DIM)
        out = (out * lax.rsqrt(mean + EPSILON) * gate_ref[:, lanes]).astype(BF)
        for k in range(size):
            start = pl.multiple_of(lax.rem(k - turn + size, size) * block, 32)
            mixed_ref[pl.ds(start, block), lanes] = out[k * block : (k + 1) * block, :]
    for n in range(w_ref.shape[1] // STRIP):
        here = slice(n * STRIP, (n + 1) * STRIP)
        got = dot(mixed_ref[...], w_ref[:, here])
        for k, out_ref in enumerate(out_refs):
            out_ref[:, here] = got[k * block : (k + 1) * block, :].astype(out_ref.dtype)


def mixed_and_projected(size, early, late, states, gate, w_out):
    length, width = gate.shape
    return call(
        mixed_kernel,
        [*early, *late, *states, gate, w_out],
        [((length // size, w_out.shape[1]), BF if k else F32) for k in range(size)],
        [pltpu.VMEM((length, width), BF), pltpu.VMEM((width // PAIR, PAIR, PAIR), BF)],
    )


def norm_kernel(stream_ref, gain_ref, *rest):
    parts, (middle_ref, normed_ref) = rest[:-2], rest[-2:]
    projected = parts[0][...]
    for part in parts[1:]:
        projected = projected + part[...].astype(F32)
    middle = (stream_ref[...].astype(F32) + projected).astype(BF)
    middle_ref[...] = middle
    middle = middle.astype(F32)
    mean = jnp.mean(middle * middle, axis=-1, keepdims=True)
    normed_ref[...] = (middle * lax.rsqrt(mean + EPSILON) * gain_ref[...]).astype(BF)


def normed_rows(stream, gain, parts):
    return call(
        norm_kernel, [stream, gain.reshape(1, -1), *parts], [(stream.shape, BF), (stream.shape, BF)]
    )


def activated(rows, gate, up):
    got = dot(rows, jnp.concatenate([gate, up], axis=1))
    width = gate.shape[1]
    return (silu(got[:, :width]) * got[:, width:]).astype(BF)


def product_nt(a, b):
    even = a.shape[1] // 256 * 256
    return dot_nt(a[:, :even], b[:, :even]) + dot_nt(a[:, even:], b[:, even:])


TILE = 128
STRIP = 256
AHEAD = 3
UP_GROUPS = (5, 6)
DOWN_GROUPS = (5, 3)


def first_channels_kernel(w_ref, across_ref, right_ref, left_ref, *rest):
    out_refs, kept_ref = rest[:2], rest[2]
    gate_ref, up_ref, down_ref, hidden_ref, in_sems, down_sems = rest[3:]
    width, hidden = gate_ref.shape
    block = out_refs[0].shape[0]
    rows = across_ref.shape[0]
    groups, spans = [], []
    for many, spread in ((hidden // TILE, UP_GROUPS), (width // STRIP, DOWN_GROUPS)):
        assert sum(spread) == many
        starts = [sum(spread[:k]) for k in range(len(spread))]
        spans.append([range(start, start + n) for start, n in zip(starts, spread)])
    for g, tiles in enumerate(spans[0]):
        here = pl.ds(tiles[0] * TILE, len(tiles) * TILE)
        group = []
        for k, ref in enumerate((gate_ref, up_ref)):
            from_ref = w_ref.at[:, pl.ds(k * hidden + tiles[0] * TILE, len(tiles) * TILE)]
            group.append(pltpu.make_async_copy(from_ref, ref.at[:, here], in_sems.at[k, g]))
        groups.append(group)
    for g, strips in enumerate(spans[1]):
        here = pl.ds(strips[0] * STRIP, len(strips) * STRIP)
        from_ref = w_ref.at[here, pl.ds(2 * hidden, hidden)]
        groups.append([pltpu.make_async_copy(from_ref, down_ref.at[here, :], down_sems.at[g])])

    def begin(g):
        if g < len(groups):
            for copy in groups[g]:
                copy.start()

    def arrived(g):
        for copy in groups[g]:
            copy.wait()
        begin(g + AHEAD)

    for g in range(AHEAD):
        begin(g)
    for g, tiles in enumerate(spans[0]):
        arrived(g)
        for j in tiles:
            here = slice(j * TILE, (j + 1) * TILE)
            every = [across_ref[...], right_ref[...], left_ref[...]]
            every = jnp.concatenate(every, axis=0)
            units = activated(every, gate_ref[:, here], up_ref[:, here])
            hidden_ref[:, here] = units[:rows, :]
            kept_ref[:, here] = units[rows:, :]
    for g, strips in enumerate(spans[1]):
        arrived(len(spans[0]) + g)
        for n in strips:
            here = slice(n * STRIP, (n + 1) * STRIP)
            got = product_nt(hidden_ref[...], down_ref[here, :])
            for k, out_ref in enumerate(out_refs):
                out_ref[:, here] = got[k * block : (k + 1) * block, :].astype(BF)


def first_channels(weights, across, right, left, hidden):
    block, width = across.shape
    half = ((block // 2, width), BF)
    out = call(
        first_channels_kernel,
        [across, right, left],
        [half, half, ((2 * block, hidden), BF)] + [((width, hidden), BF)] * 3,
        [
            pltpu.VMEM((block, hidden), BF),
            pltpu.SemaphoreType.DMA((2, len(UP_GROUPS))),
            pltpu.SemaphoreType.DMA((len(DOWN_GROUPS),)),
        ],
        far=[pltpu.with_memory_space_constraint(weights, pltpu.HBM)],
    )
    return out[:2], out[2], out[3:]


def neighbours_kernel(hidden_ref, down_ref, *out_refs):
    half = out_refs[0].shape[0]
    for n in range(down_ref.shape[0] // STRIP):
        here = slice(n * STRIP, (n + 1) * STRIP)
        got = product_nt(hidden_ref[...], down_ref[here, :]).astype(BF)
        for k, out_ref in enumerate(out_refs):
            out_ref[:, here] = got[k * half : (k + 1) * half, :]


def neighbours(hidden, down):
    shape = (hidden.shape[0] // 4, down.shape[0])
    return call(neighbours_kernel, [hidden, down], [(shape, BF)] * 4)


def more_channels_kernel(count, *refs):
    parts, (gate_ref, up_ref, down_ref) = refs[:count], refs[count : count + 3]
    out_refs, hidden_ref = refs[count + 3 : -1], refs[-1]
    block = parts[0].shape[0]
    rows = jnp.concatenate([part[...] for part in parts], axis=0)
    for j in range(gate_ref.shape[1] // TILE):
        here = slice(j * TILE, (j + 1) * TILE)
        hidden_ref[:, here] = activated(rows, gate_ref[:, here], up_ref[:, here])
    for n in range(down_ref.shape[0] // STRIP):
        here = slice(n * STRIP, (n + 1) * STRIP)
        got = product_nt(hidden_ref[...], down_ref[here, :])
        for k, out_ref in enumerate(out_refs):
            out_ref[:, here] = got[k * block : (k + 1) * block, :].astype(BF)


def more_channels(rows, projections):
    block, width = rows[0].shape
    count = len(rows)
    return call(
        functools.partial(more_channels_kernel, count),
        [*rows, *projections],
        [((block, width), BF)] * count,
        [pltpu.VMEM((count * block, projections[0].shape[1]), BF)],
    )


def joined_kernel(low_ref, more_low_ref, high_ref, more_high_ref, low_out_ref, high_out_ref):
    low = low_ref[...].astype(F32) + more_low_ref[...].astype(F32)
    low_out_ref[...] = low.astype(BF)
    high = high_ref[...].astype(F32) + more_high_ref[...].astype(F32)
    high_out_ref[...] = high.astype(BF)


def joined(low, more_low, high, more_high):
    shapes = [(low.shape, BF)] * 2
    return call(joined_kernel, [low, more_low, high, more_high], shapes)


def last_kernel(middle_ref, own_ref, *rest):
    parts, out_ref = rest[:-1], rest[-1]
    half = parts[0].shape[0]
    for k in range(2):
        rows = slice(k * half, (k + 1) * half)
        total = own_ref[rows, :].astype(F32)
        for part in parts[2 * k : 2 * k + 2]:
            total = total + part[...].astype(F32)
        out_ref[rows, :] = (middle_ref[rows, :].astype(F32) + 0.5 * total).astype(BF)


def last_sum(middle, parts):
    near = [pltpu.with_memory_space_constraint(x, pltpu.VMEM) for x in [middle, *parts]]
    return pl.pallas_call(
        last_kernel,
        in_specs=[FULL] * len(near),
        out_specs=FULL,
        out_shape=jax.ShapeDtypeStruct(middle.shape, BF),
        compiler_params=pltpu.CompilerParams(vmem_limit_bytes=16 << 20),
        name="last_sum",
    )(*near)


def per_device(
    queries,
    keys,
    values,
    gates,
    decay_pre,
    beta_pre,
    out_gain,
    w_out,
    stream,
    norm_gain,
    w_gate,
    w_up,
    w_down,
):
    hidden = w_gate.shape[1]
    weights = jnp.concatenate([w_gate, w_up, w_down.T], axis=1)
    weights = lax.all_gather(weights, SP, axis=0, tiled=True)
    size = lax.axis_size("tp")
    before, total, solved, decay, grown = keys_side(keys, values, beta_pre, decay_pre)
    gate = gates_side(gates, out_gain)
    pairs = queries.shape[1] // PAIR
    early, late, states = state_ahead(
        total,
        lambda x: queries_side(0, x, queries, decay, solved, before, grown),
        lambda x: queries_side(pairs // 2, x, queries, decay, solved, before, grown),
    )
    parts = mixed_and_projected(size, early, late, states, gate, w_out)
    parts = [parts[0]] + [lax.ppermute(parts[k], "tp", ring(size, k)) for k in (1, 2, 3)]
    middle, normed = normed_rows(stream, norm_gain, parts)
    across = lax.ppermute(normed, "tp", ring(size, 2))
    right = lax.ppermute(normed, "tp", ring(size, 1))
    left = lax.ppermute(normed, "tp", ring(size, -1))
    far, units, projections = first_channels(weights, across, right, left, hidden)
    upper = lax.ppermute(far[0], "tp", ring(size, 1))
    lower = lax.ppermute(far[1], "tp", ring(size, -1))
    right_up, right_low, left_up, left_low = neighbours(units, projections[2])
    right_up = lax.ppermute(right_up, "tp", ring(size, -1))
    left_low = lax.ppermute(left_low, "tp", ring(size, 1))
    right_low, left_up = joined(right_low, lower, left_up, upper)
    right_low = lax.ppermute(right_low, "tp", ring(size, -1))
    left_up = lax.ppermute(left_up, "tp", ring(size, 1))
    (own,) = more_channels([normed], projections)
    return last_sum(middle, [own, right_up, left_up, right_low, left_low])


def solution(mesh):
    finer = Mesh(mesh.devices.reshape(4, 4, 2, mesh.shape["tp"]), SP_TP)
    placed = (
        P(SP, "tp"),
        P(SP, "tp"),
        P(SP, "tp"),
        P(SP, "tp"),
        P("tp", SP),
        P("tp", SP),
        P(),
        P("tp", None),
        P(SP_TP, None),
        P(),
        P(SP, "tp"),
        P(SP, "tp"),
        P("tp", SP),
    )
    return jax.shard_map(
        per_device, mesh=finer, in_specs=placed, out_specs=P(SP_TP, None), check_vma=False
    )
```
